512 devices in a mesh: ep: 32 (over z, x), tp: 16 (over y, core).
Axes of the slice: x: 4, y: 8, z: 8, core: 2. Of those that a mesh axis runs over, the one named last changes fastest.
Arguments:
- tokens: bfloat16 [1024, 4096], P(('ep', 'tp')), may hold values from -6 to 6
- lengths: int32 [1024], P('ep'), may hold values from 64 to 1024, as said below
- latent_cache: bfloat16 [1024, 1024, 256], P(('ep', 'tp')), may hold values from -6 to 6
- rope_cache: bfloat16 [1024, 1024, 64], P(('ep', 'tp')), may hold values from -1200 to 1200
- attn_gain: bfloat16 [4096], replicated, may hold values from 0.099609375 to 1.8984375
- query_weight: bfloat16 [4096, 2048], P(None, 'tp'), may hold values from -0.09375 to 0.09375
- query_rot_weight: bfloat16 [4096, 1024], P(None, 'tp'), may hold values from -0.09375 to 0.09375
- latent_weight: bfloat16 [4096, 256], P('tp'), may hold values from -0.09375 to 0.09375
- key_rot_weight: bfloat16 [4096, 64], P('tp'), may hold values from -0.09375 to 0.09375
- latent_gain: bfloat16 [256], replicated, may hold values from 0.099609375 to 1.8984375
- absorb_weight: bfloat16 [16, 128, 256], P('tp'), may hold values from -0.5 to 0.5
- value_weight: bfloat16 [16, 256, 128], P('tp'), may hold values from -0.375 to 0.375
- output_weight: bfloat16 [2048, 4096], P('tp'), may hold values from -0.125 to 0.125
- mix_gain: bfloat16 [4096], replicated, may hold values from 0.099609375 to 1.8984375
- expert_gain: bfloat16 [4096], replicated, may hold values from 0.099609375 to 1.8984375
- gate_weight: bfloat16 [32, 4096, 512], P('ep', None, 'tp'), may hold values from -0.09375 to 0.09375
- up_weight: bfloat16 [32, 4096, 512], P('ep', None, 'tp'), may hold values from -0.09375 to 0.09375
- down_weight: bfloat16 [32, 512, 4096], P('ep', 'tp'), may hold values from -0.25 to 0.25
- expert_ids: int32 [1024, 2], P('ep'), may hold values from 0 to 31, all different within a row; in each aligned block of 32 rows (0 to 31, 32 to 63, ...) at most 4 rows name the same one
- route_weights: float32 [1024, 2], P('ep'), may hold values from 0.2 to 1
Outputs:
- out: bfloat16 [1024, 4096], P('ep', 'tp')
- new_latent: bfloat16 [1024, 256], P(('ep', 'tp'))
- new_rope: bfloat16 [1024, 64], P(('ep', 'tp'))
The draws below stay inside these ranges and needn't reach their ends.
Inputs may be any that keep to these rules, and one draw needn't show every extreme that they name: The new token sits at position lengths[b]; some sequence has exactly 1024. `expert_ids`: the experts of a row differ; among the rows of one index of ep no expert is named by more than 4 rows, a bound that some block reaches there.
All inputs are finite; a program needn't handle non-finite values.
Results may differ from the reference program's by a relative error of at most 0.023.
Values may be sent and summed in bfloat16 or wider, within the bound.
A program may use at most 64 MiB of HBM per device.

```python
import math
import jax
import jax.numpy as jnp
import numpy as np
from jax import lax

D = 4096
HEADS = 16
QK_NOPE = 128
QK_ROPE = 64
VALUE_DIM = 128
LATENT = 256
FF = 512
TOPK = 2
SEQ_DEV = 2
CTX = 1024
BATCH = 1024
EXPERTS = 32
CAP = 4
N_EP = 32
N_TP = 16


def draw_lengths(key, part):
    level_key, extra_key, full_key = jax.random.split(key, 3)
    level = jax.random.randint(level_key, (BATCH,), 1, 5)
    floor_len = jnp.right_shift(jnp.full((BATCH,), CTX, jnp.int32), level)
    extra = jax.random.randint(extra_key, (BATCH,), 0, CTX + 1) % (floor_len + 1)
    chosen = jax.random.randint(full_key, (), 0, BATCH)
    values = jnp.where(jnp.arange(BATCH) == chosen, CTX, floor_len + extra)
    return values.astype(jnp.int32)


def draw_rope_cache(key, part):
    normal_key, planted_key = jax.random.split(key)
    values = jnp.clip(jax.random.normal(normal_key, (BATCH, CTX, QK_ROPE), jnp.float32), -6.0, 6.0)
    return values.astype(jnp.bfloat16)


def level_of(key, dims, shards, least, largest):
    level = 1.0
    for dim, shards_of in shards:
        steps = jax.random.uniform(jax.random.fold_in(jax.random.fold_in(key, 6), dim), (shards_of,), jnp.float32, least / len(shards), largest / len(shards))
        level = level * jnp.repeat(jnp.exp(steps), dims[dim] // shards_of).reshape((-1,) + (1,) * (len(dims) - 1 - dim))
    return level


def routed_block(rng, own, number, rows, amount, top, limit, skew):
    order = jax.random.permutation(rng, amount)
    crowded, common = shares(amount, rows * top, limit, skew, True), shares(amount, rows * top, limit, skew, False)
    places = jnp.arange(amount)

    def named(sizes, rotation):
        used = int((sizes > 0).sum())
        fixed = max(1, used // 4)
        passed = fixed + (places - fixed + rotation * (used - fixed)) % max(1, amount - fixed)
        return jnp.zeros((amount,), jnp.int32).at[order[jnp.where(places < fixed, places, passed)]].set(jnp.asarray(sizes, jnp.int32))

    sizes = jnp.where(number % 4 == 0, named(crowded, number // 4), named(common, number - number // 4 - 1))
    mixed = jax.random.permutation(jax.random.fold_in(own, 3), amount)
    source_of, receiver = mixed[0:amount // 2 * 2:2], mixed[1:amount // 2 * 2:2]
    slack = jnp.minimum(sizes[source_of] - 1, limit - sizes[receiver]) // 2
    slack = jnp.where((source_of == order[0]) | (receiver == order[0]) | (sizes[receiver] == 0), 0, jnp.maximum(slack, 0))
    passed = jax.random.randint(jax.random.fold_in(own, 4), (amount // 2,), 0, 1 << 20) % (slack + 1)
    sizes = sizes.at[source_of].add(-passed).at[receiver].add(passed)
    members = jnp.searchsorted(jnp.cumsum(sizes), jnp.arange(rows * top), side="right").astype(jnp.int32)
    table = members.reshape(top, rows).T
    table = table[jax.random.permutation(jax.random.fold_in(own, 1), rows)]
    rotation = jax.random.randint(jax.random.fold_in(own, 2), (rows, 1), 0, top)
    return jnp.take_along_axis(table, (jnp.arange(top)[None, :] + rotation) % top, axis=1)


def shares(amount, total, bound, skew, full):
    weights = [(1 << 20) // math.isqrt(standing ** skew) + 1 for standing in range(1, amount + 1)]
    largest = bound if full else min(bound, max(-(-total // amount), total * weights[0] // sum(weights)))
    least = 1 if total - largest >= amount - 1 else 0
    counts, spare = [largest] + [least] * (amount - 1), total - largest - least * (amount - 1)
    while spare > 0:
        candidates = [i for i in range(1, amount) if counts[i] < largest] or [i for i in range(1, amount) if counts[i] < bound]
        pool, budget = sum([weights[i] for i in candidates]), spare
        for i in candidates:
            more = min(bound - counts[i], max(1, budget * weights[i] // pool), spare)
            counts[i] = counts[i] + more
            spare = spare - more
    return np.array(counts)


def bell_draw(stream_key, dims, scale, limit, cuts=(), kind=jnp.bfloat16):
    result = jax.random.normal(stream_key, dims, jnp.float32) * scale
    if len(cuts) > 0:
        result = level_of(stream_key, dims, cuts, -0.22, 0.18) * result
    return jnp.clip(result, min=-limit, max=limit).astype(kind)


def setup_inputs(seed: int = 0) -> dict:
    splits = jax.random.split(jax.random.key(seed), 21)
    tokens = bell_draw(splits[0], (BATCH, D), 1.0, 6.0, ((0, 512),))
    lengths = draw_lengths(jax.random.fold_in(splits[20], 71), 0)
    latent_cache = bell_draw(splits[2], (BATCH, CTX, LATENT), 1.0, 6.0, ((0, 512),))
    rope_cache = draw_rope_cache(jax.random.fold_in(splits[20], 71), 0)
    attn_gain = jnp.clip(1.0 + 0.18 * jax.random.normal(splits[4], (D,), jnp.float32), 0.099609375, 1.8984375).astype(jnp.bfloat16)
    query_weight = bell_draw(splits[5], (D, HEADS * QK_NOPE), D ** -0.5, 0.09375, ((1, 16),))
    query_rot_weight = bell_draw(splits[6], (D, HEADS * QK_ROPE), D ** -0.5, 0.09375, ((1, 16),))
    latent_weight = bell_draw(splits[7], (D, LATENT), D ** -0.5, 0.09375, ((0, 16),))
    key_rot_weight = bell_draw(splits[8], (D, QK_ROPE), D ** -0.5, 0.09375, ((0, 16),))
    latent_gain = jnp.clip(1.0 + 0.18 * jax.random.normal(splits[9], (LATENT,), jnp.float32), 0.099609375, 1.8984375).astype(jnp.bfloat16)
    absorb_weight = bell_draw(splits[10], (HEADS, QK_NOPE, LATENT), QK_NOPE ** -0.5, 0.5, ((0, 16),))
    value_weight = bell_draw(splits[11], (HEADS, LATENT, VALUE_DIM), LATENT ** -0.5, 0.375, ((0, 16),))
    output_weight = bell_draw(splits[12], (HEADS * VALUE_DIM, D), (HEADS * VALUE_DIM) ** -0.5, 0.125, ((0, 16),))
    mix_gain = jnp.clip(1.0 + 0.18 * jax.random.normal(splits[13], (D,), jnp.float32), 0.099609375, 1.8984375).astype(jnp.bfloat16)
    expert_gain = jnp.clip(1.0 + 0.18 * jax.random.normal(splits[14], (D,), jnp.float32), 0.099609375, 1.8984375).astype(jnp.bfloat16)
    gate_weight = bell_draw(splits[15], (EXPERTS, D, FF), D ** -0.5, 0.09375, ((0, 32), (2, 16)))
    up_weight = bell_draw(splits[16], (EXPERTS, D, FF), D ** -0.5, 0.09375, ((0, 32), (2, 16)))
    down_weight = bell_draw(splits[17], (EXPERTS, FF, D), FF ** -0.5, 0.25, ((0, 32), (1, 16)))
    expert_ids_keys = jax.random.split(jax.random.fold_in(splits[18], 1), BATCH // (SEQ_DEV * N_TP))
    expert_ids_turns = jax.random.permutation(jax.random.fold_in(splits[18], 3), BATCH // (SEQ_DEV * N_TP))
    expert_ids = jax.vmap(lambda own, number: routed_block(jax.random.fold_in(splits[18], 2), own, number, SEQ_DEV * N_TP, EXPERTS, TOPK, CAP, 2))(expert_ids_keys, expert_ids_turns).reshape((BATCH, TOPK))
    route_weights = jnp.clip(0.2 + 0.8 * jax.random.uniform(splits[19], (BATCH, TOPK), jnp.float32) ** level_of(splits[19], (BATCH, TOPK), ((0, 32),), -0.2, 0.2), 0.2, 1.0)
    return {"tokens": tokens, "lengths": lengths, "latent_cache": latent_cache, "rope_cache": rope_cache, "attn_gain": attn_gain, "query_weight": query_weight, "query_rot_weight": query_rot_weight, "latent_weight": latent_weight, "key_rot_weight": key_rot_weight, "latent_gain": latent_gain, "absorb_weight": absorb_weight, "value_weight": value_weight, "output_weight": output_weight, "mix_gain": mix_gain, "expert_gain": expert_gain, "gate_weight": gate_weight, "up_weight": up_weight, "down_weight": down_weight, "expert_ids": expert_ids, "route_weights": route_weights}


norm_floor = 1e-06
rope_base = 10000.0
masked_score = -1e+30
sub_rows = 16

def normed(values, gain):
    wide = values.astype(jnp.float32)
    factor = lax.rsqrt(lax.optimization_barrier(jnp.mean(wide * wide, axis=-1, keepdims=True)) + norm_floor)
    return wide * factor * gain.astype(jnp.float32)

def rotate(values, angle_pos):
    half = values.shape[-1] // 2
    freqs = rope_base ** (-jnp.arange(half, dtype=jnp.float32) / half)
    angles = angle_pos.astype(jnp.float32)[..., None] * freqs
    cosine = jnp.cos(angles)
    sine = jnp.sin(angles)
    first_half = values[..., :half]
    second_half = values[..., half:]
    return jnp.concatenate([first_half * cosine - second_half * sine, second_half * cosine + first_half * sine], axis=-1)

def through_bf16(values):
    return lax.optimization_barrier(values.astype(jnp.bfloat16)).astype(jnp.float32)

def attend_block(operands):
    latents, rotated, query_lat, query_rot, own_lat, own_rot, seq_len = operands
    score_scale = (QK_NOPE + QK_ROPE) ** (-0.5)
    lat_wide = latents.astype(jnp.float32)
    rot_wide = rotated.astype(jnp.float32)
    query_lat = query_lat.astype(jnp.float32)
    query_rot = query_rot.astype(jnp.float32)
    own_lat = own_lat.astype(jnp.float32)
    own_rot = own_rot.astype(jnp.float32)
    scores = (jnp.einsum('bhl,bkl->bhk', query_lat, lat_wide) + jnp.einsum('bhr,bkr->bhk', query_rot, rot_wide)) * score_scale
    valid = jnp.arange(CTX)[None, None, :] < seq_len[:, None, None]
    scores = jnp.where(valid, scores, masked_score)
    own_score = (lax.optimization_barrier(jnp.sum(query_lat * own_lat[:, None, :], axis=-1)) + lax.optimization_barrier(jnp.sum(query_rot * own_rot[:, None, :], axis=-1))) * score_scale
    top = jnp.maximum(lax.optimization_barrier(jnp.max(scores, axis=-1)), own_score)
    weights = jnp.where(valid, jnp.exp(scores - top[..., None]), 0.0)
    own_weight = jnp.exp(own_score - top)
    total = lax.optimization_barrier(jnp.sum(weights, axis=-1)) + own_weight
    summed = jnp.einsum('bhk,bkl->bhl', through_bf16(weights), lat_wide) + through_bf16(own_weight)[..., None] * own_lat[:, None, :]
    return (summed / total[..., None]).astype(jnp.bfloat16)

def reference(tokens, lengths, latent_cache, rope_cache, attn_gain, query_weight, query_rot_weight, latent_weight, key_rot_weight, latent_gain, absorb_weight, value_weight, output_weight, mix_gain, expert_gain, gate_weight, up_weight, down_weight, expert_ids, route_weights):
    batch = tokens.shape[0]
    normed_in = normed(tokens, attn_gain).astype(jnp.bfloat16)
    q_nope = jnp.dot(normed_in, query_weight, preferred_element_type=jnp.float32).astype(jnp.bfloat16)
    q_nope = q_nope.reshape(batch, HEADS, QK_NOPE)
    q_rot = jnp.dot(normed_in, query_rot_weight, preferred_element_type=jnp.float32).reshape(batch, HEADS, QK_ROPE)
    q_rot = rotate(q_rot, lengths[:, None]).astype(jnp.bfloat16)
    q_latent = jnp.einsum('bhn,hnl->bhl', q_nope.astype(jnp.float32), absorb_weight.astype(jnp.float32)).astype(jnp.bfloat16)
    key_raw = jnp.dot(normed_in, jnp.concatenate([latent_weight, key_rot_weight], axis=1), preferred_element_type=jnp.float32)
    new_latent = normed(key_raw[:, :LATENT], latent_gain).astype(jnp.bfloat16)
    new_rope = rotate(key_raw[:, LATENT:], lengths).astype(jnp.bfloat16)
    blocks = batch // 8

    def split_rows(values):
        return values.reshape((blocks, 8) + values.shape[1:])
    head_latent = lax.map(attend_block, (split_rows(latent_cache), split_rows(rope_cache), split_rows(q_latent), split_rows(q_rot), split_rows(new_latent), split_rows(new_rope), split_rows(lengths)))
    head_latent = head_latent.reshape(batch, HEADS, LATENT)
    head_values = jnp.einsum('bhl,hlv->bhv', head_latent.astype(jnp.float32), value_weight.astype(jnp.float32))
    head_values = head_values.astype(jnp.bfloat16).reshape(batch, HEADS * VALUE_DIM)
    group_width = HEADS // N_TP * VALUE_DIM

    def add_group(group, total):
        begin = (group * group_width).astype(jnp.int32)
        columns = lax.dynamic_slice_in_dim(head_values, begin, group_width, 1)
        rows = lax.dynamic_slice_in_dim(output_weight, begin, group_width, 0)
        return total + through_bf16(jnp.dot(columns, rows, preferred_element_type=jnp.float32))
    mixed = lax.fori_loop(0, N_TP, add_group, jnp.zeros((batch, D), jnp.float32)).astype(jnp.bfloat16)
    resid = (tokens.astype(jnp.float32) + normed(mixed, mix_gain)).astype(jnp.bfloat16)
    expert_in = normed(resid, expert_gain).astype(jnp.bfloat16)
    routes = expert_ids.reshape(-1).astype(jnp.int32)
    count_routes = routes.shape[0]
    order = jnp.argsort(routes, stable=True).astype(jnp.int32)
    picks = (routes[:, None] == jnp.arange(EXPERTS, dtype=jnp.int32)[None, :]).astype(jnp.int32)
    loads = lax.optimization_barrier(jnp.sum(picks, axis=0)).astype(jnp.int32)
    offsets = (jnp.cumsum(loads) - loads).astype(jnp.int32)
    inverse = jnp.zeros((count_routes,), jnp.int32).at[order].set(jnp.arange(count_routes, dtype=jnp.int32))
    most_rows = N_EP * CAP
    padded = jnp.concatenate([order, jnp.zeros((most_rows,), jnp.int32)])
    ff_group = FF // N_TP

    def run_expert(operands):
        gate_mat, up_mat, down_mat, begin, load = operands
        chosen = lax.dynamic_slice_in_dim(padded, begin.astype(jnp.int32), most_rows, 0)
        rows_all = expert_in[chosen // TOPK]

        def compute(rows_in):
            gate = jnp.dot(rows_in, gate_mat, preferred_element_type=jnp.float32)
            upward = jnp.dot(rows_in, up_mat, preferred_element_type=jnp.float32)
            hidden = (jax.nn.silu(gate) * upward).astype(jnp.bfloat16)
            parts = jnp.einsum('rgf,gfd->rgd', hidden.reshape(sub_rows, N_TP, ff_group).astype(jnp.float32), down_mat.reshape(N_TP, ff_group, D).astype(jnp.float32))
            return lax.optimization_barrier(jnp.sum(through_bf16(parts), axis=1)).astype(jnp.bfloat16)

        def empty_rows(rows_in):
            return jnp.zeros((sub_rows, D), jnp.bfloat16)
        pieces = []
        for piece_index in range(most_rows // sub_rows):
            rows = rows_all[piece_index * sub_rows:(piece_index + 1) * sub_rows]
            pieces.append(lax.cond(piece_index * sub_rows < load, compute, empty_rows, rows))
        return jnp.concatenate(pieces, axis=0)
    results = lax.map(run_expert, (gate_weight, up_weight, down_weight, offsets, loads))
    ranks = inverse - offsets[routes]
    picked = results.reshape(EXPERTS * most_rows, D)[routes * most_rows + ranks]
    moe_out = lax.optimization_barrier(jnp.sum(picked.astype(jnp.float32).reshape(batch, TOPK, D) * route_weights[:, :, None], axis=1))
    out = (resid.astype(jnp.float32) + moe_out).astype(jnp.bfloat16)
    return (out, new_latent, new_rope)
```

```python
import functools

import jax
import jax.numpy as jnp
from jax import lax
from jax.experimental import pallas as pl
from jax.experimental.pallas import tpu as pltpu
from jax.sharding import PartitionSpec as P

MESH = pl.DeviceIdType.MESH
F32 = jnp.float32
BF16 = jnp.bfloat16
HIGHEST = lax.Precision.HIGHEST

QK_NOPE = 128
QK_ROPE = 64
norm_floor = 1e-06
rope_base = 10000.0
masked_score = -1e30

LAT_AT, KEY_AT, ROT_AT, KEY_ROT_AT, MESSAGE = 0, 256, 512, 640, 768


def dot(a, b, precision=None):
    return lax.dot_general(
        a, b, (((1,), (0,)), ((), ())), preferred_element_type=F32, precision=precision
    )


def dot_t(a, b, precision=None):
    return lax.dot_general(
        a, b, (((1,), (1,)), ((), ())), preferred_element_type=F32, precision=precision
    )


def swap_halves(x):
    half = x.shape[-1] // 2
    return jnp.concatenate([x[:, half:], x[:, :half]], axis=1)


def iota(shape, dim):
    return lax.broadcasted_iota(jnp.int32, shape, dim)


def kernel(
    n_tp,
    n_ep,
    tokens,
    lengths,
    latent_cache,
    rope_cache,
    gains,
    turns,
    query_weight,
    query_rot_weight,
    latent_weight,
    key_rot_weight,
    absorb_weight,
    value_weight,
    output_weight,
    gate_weight,
    up_weight,
    down_weight,
    expert_ids,
    route_weights,
    out,
    new_latent,
    new_rope,
    lat_v,
    rope_v,
    qw_v,
    qrw_v,
    lw_v,
    krw_v,
    abs_v,
    val_v,
    ow_v,
    gate_v,
    up_v,
    down_v,
    tok_f,
    normed_b,
    msg_f,
    lat_f,
    route_f,
    tok_in,
    qry_out,
    qry_in,
    att_out,
    att_in,
    mix_out,
    mix_in,
    sum_in,
    dis_out,
    dis_in,
    part_out,
    part_in,
    hid_in,
    ret_out,
    ret_in,
    gate_in,
    up_in,
    down_in,
    local_sems,
    send_sems,
    recv_sems,
):
    me = lax.axis_index("tp")
    group = lax.axis_index("ep")
    rows = tok_f.shape[0]
    own = rows // n_tp
    width = tok_f.shape[1]
    cols = width // n_tp
    slots = dis_out.shape[1]
    ff_dev = gate_v.shape[0]
    latent = abs_v.shape[1]
    my_cols = pl.ds(pl.multiple_of(me * cols, cols), cols)

    def load(index, src, dst):
        copy = pltpu.make_async_copy(src, dst, local_sems.at[index])
        copy.start()
        return copy

    tok_copy = load(0, tokens, tok_in.at[me])
    qw_copy = load(1, query_weight, qw_v)
    qrw_copy = load(2, query_rot_weight, qrw_v)
    lw_copy = load(3, latent_weight, lw_v)
    krw_copy = load(4, key_rot_weight, krw_v)
    abs_copy = load(5, absorb_weight.at[0], abs_v)
    gate_copy = load(6, gate_weight.at[0], gate_v)
    up_copy = load(7, up_weight.at[0], up_v)
    lat_copy = load(8, latent_cache, lat_v)
    rope_copy = load(9, rope_cache, rope_v)
    val_copy = load(10, value_weight.at[0], val_v)
    ow_copy = load(11, output_weight, ow_v)
    down_copy = load(12, down_weight.at[0], down_v)

    barrier = pltpu.get_barrier_semaphore()

    def greet_tp(d, _):
        pl.semaphore_signal(
            barrier, inc=1, device_id={"tp": lax.rem(me + d, n_tp)}, device_id_type=MESH
        )
        return 0

    def greet_ep(d, _):
        pl.semaphore_signal(
            barrier, inc=1, device_id={"ep": lax.rem(group + d, n_ep)}, device_id_type=MESH
        )
        return 0

    lax.fori_loop(1, n_ep, greet_ep, 0)
    lax.fori_loop(1, n_tp, greet_tp, 0)
    pl.semaphore_wait(barrier, n_tp - 1 + n_ep - 1)

    order = sorted(range(1, n_tp), key=lambda d: -min(d, n_tp - d))

    def send(src, dst, stage, device):
        pltpu.make_async_remote_copy(
            src_ref=src,
            dst_ref=dst,
            send_sem=send_sems.at[stage],
            recv_sem=recv_sems.at[stage],
            device_id=device,
            device_id_type=MESH,
        ).start()

    def send_tp(stage, src_of, dst, before=None):
        for d in order:
            peer = lax.rem(me + d, n_tp)
            send(src_of(peer), dst, stage, {"tp": peer})

    def send_ep(stage, src_of, dst):
        def step(d, _):
            peer = lax.rem(group + d, n_ep)
            send(src_of(peer), dst, stage, {"ep": peer})
            return 0

        lax.fori_loop(1, n_ep, step, 0)

    def arrived(stage, buffer):
        some = buffer.at[pl.ds(0, buffer.shape[0] - 1)]
        pltpu.make_async_copy(some, some, recv_sems.at[stage]).wait()

    def sent(stage, buffer):
        some = buffer.at[pl.ds(0, buffer.shape[0] - 1)]
        pltpu.make_async_copy(some, some, send_sems.at[stage]).wait()

    tok_copy.wait()
    send_tp(0, lambda peer: tok_in.at[me], tok_in.at[me])

    square = (rows, rows)
    eye = (iota(square, 0) == iota(square, 1)).astype(F32)
    ahead_row = iota(square, 0) < iota(square, 1)
    ahead_col = iota(square, 1) < iota(square, 0)
    ids = expert_ids[...].astype(F32)
    weights_row = route_weights[...]
    id_rows = [ids[k : k + 1, :] for k in range(2)]
    id_cols = [jnp.sum(eye * r, axis=1, keepdims=True) for r in id_rows]
    weight_cols = [
        jnp.sum(eye * weights_row[k : k + 1, :], axis=1, keepdims=True) for k in range(2)
    ]

    def same(j, k):
        return id_cols[j] == id_rows[k]

    def count(mask, axis):
        return jnp.sum(jnp.where(mask, 1.0, 0.0), axis=axis, keepdims=True)

    rank_row0 = count(same(0, 0) & ahead_row, 0)
    rank_row1 = count(same(0, 1), 0) + count(same(1, 1) & ahead_row, 0)
    rank_col0 = count(same(0, 0) & ahead_col, 1)
    rank_col1 = count(same(1, 0), 1) + count(same(1, 1) & ahead_col, 1)
    target_rows = [id_rows[0] * slots + rank_row0, id_rows[1] * slots + rank_row1]
    target_cols = [id_cols[0] * slots + rank_col0, id_cols[1] * slots + rank_col1]
    all_slots = n_ep * slots
    down_iota = iota((all_slots, rows), 0).astype(F32)
    across_iota = iota((rows, all_slots), 1).astype(F32)
    dispatch = (
        jnp.where(down_iota == target_rows[0], 1.0, 0.0)
        + jnp.where(down_iota == target_rows[1], 1.0, 0.0)
    ).astype(BF16)
    combine = jnp.where(across_iota == target_cols[0], weight_cols[0], 0.0) + jnp.where(
        across_iota == target_cols[1], weight_cols[1], 0.0
    )

    arrived(0, tok_in)
    for t in range(n_tp):
        tok_f[own * t : own * (t + 1), :] = tok_in[t].astype(F32)
    chunk = 512
    square_sum = jnp.zeros((rows, 1), F32)
    for c in range(0, width, chunk):
        x = tok_f[:, c : c + chunk]
        square_sum = square_sum + jnp.sum(x * x, axis=1, keepdims=True)
    factor = lax.rsqrt(square_sum / width + norm_floor)
    for c in range(0, width, chunk):
        x = tok_f[:, c : c + chunk]
        normed_b[:, c : c + chunk] = (x * factor * gains[0:1, c : c + chunk]).astype(BF16)

    cosine, sine = turns[0], turns[1]
    qw_copy.wait()
    q_nope = dot(normed_b[...], qw_v[...]).astype(BF16)
    abs_copy.wait()
    msg_f[:, LAT_AT : LAT_AT + latent] = dot(q_nope, abs_v[...])
    qrw_copy.wait()
    q_rot = dot_t(normed_b[...], qrw_v[...])
    msg_f[:, ROT_AT : ROT_AT + QK_ROPE] = q_rot * cosine + swap_halves(q_rot) * sine
    slice_rows = normed_b[:, my_cols]
    lw_copy.wait()
    msg_f[:, KEY_AT : KEY_AT + latent] = dot(slice_rows, lw_v[...])
    krw_copy.wait()
    msg_f[:, KEY_ROT_AT : KEY_ROT_AT + QK_ROPE] = dot_t(slice_rows, krw_v[...])
    for t in range(n_tp):
        qry_out[t] = msg_f[own * t : own * (t + 1), :].astype(BF16)

    send_tp(1, lambda peer: qry_out.at[peer], qry_in.at[me])
    qry_in[me] = qry_out[me]
    gate_copy.wait()

    def piece(ref, peer):
        return ref.at[:, pl.ds(pl.multiple_of(peer * cols, cols), cols)]

    send_tp(2, lambda peer: piece(gate_v, peer), gate_in.at[me])
    gate_in[me] = gate_v[:, my_cols]

    own_rows = (iota((8, rows), 1) == own * me + iota((8, rows), 0)).astype(F32)
    own_cosine = dot(own_rows, cosine, HIGHEST)[:own]
    own_sine = dot(own_rows, sine, HIGHEST)[:own]
    lat_copy.wait()
    rope_copy.wait()

    arrived(1, qry_in)
    key_sum = jnp.zeros((own, MESSAGE), F32)
    for h in range(n_tp):
        part = qry_in[h].astype(F32)
        key_sum = key_sum + part
        msg_f[own * h : own * (h + 1), :] = part
    key_raw = key_sum[:, KEY_AT : KEY_AT + latent]
    key_factor = lax.rsqrt(jnp.mean(key_raw * key_raw, axis=1, keepdims=True) + norm_floor)
    own_lat = (key_raw * key_factor * gains[3:4, :latent]).astype(BF16)
    rope_raw = key_sum[:, KEY_ROT_AT : KEY_ROT_AT + QK_ROPE]
    own_rot = (rope_raw * own_cosine + swap_halves(rope_raw) * own_sine).astype(BF16)
    new_latent[...] = own_lat
    new_rope[...] = own_rot
    own_lat = own_lat.astype(F32)
    own_rot = own_rot.astype(F32)

    scale = (QK_NOPE + QK_ROPE) ** (-0.5)
    queries = msg_f[:, LAT_AT : LAT_AT + latent]
    rotated = msg_f[:, ROT_AT : ROT_AT + QK_ROPE]
    queries_b = queries.astype(BF16)
    rotated_b = rotated.astype(BF16)
    context = lat_v.shape[1]
    row_col = iota((rows, 1), 0)
    first = lax.rem(row_col, own) == 0

    def of_row(a, b):
        return jnp.where(first, a, b)

    scores = of_row(
        dot_t(queries_b, lat_v[0]) + dot(rotated_b, rope_v[0]),
        dot_t(queries_b, lat_v[1]) + dot(rotated_b, rope_v[1]),
    )
    row_len = of_row(lengths[own * me], lengths[own * me + 1])
    valid = iota((rows, context), 1) < row_len
    scores = jnp.where(valid, scores * scale, masked_score)
    lat_rows = of_row(own_lat[0:1], own_lat[1:2])
    rot_rows = of_row(own_rot[0:1], own_rot[1:2])
    own_score = (
        jnp.sum(queries * lat_rows, axis=1, keepdims=True)
        + jnp.sum(rotated * rot_rows, axis=1, keepdims=True)
    ) * scale
    top = jnp.maximum(jnp.max(scores, axis=1, keepdims=True), own_score)
    weights = jnp.where(valid, jnp.exp(scores - top), 0.0)
    own_weight = jnp.exp(own_score - top)
    total = jnp.sum(weights, axis=1, keepdims=True) + own_weight
    summed = (
        dot(jnp.where(first, weights, 0.0).astype(BF16), lat_v[0])
        + dot(jnp.where(first, 0.0, weights).astype(BF16), lat_v[1])
        + own_weight.astype(BF16).astype(F32) * lat_rows
    )
    lat_f[...] = summed / total
    for h in range(n_tp):
        att_out[h] = lat_f[own * h : own * (h + 1), :].astype(BF16)

    send_tp(3, lambda peer: att_out.at[peer], att_in.at[me])
    att_in[me] = att_out[me]
    up_copy.wait()
    send_tp(4, lambda peer: piece(up_v, peer), up_in.at[me])
    up_in[me] = up_v[:, my_cols]
    val_copy.wait()
    ow_copy.wait()

    arrived(3, att_in)
    for t in range(n_tp):
        lat_f[own * t : own * (t + 1), :] = att_in[t].astype(F32)
    head_values = dot(lat_f[...].astype(BF16), val_v[...]).astype(BF16)

    for d in order + [0]:
        peer = lax.rem(me + d, n_tp)
        share = dot(
            head_values, ow_v[:, pl.ds(pl.multiple_of(peer * cols, cols), cols)]
        ).astype(BF16)
        if d:
            mix_out[peer] = share
            send(mix_out.at[peer], mix_in.at[me], 5, {"tp": peer})
        else:
            mix_in[me] = share

    tok_cols = tok_f[:, my_cols]
    mix_gain = gains[1:2, my_cols]
    expert_gain = gains[2:3, my_cols]

    arrived(5, mix_in)
    mixed = mix_in[0].astype(F32)
    for t in range(1, n_tp):
        mixed = mixed + mix_in[t].astype(F32)
    mixed = mixed.astype(BF16).astype(F32)
    scaled = mixed * mix_gain

    def as_row(col):
        return jnp.sum(eye * col, axis=0, keepdims=True)

    def as_col(row):
        return jnp.sum(eye * row, axis=1, keepdims=True)

    def row_sum(value):
        return as_row(jnp.sum(value, axis=1, keepdims=True))

    sums = jnp.concatenate(
        [
            row_sum(mixed * mixed),
            row_sum(tok_cols * scaled),
            row_sum(scaled * scaled),
            jnp.zeros((1, rows), F32),
        ],
        axis=1,
    )
    sum_in[me] = sums
    send_tp(6, lambda peer: sum_in.at[me], sum_in.at[me])
    arrived(6, sum_in)
    sums = sum_in[0]
    for t in range(1, n_tp):
        sums = sums + sum_in[t]
    mix_square = as_col(sums[:, 0:rows])
    cross = as_col(sums[:, rows : 2 * rows])
    scaled_square = as_col(sums[:, 2 * rows : 3 * rows])
    mix_factor = lax.rsqrt(mix_square / width + norm_floor)
    resid = (tok_cols + scaled * mix_factor).astype(BF16).astype(F32)
    resid_square = square_sum + mix_factor * (2.0 * cross + mix_factor * scaled_square)
    resid_factor = lax.rsqrt(jnp.maximum(resid_square, 0.0) / width + norm_floor)
    expert_in = (resid * resid_factor * expert_gain).astype(BF16)

    route_f[...] = dot(dispatch, expert_in)
    for e in range(n_ep):
        dis_out[e] = route_f[slots * e : slots * (e + 1), :].astype(BF16)
    send_ep(7, lambda peer: dis_out.at[peer], dis_in.at[group])
    dis_in[group] = dis_out[group]
    down_copy.wait()
    send_tp(8, lambda peer: piece(down_v, peer), down_in.at[me])
    down_in[me] = down_v[:, my_cols]

    arrived(2, gate_in)
    arrived(4, up_in)
    arrived(7, dis_in)
    for g in range(n_ep):
        route_f[slots * g : slots * (g + 1), :] = dis_in[g].astype(F32)
    received = route_f[...].astype(BF16)
    ff = n_tp * ff_dev
    out_rows = all_slots // n_tp
    for n, source in enumerate((gate_in, up_in)):
        part = dot_t(received, source[...].reshape(ff, cols))
        part_out[:, :, n * ff : (n + 1) * ff] = part.reshape(n_tp, out_rows, ff).astype(BF16)

    send_tp(9, lambda peer: part_out.at[peer], part_in.at[me])
    part_in[me] = part_out[me]
    arrived(9, part_in)
    both = part_in[0].astype(F32)
    for t in range(1, n_tp):
        both = both + part_in[t].astype(F32)
    gate, upward = both[:, :ff], both[:, ff:]
    hid_in[me] = (gate / (1.0 + jnp.exp(-gate)) * upward).astype(BF16)

    send_tp(10, lambda peer: hid_in.at[me], hid_in.at[me])
    arrived(8, down_in)
    arrived(10, hid_in)
    hidden = hid_in[...].astype(F32).reshape(all_slots, ff).astype(BF16)
    route_f[...] = dot(hidden, down_in[...].reshape(ff, cols))
    for g in range(n_ep):
        ret_out[g] = route_f[slots * g : slots * (g + 1), :].astype(BF16)

    send_ep(11, lambda peer: ret_out.at[peer], ret_in.at[group])
    ret_in[group] = ret_out[group]
    arrived(11, ret_in)
    for e in range(n_ep):
        route_f[slots * e : slots * (e + 1), :] = ret_in[e].astype(F32)
    out[...] = (resid + dot(combine, route_f[...], HIGHEST)).astype(BF16)

    for stage, buffer in (
        (0, tok_in),
        (1, qry_in),
        (2, gate_in),
        (3, att_in),
        (4, up_in),
        (5, mix_in),
        (6, sum_in),
        (7, dis_in),
        (8, down_in),
        (9, part_in),
        (10, hid_in),
        (11, ret_in),
    ):
        sent(stage, buffer)


def per_device(
    tokens,
    lengths,
    latent_cache,
    rope_cache,
    attn_gain,
    query_weight,
    query_rot_weight,
    latent_weight,
    key_rot_weight,
    latent_gain,
    absorb_weight,
    value_weight,
    output_weight,
    mix_gain,
    expert_gain,
    gate_weight,
    up_weight,
    down_weight,
    expert_ids,
    route_weights,
):
    n_tp, n_ep = lax.axis_size("tp"), lax.axis_size("ep")
    own, width = tokens.shape
    rows = own * n_tp
    cols = width // n_tp
    latent = latent_weight.shape[1]
    context = latent_cache.shape[1]
    ff_dev = gate_weight.shape[2]
    ff = ff_dev * n_tp
    slots = 2 * rows * expert_ids.shape[1] // n_ep
    all_slots = n_ep * slots
    out_rows = all_slots // n_tp

    half = QK_ROPE // 2
    freqs = rope_base ** (-jnp.arange(half, dtype=F32) / half)
    angles = lengths.astype(F32)[:, None] * freqs
    cosine, sine = jnp.cos(angles), jnp.sin(angles)
    turns = jnp.stack(
        [jnp.concatenate([cosine, cosine], 1), jnp.concatenate([-sine, sine], 1)]
    )
    gains = jnp.stack(
        [attn_gain, mix_gain, expert_gain, jnp.pad(latent_gain, (0, width - latent))]
    ).astype(F32)

    operands = (
        tokens,
        lengths,
        latent_cache,
        jnp.swapaxes(rope_cache, 1, 2),
        gains,
        turns,
        query_weight,
        query_rot_weight.T,
        latent_weight,
        key_rot_weight.T,
        absorb_weight,
        value_weight,
        output_weight,
        jnp.swapaxes(gate_weight, 1, 2),
        jnp.swapaxes(up_weight, 1, 2),
        down_weight,
        expert_ids.T,
        route_weights.T,
    )
    spaces = {1: pltpu.SMEM, 4: pltpu.VMEM, 5: pltpu.VMEM, 16: pltpu.VMEM, 17: pltpu.VMEM}
    vmem = pltpu.VMEM
    return pl.pallas_call(
        functools.partial(kernel, n_tp, n_ep),
        out_shape=(
            jax.ShapeDtypeStruct((rows, cols), BF16),
            jax.ShapeDtypeStruct((own, latent), BF16),
            jax.ShapeDtypeStruct((own, QK_ROPE), BF16),
        ),
        in_specs=[
            pl.BlockSpec(memory_space=spaces.get(i, pl.ANY)) for i in range(len(operands))
        ],
        out_specs=[pl.BlockSpec(memory_space=vmem)] * 3,
        scratch_shapes=[
            vmem(latent_cache.shape, BF16),
            vmem((own, QK_ROPE, context), BF16),
            vmem(query_weight.shape, BF16),
            vmem((QK_ROPE, width), BF16),
            vmem(latent_weight.shape, BF16),
            vmem((QK_ROPE, cols), BF16),
            vmem(absorb_weight.shape[1:], BF16),
            vmem(value_weight.shape[1:], BF16),
            vmem(output_weight.shape, BF16),
            vmem((ff_dev, width), BF16),
            vmem((ff_dev, width), BF16),
            vmem((ff_dev, width), BF16),
            vmem((rows, width), F32),
            vmem((rows, width), BF16),
            vmem((rows, MESSAGE), F32),
            vmem((rows, latent), F32),
            vmem((all_slots, cols), F32),
            vmem((n_tp, own, width), BF16),
            vmem((n_tp, own, MESSAGE), BF16),
            vmem((n_tp, own, MESSAGE), BF16),
            vmem((n_tp, own, latent), BF16),
            vmem((n_tp, own, latent), BF16),
            vmem((n_tp, rows, cols), BF16),
            vmem((n_tp, rows, cols), BF16),
            vmem((n_tp, 1, 4 * rows), F32),
            vmem((n_ep, slots, cols), BF16),
            vmem((n_ep, slots, cols), BF16),
            vmem((n_tp, out_rows, 2 * ff), BF16),
            vmem((n_tp, out_rows, 2 * ff), BF16),
            vmem((n_tp, out_rows, ff), BF16),
            vmem((n_ep, slots, cols), BF16),
            vmem((n_ep, slots, cols), BF16),
            vmem((n_tp, ff_dev, cols), BF16),
            vmem((n_tp, ff_dev, cols), BF16),
            vmem((n_tp, ff_dev, cols), BF16),
            pltpu.SemaphoreType.DMA((13,)),
            pltpu.SemaphoreType.DMA((12,)),
            pltpu.SemaphoreType.DMA((12,)),
        ],
        compiler_params=pltpu.CompilerParams(
            collective_id=0, has_side_effects=True, vmem_limit_bytes=48 * 1024 * 1024
        ),
    )(*operands)


def solution(mesh):
    placed = (
        P(("ep", "tp"), None),
        P("ep"),
        P(("ep", "tp"), None, None),
        P(("ep", "tp"), None, None),
        P(),
        P(None, "tp"),
        P(None, "tp"),
        P("tp", None),
        P("tp", None),
        P(),
        P("tp", None, None),
        P("tp", None, None),
        P("tp", None),
        P(),
        P(),
        P("ep", None, "tp"),
        P("ep", None, "tp"),
        P("ep", "tp", None),
        P("ep", None),
        P("ep", None),
    )
    return jax.shard_map(
        per_device,
        mesh=mesh,
        in_specs=placed,
        out_specs=(P("ep", "tp"), P(("ep", "tp"), None), P(("ep", "tp"), None)),
        check_vma=False,
    )
```

```python
import functools

import jax
import jax.numpy as jnp
import numpy as np
from jax import lax
from jax.experimental import pallas as pl
from jax.experimental.pallas import tpu as pltpu
from jax.sharding import PartitionSpec as P

MESH = pl.DeviceIdType.MESH
F32 = jnp.float32
BF16 = jnp.bfloat16
HIGHEST = lax.Precision.HIGHEST

QK_NOPE = 128
QK_ROPE = 64
norm_floor = 1e-06
rope_base = 10000.0
masked_score = -1e30

LAT_AT, KEY_AT, ROT_AT, KEY_ROT_AT, MESSAGE = 0, 256, 512, 640, 768


def dot(a, b, precision=None):
    return lax.dot_general(
        a, b, (((1,), (0,)), ((), ())), preferred_element_type=F32, precision=precision
    )


def dot_t(a, b, precision=None):
    return lax.dot_general(
        a, b, (((1,), (1,)), ((), ())), preferred_element_type=F32, precision=precision
    )


def swap_halves(x):
    half = x.shape[-1] // 2
    return jnp.concatenate([x[:, half:], x[:, :half]], axis=1)


def gain_row(ref, first, size):
    return ref[pl.ds(first, size)].astype(F32).reshape(1, size)


def cos_sin(x):
    return jnp.cos(x), jnp.sin(x)


def iota(shape, dim):
    return lax.broadcasted_iota(jnp.int32, shape, dim)


def kernel(
    n_tp,
    n_ep,
    tokens,
    lengths,
    latent_cache,
    rope_cache,
    attn_gain,
    mix_gain,
    expert_gain,
    latent_gain,
    query_weight,
    query_rot_weight,
    latent_weight,
    key_rot_weight,
    absorb_weight,
    value_weight,
    output_weight,
    gate_weight,
    up_weight,
    down_weight,
    expert_ids,
    route_weights,
    out,
    new_latent,
    new_rope,
    len_v,
    ids_v,
    rw_v,
    attn_v,
    mixg_v,
    expg_v,
    latg_v,
    lat_v,
    rope_v,
    qw_v,
    qrw_v,
    lw_v,
    krw_v,
    abs_v,
    val_v,
    ow_v,
    gate_v,
    up_v,
    down_v,
    tok_f,
    normed_b,
    msg_f,
    lat_f,
    route_f,
    tok_in,
    qry_out,
    qry_in,
    att_out,
    att_in,
    mix_out,
    mix_in,
    sum_in,
    dis_out,
    dis_in,
    part_out,
    part_in,
    hid_in,
    ret_out,
    ret_in,
    gate_in,
    up_in,
    down_in,
    local_sems,
    send_sems,
    recv_sems,
):
    me = lax.axis_index("tp")
    group = lax.axis_index("ep")
    rows = tok_f.shape[0]
    own = rows // n_tp
    width = tok_f.shape[1]
    cols = width // n_tp
    slots = dis_out.shape[1]
    ff_dev = gate_v.shape[0]
    latent = abs_v.shape[1]
    my_first = pl.multiple_of(me * cols, cols)
    my_cols = pl.ds(my_first, cols)

    def load(index, src, dst):
        copy = pltpu.make_async_copy(src, dst, local_sems.at[index])
        copy.start()
        return copy

    tok_copy = load(0, tokens, tok_in.at[me])
    small = [
        load(13, lengths, len_v),
        load(14, expert_ids, ids_v),
        load(15, route_weights, rw_v),
        load(16, attn_gain, attn_v),
        load(17, mix_gain, mixg_v),
        load(18, expert_gain, expg_v),
        load(19, latent_gain, latg_v),
    ]
    qw_copy = load(1, query_weight, qw_v)
    qrw_copy = load(2, query_rot_weight, qrw_v)
    lw_copy = load(3, latent_weight, lw_v)
    krw_copy = load(4, key_rot_weight, krw_v)
    abs_copy = load(5, absorb_weight.at[0], abs_v)
    gate_copy = load(6, gate_weight.at[0], gate_v)
    up_copy = load(7, up_weight.at[0], up_v)
    lat_copy = load(8, latent_cache, lat_v)
    rope_copy = load(9, rope_cache, rope_v)
    val_copy = load(10, value_weight.at[0], val_v)
    ow_copy = load(11, output_weight, ow_v)
    down_copy = load(12, down_weight.at[0], down_v)

    barrier = pltpu.get_barrier_semaphore()

    def greet_tp(d, _):
        pl.semaphore_signal(
            barrier, inc=1, device_id={"tp": lax.rem(me + d, n_tp)}, device_id_type=MESH
        )
        return 0

    def greet_ep(d, _):
        pl.semaphore_signal(
            barrier, inc=1, device_id={"ep": lax.rem(group + d, n_ep)}, device_id_type=MESH
        )
        return 0

    lax.fori_loop(1, n_ep, greet_ep, 0)
    lax.fori_loop(1, n_tp, greet_tp, 0)
    pl.semaphore_wait(barrier, n_tp - 1 + n_ep - 1)

    order = sorted(range(1, n_tp), key=lambda d: -min(d, n_tp - d))

    def send(src, dst, stage, device):
        pltpu.make_async_remote_copy(
            src_ref=src,
            dst_ref=dst,
            send_sem=send_sems.at[stage],
            recv_sem=recv_sems.at[stage],
            device_id=device,
            device_id_type=MESH,
        ).start()

    def send_tp(stage, src_of, dst, before=None):
        for d in order:
            peer = lax.rem(me + d, n_tp)
            send(src_of(peer), dst, stage, {"tp": peer})

    def send_ep(stage, src_of, dst):
        def step(d, _):
            peer = lax.rem(group + d, n_ep)
            send(src_of(peer), dst, stage, {"ep": peer})
            return 0

        lax.fori_loop(1, n_ep, step, 0)

    def arrived(stage, buffer):
        some = buffer.at[pl.ds(0, buffer.shape[0] - 1)]
        pltpu.make_async_copy(some, some, recv_sems.at[stage]).wait()

    def sent(stage, buffer):
        some = buffer.at[pl.ds(0, buffer.shape[0] - 1)]
        pltpu.make_async_copy(some, some, send_sems.at[stage]).wait()

    tok_copy.wait()
    send_tp(0, lambda peer: tok_in.at[me], tok_in.at[me])

    square = (rows, rows)
    eye = (iota(square, 0) == iota(square, 1)).astype(F32)
    ahead_row = iota(square, 0) < iota(square, 1)
    ahead_col = iota(square, 1) < iota(square, 0)
    for copy in small:
        copy.wait()
    ids = ids_v[...].astype(F32)
    weights_row = rw_v[...]
    id_rows = [ids[k : k + 1, :] for k in range(2)]
    id_cols = [jnp.sum(eye * r, axis=1, keepdims=True) for r in id_rows]
    weight_cols = [
        jnp.sum(eye * weights_row[k : k + 1, :], axis=1, keepdims=True) for k in range(2)
    ]

    def same(j, k):
        return id_cols[j] == id_rows[k]

    def count(mask, axis):
        return jnp.sum(jnp.where(mask, 1.0, 0.0), axis=axis, keepdims=True)

    rank_row0 = count(same(0, 0) & ahead_row, 0)
    rank_row1 = count(same(0, 1), 0) + count(same(1, 1) & ahead_row, 0)
    rank_col0 = count(same(0, 0) & ahead_col, 1)
    rank_col1 = count(same(1, 0), 1) + count(same(1, 1) & ahead_col, 1)
    target_rows = [id_rows[0] * slots + rank_row0, id_rows[1] * slots + rank_row1]
    target_cols = [id_cols[0] * slots + rank_col0, id_cols[1] * slots + rank_col1]
    all_slots = n_ep * slots
    down_iota = iota((all_slots, rows), 0).astype(F32)
    across_iota = iota((rows, all_slots), 1).astype(F32)
    dispatch = (
        jnp.where(down_iota == target_rows[0], 1.0, 0.0)
        + jnp.where(down_iota == target_rows[1], 1.0, 0.0)
    ).astype(BF16)
    combine = jnp.where(across_iota == target_cols[0], weight_cols[0], 0.0) + jnp.where(
        across_iota == target_cols[1], weight_cols[1], 0.0
    )

    half = QK_ROPE // 2
    freqs = jnp.zeros((1, QK_ROPE), F32)
    lane = lax.rem(iota((1, QK_ROPE), 1), half)
    for i in range(half):
        freqs = jnp.where(lane == i, float(np.float32(rope_base ** (-i / half))), freqs)
    lengths_row = len_v[...].astype(F32)
    lengths_col = jnp.sum(eye * lengths_row, axis=1, keepdims=True)
    cosine, sine = cos_sin(lengths_col * freqs)
    sine = jnp.where(iota((1, QK_ROPE), 1) < half, -sine, sine)
    own_rows = (iota((8, rows), 1) == own * me + iota((8, rows), 0)).astype(F32)
    own_cosine = dot(own_rows, cosine, HIGHEST)[:own]
    own_sine = dot(own_rows, sine, HIGHEST)[:own]
    own_lengths = jnp.sum(own_rows * lengths_row, axis=1, keepdims=True).astype(jnp.int32)

    arrived(0, tok_in)
    for t in range(n_tp):
        tok_f[own * t : own * (t + 1), :] = tok_in[t].astype(F32)
    chunk = 512
    square_sum = jnp.zeros((rows, 1), F32)
    for c in range(0, width, chunk):
        x = tok_f[:, c : c + chunk]
        square_sum = square_sum + jnp.sum(x * x, axis=1, keepdims=True)
    factor = lax.rsqrt(square_sum / width + norm_floor)
    for c in range(0, width, chunk):
        x = tok_f[:, c : c + chunk]
        normed_b[:, c : c + chunk] = (x * factor * gain_row(attn_v, c, chunk)).astype(BF16)

    qw_copy.wait()
    q_nope = dot(normed_b[...], qw_v[...]).astype(BF16)
    abs_copy.wait()
    msg_f[:, LAT_AT : LAT_AT + latent] = dot(q_nope, abs_v[...])
    qrw_copy.wait()
    q_rot = dot_t(normed_b[...], qrw_v[...])
    msg_f[:, ROT_AT : ROT_AT + QK_ROPE] = q_rot * cosine + swap_halves(q_rot) * sine
    slice_rows = normed_b[:, my_cols]
    lw_copy.wait()
    msg_f[:, KEY_AT : KEY_AT + latent] = dot(slice_rows, lw_v[...])
    krw_copy.wait()
    msg_f[:, KEY_ROT_AT : KEY_ROT_AT + QK_ROPE] = dot_t(slice_rows, krw_v[...])
    for t in range(n_tp):
        qry_out[t] = msg_f[own * t : own * (t + 1), :].astype(BF16)

    send_tp(1, lambda peer: qry_out.at[peer], qry_in.at[me])
    qry_in[me] = qry_out[me]
    gate_copy.wait()

    def piece(ref, peer):
        return ref.at[:, pl.ds(pl.multiple_of(peer * cols, cols), cols)]

    send_tp(2, lambda peer: piece(gate_v, peer), gate_in.at[me])
    gate_in[me] = gate_v[:, my_cols]

    lat_copy.wait()
    rope_copy.wait()

    arrived(1, qry_in)
    key_sum = jnp.zeros((own, MESSAGE), F32)
    for h in range(n_tp):
        part = qry_in[h].astype(F32)
        key_sum = key_sum + part
        msg_f[own * h : own * (h + 1), :] = part
    key_raw = key_sum[:, KEY_AT : KEY_AT + latent]
    key_factor = lax.rsqrt(jnp.mean(key_raw * key_raw, axis=1, keepdims=True) + norm_floor)
    own_lat = (key_raw * key_factor * gain_row(latg_v, 0, latent)).astype(BF16)
    rope_raw = key_sum[:, KEY_ROT_AT : KEY_ROT_AT + QK_ROPE]
    own_rot = (rope_raw * own_cosine + swap_halves(rope_raw) * own_sine).astype(BF16)
    new_latent[...] = own_lat
    new_rope[...] = own_rot
    own_lat = own_lat.astype(F32)
    own_rot = own_rot.astype(F32)

    scale = (QK_NOPE + QK_ROPE) ** (-0.5)
    queries = msg_f[:, LAT_AT : LAT_AT + latent]
    rotated = msg_f[:, ROT_AT : ROT_AT + QK_ROPE]
    queries_b = queries.astype(BF16)
    rotated_b = rotated.astype(BF16)
    context = lat_v.shape[1]
    row_col = iota((rows, 1), 0)
    first = lax.rem(row_col, own) == 0

    def of_row(a, b):
        return jnp.where(first, a, b)

    scores = of_row(
        dot_t(queries_b, lat_v[0]) + dot(rotated_b, rope_v[0]),
        dot_t(queries_b, lat_v[1]) + dot(rotated_b, rope_v[1]),
    )
    row_len = of_row(own_lengths[0:1], own_lengths[1:2])
    valid = iota((rows, context), 1) < row_len
    scores = jnp.where(valid, scores * scale, masked_score)
    lat_rows = of_row(own_lat[0:1], own_lat[1:2])
    rot_rows = of_row(own_rot[0:1], own_rot[1:2])
    own_score = (
        jnp.sum(queries * lat_rows, axis=1, keepdims=True)
        + jnp.sum(rotated * rot_rows, axis=1, keepdims=True)
    ) * scale
    top = jnp.maximum(jnp.max(scores, axis=1, keepdims=True), own_score)
    weights = jnp.where(valid, jnp.exp(scores - top), 0.0)
    own_weight = jnp.exp(own_score - top)
    total = jnp.sum(weights, axis=1, keepdims=True) + own_weight
    summed = (
        dot(jnp.where(first, weights, 0.0).astype(BF16), lat_v[0])
        + dot(jnp.where(first, 0.0, weights).astype(BF16), lat_v[1])
        + own_weight.astype(BF16).astype(F32) * lat_rows
    )
    lat_f[...] = summed / total
    for h in range(n_tp):
        att_out[h] = lat_f[own * h : own * (h + 1), :].astype(BF16)

    send_tp(3, lambda peer: att_out.at[peer], att_in.at[me])
    att_in[me] = att_out[me]
    up_copy.wait()
    send_tp(4, lambda peer: piece(up_v, peer), up_in.at[me])
    up_in[me] = up_v[:, my_cols]
    val_copy.wait()
    ow_copy.wait()

    arrived(3, att_in)
    for t in range(n_tp):
        lat_f[own * t : own * (t + 1), :] = att_in[t].astype(F32)
    head_values = dot(lat_f[...].astype(BF16), val_v[...]).astype(BF16)

    for d in order + [0]:
        peer = lax.rem(me + d, n_tp)
        share = dot(
            head_values, ow_v[:, pl.ds(pl.multiple_of(peer * cols, cols), cols)]
        ).astype(BF16)
        if d:
            mix_out[peer] = share
            send(mix_out.at[peer], mix_in.at[me], 5, {"tp": peer})
        else:
            mix_in[me] = share

    tok_cols = tok_f[:, my_cols]
    my_mix_gain = gain_row(mixg_v, my_first, cols)
    my_expert_gain = gain_row(expg_v, my_first, cols)

    arrived(5, mix_in)
    mixed = mix_in[0].astype(F32)
    for t in range(1, n_tp):
        mixed = mixed + mix_in[t].astype(F32)
    mixed = mixed.astype(BF16).astype(F32)
    scaled = mixed * my_mix_gain

    def as_row(col):
        return jnp.sum(eye * col, axis=0, keepdims=True)

    def as_col(row):
        return jnp.sum(eye * row, axis=1, keepdims=True)

    def row_sum(value):
        return as_row(jnp.sum(value, axis=1, keepdims=True))

    sums = jnp.concatenate(
        [
            row_sum(mixed * mixed),
            row_sum(tok_cols * scaled),
            row_sum(scaled * scaled),
            jnp.zeros((1, rows), F32),
        ],
        axis=1,
    )
    sum_in[me] = sums
    send_tp(6, lambda peer: sum_in.at[me], sum_in.at[me])
    arrived(6, sum_in)
    sums = sum_in[0]
    for t in range(1, n_tp):
        sums = sums + sum_in[t]
    mix_square = as_col(sums[:, 0:rows])
    cross = as_col(sums[:, rows : 2 * rows])
    scaled_square = as_col(sums[:, 2 * rows : 3 * rows])
    mix_factor = lax.rsqrt(mix_square / width + norm_floor)
    resid = (tok_cols + scaled * mix_factor).astype(BF16).astype(F32)
    resid_square = square_sum + mix_factor * (2.0 * cross + mix_factor * scaled_square)
    resid_factor = lax.rsqrt(jnp.maximum(resid_square, 0.0) / width + norm_floor)
    expert_in = (resid * resid_factor * my_expert_gain).astype(BF16)

    route_f[...] = dot(dispatch, expert_in)
    for e in range(n_ep):
        dis_out[e] = route_f[slots * e : slots * (e + 1), :].astype(BF16)
    send_ep(7, lambda peer: dis_out.at[peer], dis_in.at[group])
    dis_in[group] = dis_out[group]
    down_copy.wait()
    send_tp(8, lambda peer: piece(down_v, peer), down_in.at[me])
    down_in[me] = down_v[:, my_cols]

    arrived(2, gate_in)
    arrived(4, up_in)
    arrived(7, dis_in)
    for g in range(n_ep):
        route_f[slots * g : slots * (g + 1), :] = dis_in[g].astype(F32)
    received = route_f[...].astype(BF16)
    ff = n_tp * ff_dev
    out_rows = all_slots // n_tp
    for n, source in enumerate((gate_in, up_in)):
        part = dot_t(received, source[...].reshape(ff, cols))
        part_out[:, :, n * ff : (n + 1) * ff] = part.reshape(n_tp, out_rows, ff).astype(BF16)

    send_tp(9, lambda peer: part_out.at[peer], part_in.at[me])
    part_in[me] = part_out[me]
    arrived(9, part_in)
    both = part_in[0].astype(F32)
    for t in range(1, n_tp):
        both = both + part_in[t].astype(F32)
    gate, upward = both[:, :ff], both[:, ff:]
    hid_in[me] = (gate / (1.0 + jnp.exp(-gate)) * upward).astype(BF16)

    send_tp(10, lambda peer: hid_in.at[me], hid_in.at[me])
    arrived(8, down_in)
    arrived(10, hid_in)
    hidden = hid_in[...].astype(F32).reshape(all_slots, ff).astype(BF16)
    route_f[...] = dot(hidden, down_in[...].reshape(ff, cols))
    for g in range(n_ep):
        ret_out[g] = route_f[slots * g : slots * (g + 1), :].astype(BF16)

    send_ep(11, lambda peer: ret_out.at[peer], ret_in.at[group])
    ret_in[group] = ret_out[group]
    arrived(11, ret_in)
    for e in range(n_ep):
        route_f[slots * e : slots * (e + 1), :] = ret_in[e].astype(F32)
    out[...] = (resid + dot(combine, route_f[...], HIGHEST)).astype(BF16)

    for stage, buffer in (
        (0, tok_in),
        (1, qry_in),
        (2, gate_in),
        (3, att_in),
        (4, up_in),
        (5, mix_in),
        (6, sum_in),
        (7, dis_in),
        (8, down_in),
        (9, part_in),
        (10, hid_in),
        (11, ret_in),
    ):
        sent(stage, buffer)


def per_device(
    tokens,
    lengths,
    latent_cache,
    rope_cache,
    attn_gain,
    query_weight,
    query_rot_weight,
    latent_weight,
    key_rot_weight,
    latent_gain,
    absorb_weight,
    value_weight,
    output_weight,
    mix_gain,
    expert_gain,
    gate_weight,
    up_weight,
    down_weight,
    expert_ids,
    route_weights,
):
    n_tp, n_ep = lax.axis_size("tp"), lax.axis_size("ep")
    own, width = tokens.shape
    rows = own * n_tp
    cols = width // n_tp
    latent = latent_weight.shape[1]
    context = latent_cache.shape[1]
    ff_dev = gate_weight.shape[2]
    ff = ff_dev * n_tp
    slots = 2 * rows * expert_ids.shape[1] // n_ep
    all_slots = n_ep * slots
    out_rows = all_slots // n_tp

    operands = (
        tokens,
        lengths.reshape(1, rows),
        latent_cache,
        jnp.swapaxes(rope_cache, 1, 2),
        attn_gain,
        mix_gain,
        expert_gain,
        latent_gain,
        query_weight,
        query_rot_weight.T,
        latent_weight,
        key_rot_weight.T,
        absorb_weight,
        value_weight,
        output_weight,
        jnp.swapaxes(gate_weight, 1, 2),
        jnp.swapaxes(up_weight, 1, 2),
        down_weight,
        expert_ids.T,
        route_weights.T,
    )
    vmem = pltpu.VMEM
    return pl.pallas_call(
        functools.partial(kernel, n_tp, n_ep),
        out_shape=(
            jax.ShapeDtypeStruct((rows, cols), BF16),
            jax.ShapeDtypeStruct((own, latent), BF16),
            jax.ShapeDtypeStruct((own, QK_ROPE), BF16),
        ),
        in_specs=[
            pl.BlockSpec(memory_space=pl.ANY) for _ in operands
        ],
        out_specs=[pl.BlockSpec(memory_space=vmem)] * 3,
        scratch_shapes=[
            vmem((1, rows), jnp.int32),
            vmem(expert_ids.shape[::-1], jnp.int32),
            vmem(route_weights.shape[::-1], F32),
            vmem((width,), BF16),
            vmem((width,), BF16),
            vmem((width,), BF16),
            vmem((latent,), BF16),
            vmem(latent_cache.shape, BF16),
            vmem((own, QK_ROPE, context), BF16),
            vmem(query_weight.shape, BF16),
            vmem((QK_ROPE, width), BF16),
            vmem(latent_weight.shape, BF16),
            vmem((QK_ROPE, cols), BF16),
            vmem(absorb_weight.shape[1:], BF16),
            vmem(value_weight.shape[1:], BF16),
            vmem(output_weight.shape, BF16),
            vmem((ff_dev, width), BF16),
            vmem((ff_dev, width), BF16),
            vmem((ff_dev, width), BF16),
            vmem((rows, width), F32),
            vmem((rows, width), BF16),
            vmem((rows, MESSAGE), F32),
            vmem((rows, latent), F32),
            vmem((all_slots, cols), F32),
            vmem((n_tp, own, width), BF16),
            vmem((n_tp, own, MESSAGE), BF16),
            vmem((n_tp, own, MESSAGE), BF16),
            vmem((n_tp, own, latent), BF16),
            vmem((n_tp, own, latent), BF16),
            vmem((n_tp, rows, cols), BF16),
            vmem((n_tp, rows, cols), BF16),
            vmem((n_tp, 1, 4 * rows), F32),
            vmem((n_ep, slots, cols), BF16),
            vmem((n_ep, slots, cols), BF16),
            vmem((n_tp, out_rows, 2 * ff), BF16),
            vmem((n_tp, out_rows, 2 * ff), BF16),
            vmem((n_tp, out_rows, ff), BF16),
            vmem((n_ep, slots, cols), BF16),
            vmem((n_ep, slots, cols), BF16),
            vmem((n_tp, ff_dev, cols), BF16),
            vmem((n_tp, ff_dev, cols), BF16),
            vmem((n_tp, ff_dev, cols), BF16),
            pltpu.SemaphoreType.DMA((20,)),
            pltpu.SemaphoreType.DMA((12,)),
            pltpu.SemaphoreType.DMA((12,)),
        ],
        compiler_params=pltpu.CompilerParams(
            collective_id=0, has_side_effects=True, vmem_limit_bytes=67_043_328
        ),
    )(*operands)


def solution(mesh):
    placed = (
        P(("ep", "tp"), None),
        P("ep"),
        P(("ep", "tp"), None, None),
        P(("ep", "tp"), None, None),
        P(),
        P(None, "tp"),
        P(None, "tp"),
        P("tp", None),
        P("tp", None),
        P(),
        P("tp", None, None),
        P("tp", None, None),
        P("tp", None),
        P(),
        P(),
        P("ep", None, "tp"),
        P("ep", None, "tp"),
        P("ep", "tp", None),
        P("ep", None),
        P("ep", None),
    )
    return jax.shard_map(
        per_device,
        mesh=mesh,
        in_specs=placed,
        out_specs=(P("ep", "tp"), P(("ep", "tp"), None), P(("ep", "tp"), None)),
        check_vma=False,
    )
```

```python
import functools

import jax
import jax.numpy as jnp
import numpy as np
from jax import lax
from jax.experimental import pallas as pl
from jax.experimental.pallas import tpu as pltpu
from jax.sharding import PartitionSpec as P

MESH = pl.DeviceIdType.MESH
F32 = jnp.float32
BF16 = jnp.bfloat16
HIGHEST = lax.Precision.HIGHEST

QK_NOPE = 128
QK_ROPE = 64
norm_floor = 1e-06
rope_base = 10000.0
masked_score = -1e30

LAT_AT, KEY_AT, ROT_AT, KEY_ROT_AT, MESSAGE = 0, 256, 512, 640, 768


def dot(a, b, precision=None):
    return lax.dot_general(
        a, b, (((1,), (0,)), ((), ())), preferred_element_type=F32, precision=precision
    )


def dot_t(a, b, precision=None):
    return lax.dot_general(
        a, b, (((1,), (1,)), ((), ())), preferred_element_type=F32, precision=precision
    )


def swap_halves(x):
    half = x.shape[-1] // 2
    return jnp.concatenate([x[:, half:], x[:, :half]], axis=1)


def gain_row(ref, first, size):
    return ref[pl.ds(first, size)].astype(F32).reshape(1, size)


def cos_sin(x):
    return jnp.cos(x), jnp.sin(x)


def iota(shape, dim):
    return lax.broadcasted_iota(jnp.int32, shape, dim)


def kernel(
    n_tp,
    n_ep,
    tokens,
    lengths,
    latent_cache,
    rope_cache,
    attn_gain,
    mix_gain,
    expert_gain,
    latent_gain,
    query_weight,
    query_rot_weight,
    latent_weight,
    key_rot_weight,
    absorb_weight,
    value_weight,
    output_weight,
    gate_weight,
    up_weight,
    down_weight,
    expert_ids,
    route_weights,
    out,
    new_latent,
    new_rope,
    len_v,
    ids_v,
    rw_v,
    attn_v,
    mixg_v,
    expg_v,
    latg_v,
    lat_v,
    rope_v,
    qw_v,
    qrw_v,
    lw_v,
    krw_v,
    abs_v,
    val_pair,
    ow_pair,
    gate_v,
    up_v,
    down_v,
    tok_f,
    normed_b,
    msg_f,
    lat_f,
    route_f,
    tok_in,
    qry_out,
    qry_in,
    att_out,
    att_in,
    mix_out,
    mix_in,
    sum_in,
    dis_out,
    dis_in,
    part_out,
    part_in,
    hid_in,
    ret_out,
    ret_in,
    gate_in,
    up_in,
    down_in,
    local_sems,
    send_sems,
    recv_sems,
    tok_sems,
):
    me = lax.axis_index("tp")
    group = lax.axis_index("ep")
    rows = tok_f.shape[0]
    own = rows // n_tp
    width = tok_f.shape[1]
    cols = width // n_tp
    slots = dis_out.shape[1]
    ff_dev = gate_v.shape[0]
    latent = abs_v.shape[1]
    my_first = pl.multiple_of(me * cols, cols)
    my_cols = pl.ds(my_first, cols)
    n_chip = n_tp // 2
    half_ep = n_ep // 2
    chip = me // 2
    core = lax.rem(me, 2)
    sibling = me + 1 - 2 * core
    side = lax.rem(group, 2)
    at_home = side == core

    def load(index, src, dst):
        copy = pltpu.make_async_copy(src, dst, local_sems.at[index])
        copy.start()
        return copy

    tok_copy = load(0, tokens, tok_in.at[me])

    barrier = pltpu.get_barrier_semaphore()

    def greet(device):
        pl.semaphore_signal(barrier, inc=1, device_id=device, device_id_type=MESH)

    for d in range(1, n_tp):
        greet({"tp": lax.rem(me + d, n_tp)})

    def greet_ep(d, _):
        greet({"ep": lax.rem(group + d, n_ep), "tp": 2 * chip + side})
        return 0

    lax.fori_loop(1, n_ep, greet_ep, 0)

    @pl.when(jnp.logical_not(at_home))
    def _():
        greet({"tp": sibling})

    def greet_back(d, _):
        greet({"ep": 2 * d + core, "tp": 2 * chip + 1 - side})
        return 0

    lax.fori_loop(0, half_ep, greet_back, 0)

    small = [
        load(13, lengths, len_v),
        load(14, expert_ids, ids_v),
        load(15, route_weights, rw_v),
        load(16, attn_gain, attn_v),
        load(17, mix_gain, mixg_v),
        load(18, expert_gain, expg_v),
        load(19, latent_gain, latg_v),
    ]
    qw_copy = load(1, query_weight, qw_v)
    qrw_copy = load(2, query_rot_weight, qrw_v)
    lw_copy = load(3, latent_weight, lw_v)
    krw_copy = load(4, key_rot_weight, krw_v)
    abs_copy = load(5, absorb_weight.at[0], abs_v)
    gate_copy = load(6, gate_weight.at[0], gate_v)
    up_copy = load(7, up_weight.at[0], up_v)
    lat_copy = load(8, latent_cache, lat_v)
    rope_copy = load(9, rope_cache, rope_v)
    val_copy = load(10, value_weight.at[0], val_pair.at[core])
    value_dim = value_weight.shape[2]
    head_rows = pl.ds(pl.multiple_of(core * value_dim, value_dim), value_dim)

    def block(index):
        return pl.ds(pl.multiple_of(index * cols, cols), cols)

    for y in range(n_chip):
        pltpu.make_async_copy(
            output_weight.at[:, block(2 * y + core)],
            ow_pair.at[y, head_rows],
            local_sems.at[11],
        ).start()
    down_copy = load(12, down_weight.at[0], down_v)

    pl.semaphore_wait(
        barrier, n_tp - 1 + n_ep + half_ep - jnp.where(at_home, 1, 0)
    )

    order = sorted(range(1, n_tp), key=lambda d: -min(d, n_tp - d))
    chip_order = sorted(range(1, n_chip), key=lambda d: -min(d, n_chip - d))

    def send(src, dst, stage, device, recv_sem=None):
        pltpu.make_async_remote_copy(
            src_ref=src,
            dst_ref=dst,
            send_sem=send_sems.at[stage],
            recv_sem=recv_sems.at[stage] if recv_sem is None else recv_sem,
            device_id=device,
            device_id_type=MESH,
        ).start()

    def send_tp(stage, src_of, dst):
        for d in order:
            peer = lax.rem(me + d, n_tp)
            send(src_of(peer), dst(peer) if callable(dst) else dst, stage, {"tp": peer})

    def send_chips(stage, src_of, dst):
        for d in chip_order:
            peer = lax.rem(chip + d, n_chip)
            send(src_of(peer), dst, stage, {"tp": 2 * peer + core})

    def wait_for(sem, buffer, count):
        some = buffer.at[pl.ds(0, count)]
        pltpu.make_async_copy(some, some, sem).wait()

    def arrived(stage, buffer, count=None):
        wait_for(recv_sems.at[stage], buffer, buffer.shape[0] - 1 if count is None else count)

    def sent(stage, buffer, count=None):
        wait_for(send_sems.at[stage], buffer, buffer.shape[0] - 1 if count is None else count)

    def arrived_all(stage, buffer):
        pltpu.make_async_copy(buffer, buffer, recv_sems.at[stage]).wait()

    def sent_all(stage, buffer):
        pltpu.make_async_copy(buffer, buffer, send_sems.at[stage]).wait()

    def at_home_or_not(stage, buffer, sems):
        count = buffer.shape[0]

        @pl.when(at_home)
        def _():
            wait_for(sems.at[stage], buffer, count - 1)

        @pl.when(jnp.logical_not(at_home))
        def _():
            wait_for(sems.at[stage], buffer, count)

    tok_copy.wait()
    send(tok_in.at[me], tok_in.at[me], 0, {"tp": sibling}, recv_sems.at[12])
    for d in chip_order:
        peer = lax.rem(chip + d, n_chip)
        send(tok_in.at[me], tok_in.at[me], 0, {"tp": 2 * peer + core}, tok_sems.at[chip])

    square = (rows, rows)
    eye = (iota(square, 0) == iota(square, 1)).astype(F32)
    ahead_row = iota(square, 0) < iota(square, 1)
    ahead_col = iota(square, 1) < iota(square, 0)
    for copy in small:
        copy.wait()
    ids = ids_v[...].astype(F32)
    weights_row = rw_v[...]
    id_rows = [ids[k : k + 1, :] for k in range(2)]
    id_cols = [jnp.sum(eye * r, axis=1, keepdims=True) for r in id_rows]
    weight_cols = [
        jnp.sum(eye * weights_row[k : k + 1, :], axis=1, keepdims=True) for k in range(2)
    ]

    def same(j, k):
        return id_cols[j] == id_rows[k]

    def count(mask, axis):
        return jnp.sum(jnp.where(mask, 1.0, 0.0), axis=axis, keepdims=True)

    rank_row0 = count(same(0, 0) & ahead_row, 0)
    rank_row1 = count(same(0, 1), 0) + count(same(1, 1) & ahead_row, 0)
    rank_col0 = count(same(0, 0) & ahead_col, 1)
    rank_col1 = count(same(1, 0), 1) + count(same(1, 1) & ahead_col, 1)
    target_rows = [id_rows[0] * slots + rank_row0, id_rows[1] * slots + rank_row1]
    target_cols = [id_cols[0] * slots + rank_col0, id_cols[1] * slots + rank_col1]
    all_slots = n_ep * slots
    down_iota = iota((all_slots, rows), 0).astype(F32)
    across_iota = iota((rows, all_slots), 1).astype(F32)
    dispatch = (
        jnp.where(down_iota == target_rows[0], 1.0, 0.0)
        + jnp.where(down_iota == target_rows[1], 1.0, 0.0)
    ).astype(BF16)
    combine = jnp.where(across_iota == target_cols[0], weight_cols[0], 0.0) + jnp.where(
        across_iota == target_cols[1], weight_cols[1], 0.0
    )

    half = QK_ROPE // 2
    freqs = jnp.zeros((1, QK_ROPE), F32)
    lane = lax.rem(iota((1, QK_ROPE), 1), half)
    for i in range(half):
        freqs = jnp.where(lane == i, float(np.float32(rope_base ** (-i / half))), freqs)
    lengths_row = len_v[...].astype(F32)
    lengths_col = jnp.sum(eye * lengths_row, axis=1, keepdims=True)
    cosine, sine = cos_sin(lengths_col * freqs)
    sine = jnp.where(iota((1, QK_ROPE), 1) < half, -sine, sine)
    own_rows = (iota((8, rows), 1) == own * me + iota((8, rows), 0)).astype(F32)
    own_cosine = dot(own_rows, cosine, HIGHEST)[:own]
    own_sine = dot(own_rows, sine, HIGHEST)[:own]
    own_lengths = jnp.sum(own_rows * lengths_row, axis=1, keepdims=True).astype(jnp.int32)

    for d in reversed(chip_order):
        peer = lax.rem(chip + d, n_chip)
        slot = tok_in.at[2 * peer + core]
        pltpu.make_async_copy(slot, slot, tok_sems.at[peer]).wait()
        send(slot, slot, 0, {"tp": sibling}, recv_sems.at[12])
    arrived(12, tok_in, n_chip)
    for t in range(n_tp):
        tok_f[own * t : own * (t + 1), :] = tok_in[t].astype(F32)
    chunk = 512
    square_sum = jnp.zeros((rows, 1), F32)
    for c in range(0, width, chunk):
        x = tok_f[:, c : c + chunk]
        square_sum = square_sum + jnp.sum(x * x, axis=1, keepdims=True)
    factor = lax.rsqrt(square_sum / width + norm_floor)
    for c in range(0, width, chunk):
        x = tok_f[:, c : c + chunk]
        normed_b[:, c : c + chunk] = (x * factor * gain_row(attn_v, c, chunk)).astype(BF16)

    qw_copy.wait()
    q_nope = dot(normed_b[...], qw_v[...]).astype(BF16)
    abs_copy.wait()
    msg_f[:, LAT_AT : LAT_AT + latent] = dot(q_nope, abs_v[...])
    qrw_copy.wait()
    q_rot = dot_t(normed_b[...], qrw_v[...])
    msg_f[:, ROT_AT : ROT_AT + QK_ROPE] = q_rot * cosine + swap_halves(q_rot) * sine
    slice_rows = normed_b[:, my_cols]
    lw_copy.wait()
    msg_f[:, KEY_AT : KEY_AT + latent] = dot(slice_rows, lw_v[...])
    krw_copy.wait()
    msg_f[:, KEY_ROT_AT : KEY_ROT_AT + QK_ROPE] = dot_t(slice_rows, krw_v[...])
    for t in range(n_tp):
        qry_out[t] = msg_f[own * t : own * (t + 1), :].astype(BF16)

    send_tp(1, lambda peer: qry_out.at[peer], qry_in.at[me])
    qry_in[me] = qry_out[me]
    send(value_weight.at[0], val_pair.at[core], 16, {"tp": sibling})
    for y in range(n_chip):
        send(
            output_weight.at[:, block(2 * y + 1 - core)],
            ow_pair.at[y, head_rows],
            17,
            {"tp": sibling},
        )
    gate_copy.wait()

    def piece(ref, peer):
        return ref.at[:, pl.ds(pl.multiple_of(peer * cols, cols), cols)]

    def half_of(ref):
        return lambda peer: ref.at[lax.rem(peer, 2), me]

    send_tp(2, lambda peer: piece(gate_v, peer), half_of(gate_in))
    gate_in[core, me] = gate_v[:, my_cols]

    lat_copy.wait()
    rope_copy.wait()

    arrived(1, qry_in)
    key_sum = jnp.zeros((own, MESSAGE), F32)
    for h in range(n_tp):
        part = qry_in[h].astype(F32)
        key_sum = key_sum + part
        msg_f[own * h : own * (h + 1), :] = part
    key_raw = key_sum[:, KEY_AT : KEY_AT + latent]
    key_factor = lax.rsqrt(jnp.mean(key_raw * key_raw, axis=1, keepdims=True) + norm_floor)
    own_lat = (key_raw * key_factor * gain_row(latg_v, 0, latent)).astype(BF16)
    rope_raw = key_sum[:, KEY_ROT_AT : KEY_ROT_AT + QK_ROPE]
    own_rot = (rope_raw * own_cosine + swap_halves(rope_raw) * own_sine).astype(BF16)
    new_latent[...] = own_lat
    new_rope[...] = own_rot
    own_lat = own_lat.astype(F32)
    own_rot = own_rot.astype(F32)

    scale = (QK_NOPE + QK_ROPE) ** (-0.5)
    queries = msg_f[:, LAT_AT : LAT_AT + latent]
    rotated = msg_f[:, ROT_AT : ROT_AT + QK_ROPE]
    queries_b = queries.astype(BF16)
    rotated_b = rotated.astype(BF16)
    context = lat_v.shape[1]
    row_col = iota((rows, 1), 0)
    first = lax.rem(row_col, own) == 0

    def of_row(a, b):
        return jnp.where(first, a, b)

    scores = of_row(
        dot_t(queries_b, lat_v[0]) + dot(rotated_b, rope_v[0]),
        dot_t(queries_b, lat_v[1]) + dot(rotated_b, rope_v[1]),
    )
    row_len = of_row(own_lengths[0:1], own_lengths[1:2])
    valid = iota((rows, context), 1) < row_len
    scores = jnp.where(valid, scores * scale, masked_score)
    lat_rows = of_row(own_lat[0:1], own_lat[1:2])
    rot_rows = of_row(own_rot[0:1], own_rot[1:2])
    own_score = (
        jnp.sum(queries * lat_rows, axis=1, keepdims=True)
        + jnp.sum(rotated * rot_rows, axis=1, keepdims=True)
    ) * scale
    top = jnp.maximum(jnp.max(scores, axis=1, keepdims=True), own_score)
    weights = jnp.where(valid, jnp.exp(scores - top), 0.0)
    own_weight = jnp.exp(own_score - top)
    total = jnp.sum(weights, axis=1, keepdims=True) + own_weight
    summed = (
        dot(jnp.where(first, weights, 0.0).astype(BF16), lat_v[0])
        + dot(jnp.where(first, 0.0, weights).astype(BF16), lat_v[1])
        + own_weight.astype(BF16).astype(F32) * lat_rows
    )
    lat_f[...] = summed / total
    for y in range(n_chip):
        for c in range(2):
            at = own * (2 * y + c)
            att_out[y, :, c * latent : (c + 1) * latent] = lat_f[at : at + own, :].astype(BF16)

    send_tp(3, lambda peer: att_out.at[peer // 2], att_in.at[me])
    att_in[me] = att_out[chip]
    up_copy.wait()
    send_tp(4, lambda peer: piece(up_v, peer), half_of(up_in))
    up_in[core, me] = up_v[:, my_cols]
    val_copy.wait()
    pltpu.make_async_copy(
        ow_pair.at[:, head_rows], ow_pair.at[:, head_rows], local_sems.at[11]
    ).wait()
    arrived(16, val_pair)
    pltpu.make_async_copy(
        ow_pair.at[:, head_rows], ow_pair.at[:, head_rows], recv_sems.at[17]
    ).wait()

    arrived(3, att_in)
    for t in range(n_tp):
        msg_f[own * t : own * (t + 1), : 2 * latent] = att_in[t].astype(F32)
    results = msg_f[:, : 2 * latent].astype(BF16)
    head_values = jnp.concatenate(
        [dot(results[:, c * latent : (c + 1) * latent], val_pair[c]) for c in range(2)], axis=1
    ).astype(BF16)

    for d in chip_order + [0]:
        peer = lax.rem(chip + d, n_chip)
        share = dot(head_values, ow_pair[peer]).astype(BF16)
        if d:
            mix_out[peer] = share
            send(mix_out.at[peer], mix_in.at[chip], 5, {"tp": 2 * peer + core})
        else:
            mix_in[chip] = share

    arrived(2, gate_in.at[core])
    send(gate_in.at[core], gate_in.at[core], 13, {"tp": sibling})
    tok_cols = tok_f[:, my_cols]
    my_mix_gain = gain_row(mixg_v, my_first, cols)
    my_expert_gain = gain_row(expg_v, my_first, cols)

    arrived(5, mix_in)
    mixed = mix_in[0].astype(F32)
    for t in range(1, n_chip):
        mixed = mixed + mix_in[t].astype(F32)
    mixed = mixed.astype(BF16).astype(F32)
    scaled = mixed * my_mix_gain

    def as_row(col):
        return jnp.sum(eye * col, axis=0, keepdims=True)

    def as_col(row):
        return jnp.sum(eye * row, axis=1, keepdims=True)

    def row_sum(value):
        return as_row(jnp.sum(value, axis=1, keepdims=True))

    sums = jnp.concatenate(
        [
            row_sum(mixed * mixed),
            row_sum(tok_cols * scaled),
            row_sum(scaled * scaled),
            jnp.zeros((1, rows), F32),
        ],
        axis=1,
    )
    sum_in[me] = sums
    send_tp(6, lambda peer: sum_in.at[me], sum_in.at[me])
    arrived(4, up_in.at[core])
    send(up_in.at[core], up_in.at[core], 14, {"tp": sibling})
    arrived(6, sum_in)
    sums = sum_in[0]
    for t in range(1, n_tp):
        sums = sums + sum_in[t]
    mix_square = as_col(sums[:, 0:rows])
    cross = as_col(sums[:, rows : 2 * rows])
    scaled_square = as_col(sums[:, 2 * rows : 3 * rows])
    mix_factor = lax.rsqrt(mix_square / width + norm_floor)
    resid = (tok_cols + scaled * mix_factor).astype(BF16).astype(F32)
    resid_square = square_sum + mix_factor * (2.0 * cross + mix_factor * scaled_square)
    resid_factor = lax.rsqrt(jnp.maximum(resid_square, 0.0) / width + norm_floor)
    expert_in = (resid * resid_factor * my_expert_gain).astype(BF16)

    route_f[...] = dot(dispatch, expert_in)
    for e in range(n_ep):
        dis_out[e] = route_f[slots * e : slots * (e + 1), :].astype(BF16)
    place = 2 * (group // 2) + core

    def send_tokens(d, _):
        peer = lax.rem(group + d, n_ep)
        send(dis_out.at[peer], dis_in.at[place], 7, {"ep": peer, "tp": 2 * chip + side})
        return 0

    lax.fori_loop(1, n_ep, send_tokens, 0)

    @pl.when(at_home)
    def _():
        dis_in[place] = dis_out[group]

    @pl.when(jnp.logical_not(at_home))
    def _():
        send(dis_out.at[group], dis_in.at[place], 7, {"tp": sibling})

    down_copy.wait()
    send_tp(8, lambda peer: piece(down_v, peer), half_of(down_in))
    down_in[core, me] = down_v[:, my_cols]

    arrived_all(13, gate_in.at[core])
    arrived_all(14, up_in.at[core])
    at_home_or_not(7, dis_in, recv_sems)
    side_rows = half_ep * slots
    for g in range(half_ep):
        for c in range(2):
            at = c * side_rows + slots * g
            route_f[at : at + slots, :] = dis_in[2 * g + c].astype(F32)
    received = [
        route_f[c * side_rows : (c + 1) * side_rows, :].astype(BF16) for c in range(2)
    ]
    ff = n_tp * ff_dev
    out_rows = side_rows // n_chip
    for n, source in enumerate((gate_in, up_in)):
        part = dot_t(received[0], source[0].reshape(ff, cols)) + dot_t(
            received[1], source[1].reshape(ff, cols)
        )
        part_out[:, :, n * ff : (n + 1) * ff] = part.reshape(n_chip, out_rows, ff).astype(BF16)

    send_chips(9, lambda peer: part_out.at[peer], part_in.at[chip])
    part_in[chip] = part_out[chip]
    arrived(9, part_in)
    both = part_in[0].astype(F32)
    for t in range(1, n_chip):
        both = both + part_in[t].astype(F32)
    gate, upward = both[:, :ff], both[:, ff:]
    hid_in[chip] = (gate / (1.0 + jnp.exp(-gate)) * upward).astype(BF16)

    send_chips(10, lambda peer: hid_in.at[chip], hid_in.at[chip])
    arrived(8, down_in.at[core])
    send(down_in.at[core], down_in.at[core], 15, {"tp": sibling})
    arrived_all(15, down_in.at[core])
    arrived(10, hid_in)
    hidden = hid_in[...].astype(F32).reshape(side_rows, ff).astype(BF16)
    for c in range(2):
        at = c * side_rows
        route_f[at : at + side_rows, :] = dot(hidden, down_in[c].reshape(ff, cols))
        for g in range(half_ep):
            at = c * side_rows + slots * g
            ret_out[2 * g + c] = route_f[at : at + slots, :].astype(BF16)

    def send_back(d, _):
        source = 2 * lax.rem(group // 2 + d, half_ep) + core
        for c in range(2):
            send(
                ret_out.at[2 * (source // 2) + c],
                ret_in.at[group],
                11,
                {"ep": source, "tp": 2 * chip + c},
            )
        return 0

    lax.fori_loop(1, half_ep, send_back, 0)

    @pl.when(at_home)
    def _():
        ret_in[group] = ret_out[place]
        send(ret_out.at[place + 1 - 2 * core], ret_in.at[group], 11, {"tp": sibling})

    @pl.when(jnp.logical_not(at_home))
    def _():
        for c in range(2):
            send(
                ret_out.at[2 * (group // 2) + c],
                ret_in.at[group],
                11,
                {"ep": 2 * (group // 2) + core, "tp": 2 * chip + c},
            )

    at_home_or_not(11, ret_in, recv_sems)
    for e in range(n_ep):
        route_f[slots * e : slots * (e + 1), :] = ret_in[e].astype(F32)
    out[...] = (resid + dot(combine, route_f[...], HIGHEST)).astype(BF16)

    sent(0, tok_in)
    for stage, buffer in (
        (1, qry_in),
        (2, gate_in.at[core]),
        (3, att_in),
        (4, up_in.at[core]),
        (5, mix_in),
        (6, sum_in),
        (8, down_in.at[core]),
        (9, part_in),
        (10, hid_in),
        (16, val_pair),
    ):
        sent(stage, buffer)
    sent_all(13, gate_in.at[core])
    sent_all(14, up_in.at[core])
    sent_all(15, down_in.at[core])
    sent_all(17, ow_pair.at[:, head_rows])
    at_home_or_not(7, dis_in, send_sems)
    at_home_or_not(11, ret_in, send_sems)


def per_device(
    tokens,
    lengths,
    latent_cache,
    rope_cache,
    attn_gain,
    query_weight,
    query_rot_weight,
    latent_weight,
    key_rot_weight,
    latent_gain,
    absorb_weight,
    value_weight,
    output_weight,
    mix_gain,
    expert_gain,
    gate_weight,
    up_weight,
    down_weight,
    expert_ids,
    route_weights,
):
    n_tp, n_ep = lax.axis_size("tp"), lax.axis_size("ep")
    own, width = tokens.shape
    rows = own * n_tp
    cols = width // n_tp
    latent = latent_weight.shape[1]
    context = latent_cache.shape[1]
    ff_dev = gate_weight.shape[2]
    ff = ff_dev * n_tp
    slots = 2 * rows * expert_ids.shape[1] // n_ep
    all_slots = n_ep * slots
    n_chip = n_tp // 2
    out_rows = all_slots // n_tp

    operands = (
        tokens,
        lengths.reshape(1, rows),
        latent_cache,
        jnp.swapaxes(rope_cache, 1, 2),
        attn_gain,
        mix_gain,
        expert_gain,
        latent_gain,
        query_weight,
        query_rot_weight.T,
        latent_weight,
        key_rot_weight.T,
        absorb_weight,
        value_weight,
        output_weight,
        jnp.swapaxes(gate_weight, 1, 2),
        jnp.swapaxes(up_weight, 1, 2),
        down_weight,
        expert_ids.T,
        route_weights.T,
    )
    vmem = pltpu.VMEM
    return pl.pallas_call(
        functools.partial(kernel, n_tp, n_ep),
        out_shape=(
            jax.ShapeDtypeStruct((rows, cols), BF16),
            jax.ShapeDtypeStruct((own, latent), BF16),
            jax.ShapeDtypeStruct((own, QK_ROPE), BF16),
        ),
        in_specs=[
            pl.BlockSpec(memory_space=pl.ANY) for _ in operands
        ],
        out_specs=[pl.BlockSpec(memory_space=vmem)] * 3,
        scratch_shapes=[
            vmem((1, rows), jnp.int32),
            vmem(expert_ids.shape[::-1], jnp.int32),
            vmem(route_weights.shape[::-1], F32),
            vmem((width,), BF16),
            vmem((width,), BF16),
            vmem((width,), BF16),
            vmem((latent,), BF16),
            vmem(latent_cache.shape, BF16),
            vmem((own, QK_ROPE, context), BF16),
            vmem(query_weight.shape, BF16),
            vmem((QK_ROPE, width), BF16),
            vmem(latent_weight.shape, BF16),
            vmem((QK_ROPE, cols), BF16),
            vmem(absorb_weight.shape[1:], BF16),
            vmem((2, *value_weight.shape[1:]), BF16),
            vmem((n_chip, 2 * output_weight.shape[0], cols), BF16),
            vmem((ff_dev, width), BF16),
            vmem((ff_dev, width), BF16),
            vmem((ff_dev, width), BF16),
            vmem((rows, width), F32),
            vmem((rows, width), BF16),
            vmem((rows, MESSAGE), F32),
            vmem((rows, latent), F32),
            vmem((all_slots, cols), F32),
            vmem((n_tp, own, width), BF16),
            vmem((n_tp, own, MESSAGE), BF16),
            vmem((n_tp, own, MESSAGE), BF16),
            vmem((n_chip, own, 2 * latent), BF16),
            vmem((n_tp, own, 2 * latent), BF16),
            vmem((n_chip, rows, cols), BF16),
            vmem((n_chip, rows, cols), BF16),
            vmem((n_tp, 1, 4 * rows), F32),
            vmem((n_ep, slots, cols), BF16),
            vmem((n_ep, slots, cols), BF16),
            vmem((n_chip, out_rows, 2 * ff), BF16),
            vmem((n_chip, out_rows, 2 * ff), BF16),
            vmem((n_chip, out_rows, ff), BF16),
            vmem((n_ep, slots, cols), BF16),
            vmem((n_ep, slots, cols), BF16),
            vmem((2, n_tp, ff_dev, cols), BF16),
            vmem((2, n_tp, ff_dev, cols), BF16),
            vmem((2, n_tp, ff_dev, cols), BF16),
            pltpu.SemaphoreType.DMA((20,)),
            pltpu.SemaphoreType.DMA((18,)),
            pltpu.SemaphoreType.DMA((18,)),
            pltpu.SemaphoreType.DMA((n_chip,)),
        ],
        compiler_params=pltpu.CompilerParams(
            collective_id=0, has_side_effects=True, vmem_limit_bytes=67_043_328
        ),
    )(*operands)


def solution(mesh):
    placed = (
        P(("ep", "tp"), None),
        P("ep"),
        P(("ep", "tp"), None, None),
        P(("ep", "tp"), None, None),
        P(),
        P(None, "tp"),
        P(None, "tp"),
        P("tp", None),
        P("tp", None),
        P(),
        P("tp", None, None),
        P("tp", None, None),
        P("tp", None),
        P(),
        P(),
        P("ep", None, "tp"),
        P("ep", None, "tp"),
        P("ep", "tp", None),
        P("ep", None),
        P("ep", None),
    )
    return jax.shard_map(
        per_device,
        mesh=mesh,
        in_specs=placed,
        out_specs=(P("ep", "tp"), P(("ep", "tp"), None), P(("ep", "tp"), None)),
        check_vma=False,
    )
```

```python
import functools

import jax
import jax.numpy as jnp
import numpy as np
from jax import lax
from jax.experimental import pallas as pl
from jax.experimental.pallas import tpu as pltpu
from jax.sharding import PartitionSpec as P

MESH = pl.DeviceIdType.MESH
F32 = jnp.float32
BF16 = jnp.bfloat16
HIGHEST = lax.Precision.HIGHEST

QK_NOPE = 128
QK_ROPE = 64
norm_floor = 1e-06
rope_base = 10000.0
masked_score = -1e30

LAT_AT, KEY_AT, ROT_AT, KEY_ROT_AT, MESSAGE = 0, 256, 512, 640, 768


def dot(a, b, precision=None):
    return lax.dot_general(
        a, b, (((1,), (0,)), ((), ())), preferred_element_type=F32, precision=precision
    )


def dot_t(a, b, precision=None):
    return lax.dot_general(
        a, b, (((1,), (1,)), ((), ())), preferred_element_type=F32, precision=precision
    )


def swap_halves(x):
    half = x.shape[-1] // 2
    return jnp.concatenate([x[:, half:], x[:, :half]], axis=1)


def gain_row(ref, first, size):
    return ref[pl.ds(first, size)].astype(F32).reshape(1, size)


def cos_sin(x):
    return jnp.cos(x), jnp.sin(x)


def iota(shape, dim):
    return lax.broadcasted_iota(jnp.int32, shape, dim)


def kernel(
    n_tp,
    n_ep,
    tokens,
    lengths,
    latent_cache,
    rope_cache,
    attn_gain,
    mix_gain,
    expert_gain,
    latent_gain,
    query_weight,
    query_rot_weight,
    latent_weight,
    key_rot_weight,
    absorb_weight,
    value_weight,
    output_weight,
    gate_weight,
    up_weight,
    down_weight,
    expert_ids,
    route_weights,
    out,
    new_latent,
    new_rope,
    len_v,
    ids_v,
    rw_v,
    attn_v,
    mixg_v,
    expg_v,
    latg_v,
    lat_v,
    rope_v,
    query_v,
    qrw_v,
    lw_v,
    krw_v,
    abs_v,
    val_pair,
    ow_pair,
    gate_v,
    up_v,
    down_v,
    tok_f,
    normed_b,
    msg_f,
    lat_f,
    route_f,
    tok_in,
    qry_out,
    qry_in,
    att_out,
    att_in,
    mix_out,
    mix_in,
    sum_in,
    dis_out,
    dis_in,
    part_out,
    part_in,
    hid_in,
    ret_out,
    ret_in,
    gate_in,
    up_in,
    down_in,
    local_sems,
    send_sems,
    recv_sems,
    tok_sems,
):
    me = lax.axis_index("tp")
    group = lax.axis_index("ep")
    rows = tok_f.shape[0]
    own = rows // n_tp
    width = tok_f.shape[1]
    cols = width // n_tp
    slots = dis_out.shape[1]
    ff_dev = gate_v.shape[0]
    latent = abs_v.shape[1]
    my_first = pl.multiple_of(me * cols, cols)
    my_cols = pl.ds(my_first, cols)
    n_chip = n_tp // 2
    half_ep = n_ep // 2
    chip = me // 2
    core = lax.rem(me, 2)
    sibling = me + 1 - 2 * core
    side = lax.rem(group, 2)
    at_home = side == core

    def load(index, src, dst):
        copy = pltpu.make_async_copy(src, dst, local_sems.at[index])
        copy.start()
        return copy

    tok_copy = load(0, tokens, tok_in.at[me])

    barrier = pltpu.get_barrier_semaphore()

    def greet(device):
        pl.semaphore_signal(barrier, inc=1, device_id=device, device_id_type=MESH)

    for d in range(1, n_tp):
        greet({"tp": lax.rem(me + d, n_tp)})

    for d in range(1, n_ep):
        greet({"ep": lax.rem(group + d, n_ep), "tp": 2 * chip + side})

    @pl.when(jnp.logical_not(at_home))
    def _():
        greet({"tp": sibling})

    for d in range(half_ep):
        greet({"ep": 2 * d + core, "tp": 2 * chip + 1 - side})

    small = [
        load(13, lengths, len_v),
        load(14, expert_ids, ids_v),
        load(15, route_weights, rw_v),
        load(16, attn_gain, attn_v),
        load(17, mix_gain, mixg_v),
        load(18, expert_gain, expg_v),
        load(19, latent_gain, latg_v),
    ]
    qw_copy = load(1, query_weight, query_v.at[:, pl.ds(0, QK_NOPE)])
    qrw_copy = load(2, query_rot_weight, qrw_v)
    lw_copy = load(3, latent_weight, lw_v)
    krw_copy = load(4, key_rot_weight, krw_v)
    abs_copy = load(5, absorb_weight.at[0], abs_v)
    gate_copy = load(6, gate_weight.at[0], gate_v)
    up_copy = load(7, up_weight.at[0], up_v)
    lat_copy = load(8, latent_cache, lat_v)
    rope_copy = load(9, rope_cache, rope_v)
    val_copy = load(10, value_weight.at[0], val_pair.at[core])
    value_dim = value_weight.shape[2]
    head_rows = pl.ds(pl.multiple_of(core * value_dim, value_dim), value_dim)

    def block(index):
        return pl.ds(pl.multiple_of(index * cols, cols), cols)

    for y in range(n_chip):
        pltpu.make_async_copy(
            output_weight.at[:, block(2 * y + core)],
            ow_pair.at[y, head_rows],
            local_sems.at[11],
        ).start()
    down_copy = load(12, down_weight.at[0], down_v)

    pl.semaphore_wait(
        barrier, n_tp - 1 + n_ep + half_ep - jnp.where(at_home, 1, 0)
    )

    order = sorted(range(1, n_tp), key=lambda d: -min(d, n_tp - d))
    chip_order = sorted(range(1, n_chip), key=lambda d: -min(d, n_chip - d))

    def send(src, dst, stage, device, recv_sem=None):
        pltpu.make_async_remote_copy(
            src_ref=src,
            dst_ref=dst,
            send_sem=send_sems.at[stage],
            recv_sem=recv_sems.at[stage] if recv_sem is None else recv_sem,
            device_id=device,
            device_id_type=MESH,
        ).start()

    def send_tp(stage, src_of, dst):
        for d in order:
            peer = lax.rem(me + d, n_tp)
            send(src_of(peer), dst(peer) if callable(dst) else dst, stage, {"tp": peer})

    def send_chips(stage, src_of, dst):
        for d in chip_order:
            peer = lax.rem(chip + d, n_chip)
            send(src_of(peer), dst, stage, {"tp": 2 * peer + core})

    def wait_for(sem, buffer, count):
        some = buffer.at[pl.ds(0, count)]
        pltpu.make_async_copy(some, some, sem).wait()

    def arrived(stage, buffer, count=None):
        wait_for(recv_sems.at[stage], buffer, buffer.shape[0] - 1 if count is None else count)

    def sent(stage, buffer, count=None):
        wait_for(send_sems.at[stage], buffer, buffer.shape[0] - 1 if count is None else count)

    def arrived_all(stage, buffer):
        pltpu.make_async_copy(buffer, buffer, recv_sems.at[stage]).wait()

    def sent_all(stage, buffer):
        pltpu.make_async_copy(buffer, buffer, send_sems.at[stage]).wait()

    def at_home_or_not(stage, buffer, sems):
        count = buffer.shape[0]

        @pl.when(at_home)
        def _():
            wait_for(sems.at[stage], buffer, count - 1)

        @pl.when(jnp.logical_not(at_home))
        def _():
            wait_for(sems.at[stage], buffer, count)

    tok_copy.wait()
    send(tok_in.at[me], tok_in.at[me], 0, {"tp": sibling}, recv_sems.at[12])
    for d in chip_order:
        peer = lax.rem(chip + d, n_chip)
        send(tok_in.at[me], tok_in.at[me], 0, {"tp": 2 * peer + core}, tok_sems.at[chip])

    square = (rows, rows)
    eye = (iota(square, 0) == iota(square, 1)).astype(F32)
    ahead_row = iota(square, 0) < iota(square, 1)
    ahead_col = iota(square, 1) < iota(square, 0)
    for copy in small:
        copy.wait()
    ids = ids_v[...].astype(F32)
    weights_row = rw_v[...]
    id_rows = [ids[k : k + 1, :] for k in range(2)]
    id_cols = [jnp.sum(eye * r, axis=1, keepdims=True) for r in id_rows]
    weight_cols = [
        jnp.sum(eye * weights_row[k : k + 1, :], axis=1, keepdims=True) for k in range(2)
    ]

    def same(j, k):
        return id_cols[j] == id_rows[k]

    def count(mask, axis):
        return jnp.sum(jnp.where(mask, 1.0, 0.0), axis=axis, keepdims=True)

    rank_row0 = count(same(0, 0) & ahead_row, 0)
    rank_row1 = count(same(0, 1), 0) + count(same(1, 1) & ahead_row, 0)
    rank_col0 = count(same(0, 0) & ahead_col, 1)
    rank_col1 = count(same(1, 0), 1) + count(same(1, 1) & ahead_col, 1)
    target_rows = [id_rows[0] * slots + rank_row0, id_rows[1] * slots + rank_row1]
    target_cols = [id_cols[0] * slots + rank_col0, id_cols[1] * slots + rank_col1]
    all_slots = n_ep * slots
    down_iota = iota((all_slots, rows), 0).astype(F32)
    across_iota = iota((rows, all_slots), 1).astype(F32)
    dispatch = (
        jnp.where(down_iota == target_rows[0], 1.0, 0.0)
        + jnp.where(down_iota == target_rows[1], 1.0, 0.0)
    ).astype(BF16)
    combine = jnp.where(across_iota == target_cols[0], weight_cols[0], 0.0) + jnp.where(
        across_iota == target_cols[1], weight_cols[1], 0.0
    )

    half = QK_ROPE // 2
    freqs = jnp.zeros((1, QK_ROPE), F32)
    lane = lax.rem(iota((1, QK_ROPE), 1), half)
    for i in range(half):
        freqs = jnp.where(lane == i, float(np.float32(rope_base ** (-i / half))), freqs)
    lengths_row = len_v[...].astype(F32)
    lengths_col = jnp.sum(eye * lengths_row, axis=1, keepdims=True)
    cosine, sine = cos_sin(lengths_col * freqs)
    sine = jnp.where(iota((1, QK_ROPE), 1) < half, -sine, sine)
    own_rows = (iota((8, rows), 1) == own * me + iota((8, rows), 0)).astype(F32)
    own_cosine = dot(own_rows, cosine, HIGHEST)[:own]
    own_sine = dot(own_rows, sine, HIGHEST)[:own]
    own_lengths = jnp.sum(own_rows * lengths_row, axis=1, keepdims=True).astype(jnp.int32)

    qrw_copy.wait()
    for c in range(0, width, 512):
        query_v[c : c + 512, QK_NOPE : QK_NOPE + QK_ROPE] = qrw_v[:, c : c + 512].T
    qw_copy.wait()
    for d in reversed(chip_order):
        peer = lax.rem(chip + d, n_chip)
        slot = tok_in.at[2 * peer + core]
        pltpu.make_async_copy(slot, slot, tok_sems.at[peer]).wait()
        send(slot, slot, 0, {"tp": sibling}, recv_sems.at[12])
    arrived(12, tok_in, n_chip)
    for t in range(n_tp):
        tok_f[own * t : own * (t + 1), :] = tok_in[t].astype(F32)
    chunk = 512
    square_sum = jnp.zeros((rows, 1), F32)
    for c in range(0, width, chunk):
        x = tok_f[:, c : c + chunk]
        square_sum = square_sum + jnp.sum(x * x, axis=1, keepdims=True)
    factor = lax.rsqrt(square_sum / width + norm_floor)
    for c in range(0, width, chunk):
        x = tok_f[:, c : c + chunk]
        normed_b[:, c : c + chunk] = (x * factor * gain_row(attn_v, c, chunk)).astype(BF16)

    query = dot(normed_b[...], query_v[...])
    q_nope = query[:, :QK_NOPE].astype(BF16)
    q_rot = query[:, QK_NOPE : QK_NOPE + QK_ROPE]
    abs_copy.wait()
    msg_f[:, LAT_AT : LAT_AT + latent] = dot(q_nope, abs_v[...])
    msg_f[:, ROT_AT : ROT_AT + QK_ROPE] = q_rot * cosine + swap_halves(q_rot) * sine
    slice_rows = normed_b[:, my_cols]
    lw_copy.wait()
    msg_f[:, KEY_AT : KEY_AT + latent] = dot(slice_rows, lw_v[...])
    krw_copy.wait()
    msg_f[:, KEY_ROT_AT : KEY_ROT_AT + QK_ROPE] = dot_t(slice_rows, krw_v[...])
    for t in range(n_tp):
        qry_out[t] = msg_f[own * t : own * (t + 1), :].astype(BF16)

    send_tp(1, lambda peer: qry_out.at[peer], qry_in.at[me])
    qry_in[me] = qry_out[me]
    send(value_weight.at[0], val_pair.at[core], 16, {"tp": sibling})
    for y in range(n_chip):
        send(
            output_weight.at[:, block(2 * y + 1 - core)],
            ow_pair.at[y, head_rows],
            17,
            {"tp": sibling},
        )
    gate_copy.wait()

    def piece(ref, peer):
        return ref.at[:, pl.ds(pl.multiple_of(peer * cols, cols), cols)]

    def half_of(ref):
        return lambda peer: ref.at[lax.rem(peer, 2), me]

    send_tp(2, lambda peer: piece(gate_v, peer), half_of(gate_in))
    gate_in[core, me] = gate_v[:, my_cols]

    lat_copy.wait()
    rope_copy.wait()

    arrived(1, qry_in)
    key_sum = jnp.zeros((own, MESSAGE), F32)
    for h in range(n_tp):
        part = qry_in[h].astype(F32)
        key_sum = key_sum + part
        msg_f[own * h : own * (h + 1), :] = part
    key_raw = key_sum[:, KEY_AT : KEY_AT + latent]
    key_factor = lax.rsqrt(jnp.mean(key_raw * key_raw, axis=1, keepdims=True) + norm_floor)
    own_lat = (key_raw * key_factor * gain_row(latg_v, 0, latent)).astype(BF16)
    rope_raw = key_sum[:, KEY_ROT_AT : KEY_ROT_AT + QK_ROPE]
    own_rot = (rope_raw * own_cosine + swap_halves(rope_raw) * own_sine).astype(BF16)
    new_latent[...] = own_lat
    new_rope[...] = own_rot
    own_lat = own_lat.astype(F32)
    own_rot = own_rot.astype(F32)

    scale = (QK_NOPE + QK_ROPE) ** (-0.5)
    queries = msg_f[:, LAT_AT : LAT_AT + latent]
    rotated = msg_f[:, ROT_AT : ROT_AT + QK_ROPE]
    queries_b = queries.astype(BF16)
    rotated_b = rotated.astype(BF16)
    context = lat_v.shape[1]
    row_col = iota((rows, 1), 0)
    first = lax.rem(row_col, own) == 0

    def of_row(a, b):
        return jnp.where(first, a, b)

    scores = of_row(
        dot_t(queries_b, lat_v[0]) + dot(rotated_b, rope_v[0]),
        dot_t(queries_b, lat_v[1]) + dot(rotated_b, rope_v[1]),
    )
    row_len = of_row(own_lengths[0:1], own_lengths[1:2])
    valid = iota((rows, context), 1) < row_len
    scores = jnp.where(valid, scores * scale, masked_score)
    lat_rows = of_row(own_lat[0:1], own_lat[1:2])
    rot_rows = of_row(own_rot[0:1], own_rot[1:2])
    own_score = (
        jnp.sum(queries * lat_rows, axis=1, keepdims=True)
        + jnp.sum(rotated * rot_rows, axis=1, keepdims=True)
    ) * scale
    top = jnp.maximum(jnp.max(scores, axis=1, keepdims=True), own_score)
    weights = jnp.where(valid, jnp.exp(scores - top), 0.0)
    own_weight = jnp.exp(own_score - top)
    total = jnp.sum(weights, axis=1, keepdims=True) + own_weight
    summed = (
        dot(jnp.where(first, weights, 0.0).astype(BF16), lat_v[0])
        + dot(jnp.where(first, 0.0, weights).astype(BF16), lat_v[1])
        + own_weight.astype(BF16).astype(F32) * lat_rows
    )
    lat_f[...] = summed / total
    for y in range(n_chip):
        for c in range(2):
            at = own * (2 * y + c)
            att_out[y, :, c * latent : (c + 1) * latent] = lat_f[at : at + own, :].astype(BF16)

    send_tp(3, lambda peer: att_out.at[peer // 2], att_in.at[me])
    att_in[me] = att_out[chip]
    up_copy.wait()
    send_tp(4, lambda peer: piece(up_v, peer), half_of(up_in))
    up_in[core, me] = up_v[:, my_cols]
    val_copy.wait()
    pltpu.make_async_copy(
        ow_pair.at[:, head_rows], ow_pair.at[:, head_rows], local_sems.at[11]
    ).wait()
    arrived(16, val_pair)
    pltpu.make_async_copy(
        ow_pair.at[:, head_rows], ow_pair.at[:, head_rows], recv_sems.at[17]
    ).wait()

    arrived(3, att_in)
    for t in range(n_tp):
        msg_f[own * t : own * (t + 1), : 2 * latent] = att_in[t].astype(F32)
    results = msg_f[:, : 2 * latent].astype(BF16)
    head_values = jnp.concatenate(
        [dot(results[:, c * latent : (c + 1) * latent], val_pair[c]) for c in range(2)], axis=1
    ).astype(BF16)

    for d in chip_order + [0]:
        peer = lax.rem(chip + d, n_chip)
        share = dot(head_values, ow_pair[peer]).astype(BF16)
        if d:
            mix_out[peer] = share
            send(mix_out.at[peer], mix_in.at[chip], 5, {"tp": 2 * peer + core})
        else:
            mix_in[chip] = share

    arrived(2, gate_in.at[core])
    send(gate_in.at[core], gate_in.at[core], 13, {"tp": sibling})
    tok_cols = tok_f[:, my_cols]
    my_mix_gain = gain_row(mixg_v, my_first, cols)
    my_expert_gain = gain_row(expg_v, my_first, cols)

    arrived(5, mix_in)
    mixed = mix_in[0].astype(F32)
    for t in range(1, n_chip):
        mixed = mixed + mix_in[t].astype(F32)
    mixed = mixed.astype(BF16).astype(F32)
    scaled = mixed * my_mix_gain

    def as_row(col):
        return jnp.sum(eye * col, axis=0, keepdims=True)

    def as_col(row):
        return jnp.sum(eye * row, axis=1, keepdims=True)

    def row_sum(value):
        return as_row(jnp.sum(value, axis=1, keepdims=True))

    sums = jnp.concatenate(
        [
            row_sum(mixed * mixed),
            row_sum(tok_cols * scaled),
            row_sum(scaled * scaled),
            jnp.zeros((1, rows), F32),
        ],
        axis=1,
    )
    sum_in[me] = sums
    send_tp(6, lambda peer: sum_in.at[me], sum_in.at[me])
    arrived(4, up_in.at[core])
    send(up_in.at[core], up_in.at[core], 14, {"tp": sibling})
    arrived(6, sum_in)
    sums = sum_in[0]
    for t in range(1, n_tp):
        sums = sums + sum_in[t]
    mix_square = as_col(sums[:, 0:rows])
    cross = as_col(sums[:, rows : 2 * rows])
    scaled_square = as_col(sums[:, 2 * rows : 3 * rows])
    mix_factor = lax.rsqrt(mix_square / width + norm_floor)
    resid = (tok_cols + scaled * mix_factor).astype(BF16).astype(F32)
    resid_square = square_sum + mix_factor * (2.0 * cross + mix_factor * scaled_square)
    resid_factor = lax.rsqrt(jnp.maximum(resid_square, 0.0) / width + norm_floor)
    expert_in = (resid * resid_factor * my_expert_gain).astype(BF16)

    route_f[...] = dot(dispatch, expert_in)
    for e in range(n_ep):
        dis_out[e] = route_f[slots * e : slots * (e + 1), :].astype(BF16)
    place = 2 * (group // 2) + core

    for d in range(1, n_ep):
        peer = lax.rem(group + d, n_ep)
        send(dis_out.at[peer], dis_in.at[place], 7, {"ep": peer, "tp": 2 * chip + side})

    @pl.when(at_home)
    def _():
        dis_in[place] = dis_out[group]

    @pl.when(jnp.logical_not(at_home))
    def _():
        send(dis_out.at[group], dis_in.at[place], 7, {"tp": sibling})

    down_copy.wait()
    send_tp(8, lambda peer: piece(down_v, peer), half_of(down_in))
    down_in[core, me] = down_v[:, my_cols]

    arrived_all(13, gate_in.at[core])
    arrived_all(14, up_in.at[core])
    at_home_or_not(7, dis_in, recv_sems)
    side_rows = half_ep * slots
    for g in range(half_ep):
        for c in range(2):
            at = c * side_rows + slots * g
            route_f[at : at + slots, :] = dis_in[2 * g + c].astype(F32)
    received = [
        route_f[c * side_rows : (c + 1) * side_rows, :].astype(BF16) for c in range(2)
    ]
    ff = n_tp * ff_dev
    out_rows = side_rows // n_chip
    for n, source in enumerate((gate_in, up_in)):
        part = dot_t(received[0], source[0].reshape(ff, cols)) + dot_t(
            received[1], source[1].reshape(ff, cols)
        )
        part_out[:, :, n * ff : (n + 1) * ff] = part.reshape(n_chip, out_rows, ff).astype(BF16)

    send_chips(9, lambda peer: part_out.at[peer], part_in.at[chip])
    part_in[chip] = part_out[chip]
    arrived(9, part_in)
    both = part_in[0].astype(F32)
    for t in range(1, n_chip):
        both = both + part_in[t].astype(F32)
    gate, upward = both[:, :ff], both[:, ff:]
    hid_in[chip] = (gate / (1.0 + jnp.exp(-gate)) * upward).astype(BF16)

    send_chips(10, lambda peer: hid_in.at[chip], hid_in.at[chip])
    arrived(8, down_in.at[core])
    send(down_in.at[core], down_in.at[core], 15, {"tp": sibling})
    arrived_all(15, down_in.at[core])
    arrived(10, hid_in)
    hidden = hid_in[...].astype(F32).reshape(side_rows, ff).astype(BF16)
    for c in range(2):
        at = c * side_rows
        route_f[at : at + side_rows, :] = dot(hidden, down_in[c].reshape(ff, cols))
        for g in range(half_ep):
            at = c * side_rows + slots * g
            ret_out[2 * g + c] = route_f[at : at + slots, :].astype(BF16)

    for d in range(1, half_ep):
        pair = lax.rem(group // 2 + d, half_ep)
        for c in range(2):
            send(
                ret_out.at[2 * pair + c],
                ret_in.at[group],
                11,
                {"ep": 2 * pair + core, "tp": 2 * chip + c},
            )

    @pl.when(at_home)
    def _():
        ret_in[group] = ret_out[place]
        send(ret_out.at[place + 1 - 2 * core], ret_in.at[group], 11, {"tp": sibling})

    @pl.when(jnp.logical_not(at_home))
    def _():
        for c in range(2):
            send(
                ret_out.at[2 * (group // 2) + c],
                ret_in.at[group],
                11,
                {"ep": 2 * (group // 2) + core, "tp": 2 * chip + c},
            )

    at_home_or_not(11, ret_in, recv_sems)
    for e in range(n_ep):
        route_f[slots * e : slots * (e + 1), :] = ret_in[e].astype(F32)
    out[...] = (resid + dot(combine, route_f[...], HIGHEST)).astype(BF16)

    sent(0, tok_in)
    for stage, buffer in (
        (1, qry_in),
        (2, gate_in.at[core]),
        (3, att_in),
        (4, up_in.at[core]),
        (5, mix_in),
        (6, sum_in),
        (8, down_in.at[core]),
        (9, part_in),
        (10, hid_in),
        (16, val_pair),
    ):
        sent(stage, buffer)
    sent_all(13, gate_in.at[core])
    sent_all(14, up_in.at[core])
    sent_all(15, down_in.at[core])
    sent_all(17, ow_pair.at[:, head_rows])
    at_home_or_not(7, dis_in, send_sems)
    at_home_or_not(11, ret_in, send_sems)


def hand_over(*refs):
    sources, targets, held, sems = refs[:3], refs[3:6], refs[6:9], refs[9]
    inward = [pltpu.make_async_copy(a, b, sems.at[i]) for i, (a, b) in enumerate(zip(sources, held))]
    outward = [
        pltpu.make_async_copy(a, b, sems.at[3 + i]) for i, (a, b) in enumerate(zip(held, targets))
    ]
    for copy in inward:
        copy.start()
    for before, copy in zip(inward, outward):
        before.wait()
        copy.start()
    for copy in outward:
        copy.wait()


def per_device(
    tokens,
    lengths,
    latent_cache,
    rope_cache,
    attn_gain,
    query_weight,
    query_rot_weight,
    latent_weight,
    key_rot_weight,
    latent_gain,
    absorb_weight,
    value_weight,
    output_weight,
    mix_gain,
    expert_gain,
    gate_weight,
    up_weight,
    down_weight,
    expert_ids,
    route_weights,
):
    n_tp, n_ep = lax.axis_size("tp"), lax.axis_size("ep")
    own, width = tokens.shape
    rows = own * n_tp
    cols = width // n_tp
    latent = latent_weight.shape[1]
    context = latent_cache.shape[1]
    ff_dev = gate_weight.shape[2]
    ff = ff_dev * n_tp
    slots = 2 * rows * expert_ids.shape[1] // n_ep
    all_slots = n_ep * slots
    n_chip = n_tp // 2
    out_rows = all_slots // n_tp

    operands = (
        tokens,
        lengths.reshape(1, rows),
        latent_cache,
        jnp.swapaxes(rope_cache, 1, 2),
        attn_gain,
        mix_gain,
        expert_gain,
        latent_gain,
        query_weight,
        query_rot_weight.T,
        latent_weight,
        key_rot_weight.T,
        absorb_weight,
        value_weight,
        output_weight,
        jnp.swapaxes(gate_weight, 1, 2),
        jnp.swapaxes(up_weight, 1, 2),
        down_weight,
        expert_ids.T,
        route_weights.T,
    )
    vmem = pltpu.VMEM
    shapes = (
        jax.ShapeDtypeStruct((rows, cols), BF16),
        jax.ShapeDtypeStruct((own, latent), BF16),
        jax.ShapeDtypeStruct((own, QK_ROPE), BF16),
    )
    results = pl.pallas_call(
        functools.partial(kernel, n_tp, n_ep),
        out_shape=shapes,
        in_specs=[
            pl.BlockSpec(memory_space=pl.ANY) for _ in operands
        ],
        out_specs=[pl.BlockSpec(memory_space=vmem)] * 3,
        scratch_shapes=[
            vmem((1, rows), jnp.int32),
            vmem(expert_ids.shape[::-1], jnp.int32),
            vmem(route_weights.shape[::-1], F32),
            vmem((width,), BF16),
            vmem((width,), BF16),
            vmem((width,), BF16),
            vmem((latent,), BF16),
            vmem(latent_cache.shape, BF16),
            vmem((own, QK_ROPE, context), BF16),
            vmem((width, QK_NOPE + QK_ROPE), BF16),
            vmem((QK_ROPE, width), BF16),
            vmem(latent_weight.shape, BF16),
            vmem((QK_ROPE, cols), BF16),
            vmem(absorb_weight.shape[1:], BF16),
            vmem((2, *value_weight.shape[1:]), BF16),
            vmem((n_chip, 2 * output_weight.shape[0], cols), BF16),
            vmem((ff_dev, width), BF16),
            vmem((ff_dev, width), BF16),
            vmem((ff_dev, width), BF16),
            vmem((rows, width), F32),
            vmem((rows, width), BF16),
            vmem((rows, MESSAGE), F32),
            vmem((rows, latent), F32),
            vmem((all_slots, cols), F32),
            vmem((n_tp, own, width), BF16),
            vmem((n_tp, own, MESSAGE), BF16),
            vmem((n_tp, own, MESSAGE), BF16),
            vmem((n_chip, own, 2 * latent), BF16),
            vmem((n_tp, own, 2 * latent), BF16),
            vmem((n_chip, rows, cols), BF16),
            vmem((n_chip, rows, cols), BF16),
            vmem((n_tp, 1, 4 * rows), F32),
            vmem((n_ep, slots, cols), BF16),
            vmem((n_ep, slots, cols), BF16),
            vmem((n_chip, out_rows, 2 * ff), BF16),
            vmem((n_chip, out_rows, 2 * ff), BF16),
            vmem((n_chip, out_rows, ff), BF16),
            vmem((n_ep, slots, cols), BF16),
            vmem((n_ep, slots, cols), BF16),
            vmem((2, n_tp, ff_dev, cols), BF16),
            vmem((2, n_tp, ff_dev, cols), BF16),
            vmem((2, n_tp, ff_dev, cols), BF16),
            pltpu.SemaphoreType.DMA((20,)),
            pltpu.SemaphoreType.DMA((18,)),
            pltpu.SemaphoreType.DMA((18,)),
            pltpu.SemaphoreType.DMA((n_chip,)),
        ],
        compiler_params=pltpu.CompilerParams(
            collective_id=0, has_side_effects=True, vmem_limit_bytes=67_043_328
        ),
    )(*operands)
    return pl.pallas_call(
        hand_over,
        out_shape=shapes,
        in_specs=[pl.BlockSpec(memory_space=pl.ANY)] * 3,
        out_specs=[pl.BlockSpec(memory_space=pl.ANY)] * 3,
        scratch_shapes=[vmem(x.shape, BF16) for x in shapes] + [pltpu.SemaphoreType.DMA((6,))],
        compiler_params=pltpu.CompilerParams(vmem_limit_bytes=67_043_328),
    )(*results)


def solution(mesh):
    placed = (
        P(("ep", "tp"), None),
        P("ep"),
        P(("ep", "tp"), None, None),
        P(("ep", "tp"), None, None),
        P(),
        P(None, "tp"),
        P(None, "tp"),
        P("tp", None),
        P("tp", None),
        P(),
        P("tp", None, None),
        P("tp", None, None),
        P("tp", None),
        P(),
        P(),
        P("ep", None, "tp"),
        P("ep", None, "tp"),
        P("ep", "tp", None),
        P("ep", None),
        P("ep", None),
    )
    return jax.shard_map(
        per_device,
        mesh=mesh,
        in_specs=placed,
        out_specs=(P("ep", "tp"), P(("ep", "tp"), None), P(("ep", "tp"), None)),
        check_vma=False,
    )
```

```python
import functools

import jax
import jax.numpy as jnp
import numpy as np
from jax import lax
from jax.experimental import pallas as pl
from jax.experimental.pallas import tpu as pltpu
from jax.sharding import PartitionSpec as P

MESH = pl.DeviceIdType.MESH
F32 = jnp.float32
BF16 = jnp.bfloat16
HIGHEST = lax.Precision.HIGHEST

QK_NOPE = 128
QK_ROPE = 64
norm_floor = 1e-06
rope_base = 10000.0
masked_score = -1e30

LAT_AT, KEY_AT, ROT_AT, KEY_ROT_AT, MESSAGE = 0, 256, 512, 640, 768


def dot(a, b, precision=None):
    return lax.dot_general(
        a, b, (((1,), (0,)), ((), ())), preferred_element_type=F32, precision=precision
    )


def dot_t(a, b, precision=None):
    return lax.dot_general(
        a, b, (((1,), (1,)), ((), ())), preferred_element_type=F32, precision=precision
    )


def swap_halves(x):
    half = x.shape[-1] // 2
    return jnp.concatenate([x[:, half:], x[:, :half]], axis=1)


def gain_row(ref, first, size):
    return ref[pl.ds(first, size)].astype(F32).reshape(1, size)


def cos_sin(x):
    return jnp.cos(x), jnp.sin(x)


def iota(shape, dim):
    return lax.broadcasted_iota(jnp.int32, shape, dim)


def kernel(
    n_tp,
    n_ep,
    tokens,
    lengths,
    latent_cache,
    rope_cache,
    attn_gain,
    mix_gain,
    expert_gain,
    latent_gain,
    query_weight,
    query_rot_weight,
    latent_weight,
    key_rot_weight,
    absorb_weight,
    value_weight,
    output_weight,
    gate_weight,
    up_weight,
    down_weight,
    expert_ids,
    route_weights,
    out,
    new_latent,
    new_rope,
    len_v,
    ids_v,
    rw_v,
    attn_v,
    mixg_v,
    expg_v,
    latg_v,
    lat_v,
    rope_v,
    query_v,
    qrw_v,
    lw_v,
    krw_v,
    abs_v,
    val_pair,
    ow_pair,
    gate_v,
    up_v,
    down_v,
    tok_f,
    normed_b,
    msg_f,
    lat_f,
    route_f,
    tok_in,
    qry_out,
    qry_in,
    att_out,
    att_in,
    mix_out,
    mix_in,
    sum_in,
    dis_out,
    dis_in,
    part_out,
    part_in,
    hid_in,
    ret_out,
    ret_in,
    gate_in,
    up_in,
    down_in,
    local_sems,
    send_sems,
    recv_sems,
    tok_sems,
):
    me = lax.axis_index("tp")
    group = lax.axis_index("ep")
    rows = tok_f.shape[0]
    own = rows // n_tp
    width = tok_f.shape[1]
    cols = width // n_tp
    slots = dis_out.shape[1]
    ff_dev = gate_v.shape[0]
    latent = abs_v.shape[1]
    my_first = pl.multiple_of(me * cols, cols)
    my_cols = pl.ds(my_first, cols)
    n_chip = n_tp // 2
    half_ep = n_ep // 2
    chip = me // 2
    core = lax.rem(me, 2)
    sibling = me + 1 - 2 * core
    side = lax.rem(group, 2)
    at_home = side == core

    def load(index, src, dst):
        copy = pltpu.make_async_copy(src, dst, local_sems.at[index])
        copy.start()
        return copy

    tok_copy = load(0, tokens, tok_in.at[me])

    barrier = pltpu.get_barrier_semaphore()

    def greet(device):
        pl.semaphore_signal(barrier, inc=1, device_id=device, device_id_type=MESH)

    for d in range(1, n_tp):
        greet({"tp": lax.rem(me + d, n_tp)})

    for d in range(1, n_ep):
        greet({"ep": lax.rem(group + d, n_ep), "tp": 2 * chip + side})

    @pl.when(jnp.logical_not(at_home))
    def _():
        greet({"tp": sibling})

    for d in range(half_ep):
        greet({"ep": 2 * d + core, "tp": 2 * chip + 1 - side})

    small = [
        load(13, lengths, len_v),
        load(14, expert_ids, ids_v),
        load(15, route_weights, rw_v),
        load(16, attn_gain, attn_v),
        load(17, mix_gain, mixg_v),
        load(18, expert_gain, expg_v),
        load(19, latent_gain, latg_v),
    ]
    qw_copy = load(1, query_weight, query_v.at[:, pl.ds(0, QK_NOPE)])
    qrw_copy = load(2, query_rot_weight, qrw_v)
    lw_copy = load(3, latent_weight, lw_v)
    krw_copy = load(4, key_rot_weight, krw_v)
    abs_copy = load(5, absorb_weight.at[0], abs_v)
    gate_copy = load(6, gate_weight.at[0], gate_v)
    up_copy = load(7, up_weight.at[0], up_v)
    lat_copy = load(8, latent_cache, lat_v)
    rope_copy = load(9, rope_cache, rope_v)
    val_copy = load(10, value_weight.at[0], val_pair.at[core])
    value_dim = value_weight.shape[2]
    head_rows = pl.ds(pl.multiple_of(core * value_dim, value_dim), value_dim)

    def block(index):
        return pl.ds(pl.multiple_of(index * cols, cols), cols)

    for y in range(n_chip):
        pltpu.make_async_copy(
            output_weight.at[:, block(2 * y + core)],
            ow_pair.at[y, head_rows],
            local_sems.at[11],
        ).start()
    down_copy = load(12, down_weight.at[0], down_v)

    pl.semaphore_wait(
        barrier, n_tp - 1 + n_ep + half_ep - jnp.where(at_home, 1, 0)
    )

    order = sorted(range(1, n_tp), key=lambda d: -min(d, n_tp - d))
    chip_order = sorted(range(1, n_chip), key=lambda d: -min(d, n_chip - d))

    def send(src, dst, stage, device, recv_sem=None):
        pltpu.make_async_remote_copy(
            src_ref=src,
            dst_ref=dst,
            send_sem=send_sems.at[stage],
            recv_sem=recv_sems.at[stage] if recv_sem is None else recv_sem,
            device_id=device,
            device_id_type=MESH,
        ).start()

    def send_tp(stage, src_of, dst):
        for d in order:
            peer = lax.rem(me + d, n_tp)
            send(src_of(peer), dst(peer) if callable(dst) else dst, stage, {"tp": peer})

    def send_chips(stage, src_of, dst):
        for d in chip_order:
            peer = lax.rem(chip + d, n_chip)
            send(src_of(peer), dst, stage, {"tp": 2 * peer + core})

    def wait_for(sem, buffer, count):
        some = buffer.at[pl.ds(0, count)]
        pltpu.make_async_copy(some, some, sem).wait()

    def arrived(stage, buffer, count=None):
        wait_for(recv_sems.at[stage], buffer, buffer.shape[0] - 1 if count is None else count)

    def sent(stage, buffer, count=None):
        wait_for(send_sems.at[stage], buffer, buffer.shape[0] - 1 if count is None else count)

    def arrived_all(stage, buffer):
        pltpu.make_async_copy(buffer, buffer, recv_sems.at[stage]).wait()

    def sent_all(stage, buffer):
        pltpu.make_async_copy(buffer, buffer, send_sems.at[stage]).wait()

    def at_home_or_not(stage, buffer, sems):
        count = buffer.shape[0]

        @pl.when(at_home)
        def _():
            wait_for(sems.at[stage], buffer, count - 1)

        @pl.when(jnp.logical_not(at_home))
        def _():
            wait_for(sems.at[stage], buffer, count)

    tok_copy.wait()
    send(tok_in.at[me], tok_in.at[me], 0, {"tp": sibling}, recv_sems.at[12])
    for d in chip_order:
        peer = lax.rem(chip + d, n_chip)
        send(tok_in.at[me], tok_in.at[me], 0, {"tp": 2 * peer + core}, tok_sems.at[chip])

    square = (rows, rows)
    eye = (iota(square, 0) == iota(square, 1)).astype(F32)
    ahead_row = iota(square, 0) < iota(square, 1)
    ahead_col = iota(square, 1) < iota(square, 0)
    for copy in small:
        copy.wait()
    ids = ids_v[...].astype(F32)
    weights_row = rw_v[...]
    id_rows = [ids[k : k + 1, :] for k in range(2)]
    id_cols = [jnp.sum(eye * r, axis=1, keepdims=True) for r in id_rows]
    weight_cols = [
        jnp.sum(eye * weights_row[k : k + 1, :], axis=1, keepdims=True) for k in range(2)
    ]

    def same(j, k):
        return id_cols[j] == id_rows[k]

    def count(mask, axis):
        return jnp.sum(jnp.where(mask, 1.0, 0.0), axis=axis, keepdims=True)

    rank_row0 = count(same(0, 0) & ahead_row, 0)
    rank_row1 = count(same(0, 1), 0) + count(same(1, 1) & ahead_row, 0)
    rank_col0 = count(same(0, 0) & ahead_col, 1)
    rank_col1 = count(same(1, 0), 1) + count(same(1, 1) & ahead_col, 1)
    target_rows = [id_rows[0] * slots + rank_row0, id_rows[1] * slots + rank_row1]
    target_cols = [id_cols[0] * slots + rank_col0, id_cols[1] * slots + rank_col1]
    all_slots = n_ep * slots
    down_iota = iota((all_slots, rows), 0).astype(F32)
    across_iota = iota((rows, all_slots), 1).astype(F32)
    dispatch = (
        jnp.where(down_iota == target_rows[0], 1.0, 0.0)
        + jnp.where(down_iota == target_rows[1], 1.0, 0.0)
    ).astype(BF16)
    combine = jnp.where(across_iota == target_cols[0], weight_cols[0], 0.0) + jnp.where(
        across_iota == target_cols[1], weight_cols[1], 0.0
    )

    half = QK_ROPE // 2
    freqs = jnp.zeros((1, QK_ROPE), F32)
    lane = lax.rem(iota((1, QK_ROPE), 1), half)
    for i in range(half):
        freqs = jnp.where(lane == i, float(np.float32(rope_base ** (-i / half))), freqs)
    lengths_row = len_v[...].astype(F32)
    lengths_col = jnp.sum(eye * lengths_row, axis=1, keepdims=True)
    cosine, sine = cos_sin(lengths_col * freqs)
    sine = jnp.where(iota((1, QK_ROPE), 1) < half, -sine, sine)
    own_rows = (iota((8, rows), 1) == own * me + iota((8, rows), 0)).astype(F32)
    own_cosine = dot(own_rows, cosine, HIGHEST)[:own]
    own_sine = dot(own_rows, sine, HIGHEST)[:own]
    own_lengths = jnp.sum(own_rows * lengths_row, axis=1, keepdims=True).astype(jnp.int32)

    qrw_copy.wait()
    for c in range(0, width, 512):
        query_v[c : c + 512, QK_NOPE : QK_NOPE + QK_ROPE] = qrw_v[:, c : c + 512].T
    qw_copy.wait()
    for d in reversed(chip_order):
        peer = lax.rem(chip + d, n_chip)
        slot = tok_in.at[2 * peer + core]
        pltpu.make_async_copy(slot, slot, tok_sems.at[peer]).wait()
        send(slot, slot, 0, {"tp": sibling}, recv_sems.at[12])
    arrived(12, tok_in, n_chip)
    for t in range(n_tp):
        tok_f[own * t : own * (t + 1), :] = tok_in[t].astype(F32)
    chunk = 512
    square_sum = jnp.zeros((rows, 1), F32)
    for c in range(0, width, chunk):
        x = tok_f[:, c : c + chunk]
        square_sum = square_sum + jnp.sum(x * x, axis=1, keepdims=True)
    factor = lax.rsqrt(square_sum / width + norm_floor)
    for c in range(0, width, chunk):
        x = tok_f[:, c : c + chunk]
        normed_b[:, c : c + chunk] = (x * factor * gain_row(attn_v, c, chunk)).astype(BF16)

    mid = width // 2
    query = dot(normed_b[:, :mid], query_v[:mid]) + dot(normed_b[:, mid:], query_v[mid:])
    q_nope = query[:, :QK_NOPE].astype(BF16)
    q_rot = query[:, QK_NOPE : QK_NOPE + QK_ROPE]
    abs_copy.wait()
    msg_f[:, LAT_AT : LAT_AT + latent] = dot(q_nope, abs_v[...])
    msg_f[:, ROT_AT : ROT_AT + QK_ROPE] = q_rot * cosine + swap_halves(q_rot) * sine
    slice_rows = normed_b[:, my_cols]
    lw_copy.wait()
    msg_f[:, KEY_AT : KEY_AT + latent] = dot(slice_rows, lw_v[...])
    krw_copy.wait()
    msg_f[:, KEY_ROT_AT : KEY_ROT_AT + QK_ROPE] = dot_t(slice_rows, krw_v[...])
    for t in range(n_tp):
        qry_out[t] = msg_f[own * t : own * (t + 1), :].astype(BF16)

    send_tp(1, lambda peer: qry_out.at[peer], qry_in.at[me])
    qry_in[me] = qry_out[me]
    send(value_weight.at[0], val_pair.at[core], 16, {"tp": sibling})
    for y in range(n_chip):
        send(
            output_weight.at[:, block(2 * y + 1 - core)],
            ow_pair.at[y, head_rows],
            17,
            {"tp": sibling},
        )
    gate_copy.wait()

    def piece(ref, peer):
        return ref.at[:, pl.ds(pl.multiple_of(peer * cols, cols), cols)]

    def half_of(ref):
        return lambda peer: ref.at[lax.rem(peer, 2), me]

    send_tp(2, lambda peer: piece(gate_v, peer), half_of(gate_in))
    gate_in[core, me] = gate_v[:, my_cols]

    lat_copy.wait()
    rope_copy.wait()

    arrived(1, qry_in)
    key_sum = jnp.zeros((own, MESSAGE), F32)
    for h in range(n_tp):
        part = qry_in[h].astype(F32)
        key_sum = key_sum + part
        msg_f[own * h : own * (h + 1), :] = part
    key_raw = key_sum[:, KEY_AT : KEY_AT + latent]
    key_factor = lax.rsqrt(jnp.mean(key_raw * key_raw, axis=1, keepdims=True) + norm_floor)
    own_lat = (key_raw * key_factor * gain_row(latg_v, 0, latent)).astype(BF16)
    rope_raw = key_sum[:, KEY_ROT_AT : KEY_ROT_AT + QK_ROPE]
    own_rot = (rope_raw * own_cosine + swap_halves(rope_raw) * own_sine).astype(BF16)
    new_latent[...] = own_lat
    new_rope[...] = own_rot
    own_lat = own_lat.astype(F32)
    own_rot = own_rot.astype(F32)

    scale = (QK_NOPE + QK_ROPE) ** (-0.5)
    queries = msg_f[:, LAT_AT : LAT_AT + latent]
    rotated = msg_f[:, ROT_AT : ROT_AT + QK_ROPE]
    queries_b = queries.astype(BF16)
    rotated_b = rotated.astype(BF16)
    context = lat_v.shape[1]
    row_col = iota((rows, 1), 0)
    first = lax.rem(row_col, own) == 0

    def of_row(a, b):
        return jnp.where(first, a, b)

    scores = of_row(
        dot_t(queries_b, lat_v[0]) + dot(rotated_b, rope_v[0]),
        dot_t(queries_b, lat_v[1]) + dot(rotated_b, rope_v[1]),
    )
    row_len = of_row(own_lengths[0:1], own_lengths[1:2])
    valid = iota((rows, context), 1) < row_len
    scores = jnp.where(valid, scores * scale, masked_score)
    lat_rows = of_row(own_lat[0:1], own_lat[1:2])
    rot_rows = of_row(own_rot[0:1], own_rot[1:2])
    own_score = (
        jnp.sum(queries * lat_rows, axis=1, keepdims=True)
        + jnp.sum(rotated * rot_rows, axis=1, keepdims=True)
    ) * scale
    top = jnp.maximum(jnp.max(scores, axis=1, keepdims=True), own_score)
    weights = jnp.where(valid, jnp.exp(scores - top), 0.0)
    own_weight = jnp.exp(own_score - top)
    total = jnp.sum(weights, axis=1, keepdims=True) + own_weight
    summed = (
        dot(jnp.where(first, weights, 0.0).astype(BF16), lat_v[0])
        + dot(jnp.where(first, 0.0, weights).astype(BF16), lat_v[1])
        + own_weight.astype(BF16).astype(F32) * lat_rows
    )
    lat_f[...] = summed / total
    for y in range(n_chip):
        for c in range(2):
            at = own * (2 * y + c)
            att_out[y, :, c * latent : (c + 1) * latent] = lat_f[at : at + own, :].astype(BF16)

    send_tp(3, lambda peer: att_out.at[peer // 2], att_in.at[me])
    att_in[me] = att_out[chip]
    up_copy.wait()
    send_tp(4, lambda peer: piece(up_v, peer), half_of(up_in))
    up_in[core, me] = up_v[:, my_cols]
    val_copy.wait()
    pltpu.make_async_copy(
        ow_pair.at[:, head_rows], ow_pair.at[:, head_rows], local_sems.at[11]
    ).wait()
    arrived(16, val_pair)
    pltpu.make_async_copy(
        ow_pair.at[:, head_rows], ow_pair.at[:, head_rows], recv_sems.at[17]
    ).wait()

    arrived(3, att_in)
    for t in range(n_tp):
        msg_f[own * t : own * (t + 1), : 2 * latent] = att_in[t].astype(F32)
    results = msg_f[:, : 2 * latent].astype(BF16)
    head_values = jnp.concatenate(
        [dot(results[:, c * latent : (c + 1) * latent], val_pair[c]) for c in range(2)], axis=1
    ).astype(BF16)

    for batch in (chip_order[:3], chip_order[3:]):
        peers = [lax.rem(chip + d, n_chip) for d in batch]
        for peer in peers:
            mix_out[peer] = dot(head_values, ow_pair[peer]).astype(BF16)
        for peer in peers:
            send(mix_out.at[peer], mix_in.at[chip], 5, {"tp": 2 * peer + core})
    mix_in[chip] = dot(head_values, ow_pair[chip]).astype(BF16)

    arrived(2, gate_in.at[core])
    send(gate_in.at[core], gate_in.at[core], 13, {"tp": sibling})
    tok_cols = tok_f[:, my_cols]
    my_mix_gain = gain_row(mixg_v, my_first, cols)
    my_expert_gain = gain_row(expg_v, my_first, cols)

    arrived(5, mix_in)
    mixed = mix_in[0].astype(F32)
    for t in range(1, n_chip):
        mixed = mixed + mix_in[t].astype(F32)
    mixed = mixed.astype(BF16).astype(F32)
    scaled = mixed * my_mix_gain

    def as_row(col):
        return jnp.sum(eye * col, axis=0, keepdims=True)

    def as_col(row):
        return jnp.sum(eye * row, axis=1, keepdims=True)

    def row_sum(value):
        return as_row(jnp.sum(value, axis=1, keepdims=True))

    sums = jnp.concatenate(
        [
            row_sum(mixed * mixed),
            row_sum(tok_cols * scaled),
            row_sum(scaled * scaled),
            jnp.zeros((1, rows), F32),
        ],
        axis=1,
    )
    sum_in[me] = sums
    send_tp(6, lambda peer: sum_in.at[me], sum_in.at[me])
    arrived(4, up_in.at[core])
    send(up_in.at[core], up_in.at[core], 14, {"tp": sibling})
    arrived(6, sum_in)
    sums = sum_in[0]
    for t in range(1, n_tp):
        sums = sums + sum_in[t]
    mix_square = as_col(sums[:, 0:rows])
    cross = as_col(sums[:, rows : 2 * rows])
    scaled_square = as_col(sums[:, 2 * rows : 3 * rows])
    mix_factor = lax.rsqrt(mix_square / width + norm_floor)
    resid = (tok_cols + scaled * mix_factor).astype(BF16).astype(F32)
    resid_square = square_sum + mix_factor * (2.0 * cross + mix_factor * scaled_square)
    resid_factor = lax.rsqrt(jnp.maximum(resid_square, 0.0) / width + norm_floor)
    expert_in = (resid * resid_factor * my_expert_gain).astype(BF16)

    route_f[...] = dot(dispatch, expert_in)
    for e in range(n_ep):
        dis_out[e] = route_f[slots * e : slots * (e + 1), :].astype(BF16)
    place = 2 * (group // 2) + core

    for d in range(1, n_ep):
        peer = lax.rem(group + d, n_ep)
        send(dis_out.at[peer], dis_in.at[place], 7, {"ep": peer, "tp": 2 * chip + side})

    @pl.when(at_home)
    def _():
        dis_in[place] = dis_out[group]

    @pl.when(jnp.logical_not(at_home))
    def _():
        send(dis_out.at[group], dis_in.at[place], 7, {"tp": sibling})

    down_copy.wait()
    send_tp(8, lambda peer: piece(down_v, peer), half_of(down_in))
    down_in[core, me] = down_v[:, my_cols]

    arrived_all(13, gate_in.at[core])
    arrived_all(14, up_in.at[core])
    at_home_or_not(7, dis_in, recv_sems)
    side_rows = half_ep * slots
    for g in range(half_ep):
        for c in range(2):
            at = c * side_rows + slots * g
            route_f[at : at + slots, :] = dis_in[2 * g + c].astype(F32)
    received = [
        route_f[c * side_rows : (c + 1) * side_rows, :].astype(BF16) for c in range(2)
    ]
    ff = n_tp * ff_dev
    out_rows = side_rows // n_chip
    for n, source in enumerate((gate_in, up_in)):
        part = dot_t(received[0], source[0].reshape(ff, cols)) + dot_t(
            received[1], source[1].reshape(ff, cols)
        )
        part_out[:, :, n * ff : (n + 1) * ff] = part.reshape(n_chip, out_rows, ff).astype(BF16)

    send_chips(9, lambda peer: part_out.at[peer], part_in.at[chip])
    part_in[chip] = part_out[chip]
    arrived(9, part_in)
    both = part_in[0].astype(F32)
    for t in range(1, n_chip):
        both = both + part_in[t].astype(F32)
    gate, upward = both[:, :ff], both[:, ff:]
    hid_in[chip] = (gate / (1.0 + jnp.exp(-gate)) * upward).astype(BF16)

    send_chips(10, lambda peer: hid_in.at[chip], hid_in.at[chip])
    arrived(8, down_in.at[core])
    send(down_in.at[core], down_in.at[core], 15, {"tp": sibling})
    arrived_all(15, down_in.at[core])
    arrived(10, hid_in)
    hidden = hid_in[...].astype(F32).reshape(side_rows, ff).astype(BF16)
    for c in range(2):
        at = c * side_rows
        route_f[at : at + side_rows, :] = dot(hidden, down_in[c].reshape(ff, cols))
        for g in range(half_ep):
            at = c * side_rows + slots * g
            ret_out[2 * g + c] = route_f[at : at + slots, :].astype(BF16)

    for d in range(1, half_ep):
        pair = lax.rem(group // 2 + d, half_ep)
        for c in range(2):
            send(
                ret_out.at[2 * pair + c],
                ret_in.at[group],
                11,
                {"ep": 2 * pair + core, "tp": 2 * chip + c},
            )

    @pl.when(at_home)
    def _():
        ret_in[group] = ret_out[place]
        send(ret_out.at[place + 1 - 2 * core], ret_in.at[group], 11, {"tp": sibling})

    @pl.when(jnp.logical_not(at_home))
    def _():
        for c in range(2):
            send(
                ret_out.at[2 * (group // 2) + c],
                ret_in.at[group],
                11,
                {"ep": 2 * (group // 2) + core, "tp": 2 * chip + c},
            )

    at_home_or_not(11, ret_in, recv_sems)
    for e in range(n_ep):
        route_f[slots * e : slots * (e + 1), :] = ret_in[e].astype(F32)
    out[...] = (resid + dot(combine, route_f[...], HIGHEST)).astype(BF16)

    sent(0, tok_in)
    for stage, buffer in (
        (1, qry_in),
        (2, gate_in.at[core]),
        (3, att_in),
        (4, up_in.at[core]),
        (5, mix_in),
        (6, sum_in),
        (8, down_in.at[core]),
        (9, part_in),
        (10, hid_in),
        (16, val_pair),
    ):
        sent(stage, buffer)
    sent_all(13, gate_in.at[core])
    sent_all(14, up_in.at[core])
    sent_all(15, down_in.at[core])
    sent_all(17, ow_pair.at[:, head_rows])
    at_home_or_not(7, dis_in, send_sems)
    at_home_or_not(11, ret_in, send_sems)


def hand_over(*refs):
    sources, targets, sems = refs[:3], refs[3:6], refs[6]
    copies = [
        pltpu.make_async_copy(a, b, sems.at[i]) for i, (a, b) in enumerate(zip(sources, targets))
    ]
    for copy in copies:
        copy.start()
    for copy in copies:
        copy.wait()


def per_device(
    tokens,
    lengths,
    latent_cache,
    rope_cache,
    attn_gain,
    query_weight,
    query_rot_weight,
    latent_weight,
    key_rot_weight,
    latent_gain,
    absorb_weight,
    value_weight,
    output_weight,
    mix_gain,
    expert_gain,
    gate_weight,
    up_weight,
    down_weight,
    expert_ids,
    route_weights,
):
    n_tp, n_ep = lax.axis_size("tp"), lax.axis_size("ep")
    own, width = tokens.shape
    rows = own * n_tp
    cols = width // n_tp
    latent = latent_weight.shape[1]
    context = latent_cache.shape[1]
    ff_dev = gate_weight.shape[2]
    ff = ff_dev * n_tp
    slots = 2 * rows * expert_ids.shape[1] // n_ep
    all_slots = n_ep * slots
    n_chip = n_tp // 2
    out_rows = all_slots // n_tp

    operands = (
        tokens,
        lengths.reshape(1, rows),
        latent_cache,
        jnp.swapaxes(rope_cache, 1, 2),
        attn_gain,
        mix_gain,
        expert_gain,
        latent_gain,
        query_weight,
        query_rot_weight.T,
        latent_weight,
        key_rot_weight.T,
        absorb_weight,
        value_weight,
        output_weight,
        jnp.swapaxes(gate_weight, 1, 2),
        jnp.swapaxes(up_weight, 1, 2),
        down_weight,
        expert_ids.T,
        route_weights.T,
    )
    vmem = pltpu.VMEM
    shapes = (
        jax.ShapeDtypeStruct((rows, cols), BF16),
        jax.ShapeDtypeStruct((own, latent), BF16),
        jax.ShapeDtypeStruct((own, QK_ROPE), BF16),
    )
    results = pl.pallas_call(
        functools.partial(kernel, n_tp, n_ep),
        out_shape=shapes,
        in_specs=[
            pl.BlockSpec(memory_space=pltpu.HBM) for _ in operands
        ],
        out_specs=[pl.BlockSpec(memory_space=vmem)] * 3,
        scratch_shapes=[
            vmem((1, rows), jnp.int32),
            vmem(expert_ids.shape[::-1], jnp.int32),
            vmem(route_weights.shape[::-1], F32),
            vmem((width,), BF16),
            vmem((width,), BF16),
            vmem((width,), BF16),
            vmem((latent,), BF16),
            vmem(latent_cache.shape, BF16),
            vmem((own, QK_ROPE, context), BF16),
            vmem((width, QK_NOPE + QK_ROPE), BF16),
            vmem((QK_ROPE, width), BF16),
            vmem(latent_weight.shape, BF16),
            vmem((QK_ROPE, cols), BF16),
            vmem(absorb_weight.shape[1:], BF16),
            vmem((2, *value_weight.shape[1:]), BF16),
            vmem((n_chip, 2 * output_weight.shape[0], cols), BF16),
            vmem((ff_dev, width), BF16),
            vmem((ff_dev, width), BF16),
            vmem((ff_dev, width), BF16),
            vmem((rows, width), F32),
            vmem((rows, width), BF16),
            vmem((rows, MESSAGE), F32),
            vmem((rows, latent), F32),
            vmem((all_slots, cols), F32),
            vmem((n_tp, own, width), BF16),
            vmem((n_tp, own, MESSAGE), BF16),
            vmem((n_tp, own, MESSAGE), BF16),
            vmem((n_chip, own, 2 * latent), BF16),
            vmem((n_tp, own, 2 * latent), BF16),
            vmem((n_chip, rows, cols), BF16),
            vmem((n_chip, rows, cols), BF16),
            vmem((n_tp, 1, 4 * rows), F32),
            vmem((n_ep, slots, cols), BF16),
            vmem((n_ep, slots, cols), BF16),
            vmem((n_chip, out_rows, 2 * ff), BF16),
            vmem((n_chip, out_rows, 2 * ff), BF16),
            vmem((n_chip, out_rows, ff), BF16),
            vmem((n_ep, slots, cols), BF16),
            vmem((n_ep, slots, cols), BF16),
            vmem((2, n_tp, ff_dev, cols), BF16),
            vmem((2, n_tp, ff_dev, cols), BF16),
            vmem((2, n_tp, ff_dev, cols), BF16),
            pltpu.SemaphoreType.DMA((20,)),
            pltpu.SemaphoreType.DMA((18,)),
            pltpu.SemaphoreType.DMA((18,)),
            pltpu.SemaphoreType.DMA((n_chip,)),
        ],
        compiler_params=pltpu.CompilerParams(
            collective_id=0, has_side_effects=True, vmem_limit_bytes=40 * 1024 * 1024
        ),
    )(*[pltpu.with_memory_space_constraint(x, pltpu.HBM) for x in operands])
    return pl.pallas_call(
        hand_over,
        out_shape=shapes,
        in_specs=[pl.BlockSpec(memory_space=vmem)] * 3,
        out_specs=[pl.BlockSpec(memory_space=pltpu.HBM)] * 3,
        scratch_shapes=[pltpu.SemaphoreType.DMA((3,))],
        compiler_params=pltpu.CompilerParams(vmem_limit_bytes=16 * 1024 * 1024),
    )(*results)


def solution(mesh):
    placed = (
        P(("ep", "tp"), None),
        P("ep"),
        P(("ep", "tp"), None, None),
        P(("ep", "tp"), None, None),
        P(),
        P(None, "tp"),
        P(None, "tp"),
        P("tp", None),
        P("tp", None),
        P(),
        P("tp", None, None),
        P("tp", None, None),
        P("tp", None),
        P(),
        P(),
        P("ep", None, "tp"),
        P("ep", None, "tp"),
        P("ep", "tp", None),
        P("ep", None),
        P("ep", None),
    )
    return jax.shard_map(
        per_device,
        mesh=mesh,
        in_specs=placed,
        out_specs=(P("ep", "tp"), P(("ep", "tp"), None), P(("ep", "tp"), None)),
        check_vma=False,
    )
```

```python
import functools

import jax
import jax.numpy as jnp
import numpy as np
from jax import lax
from jax.experimental import pallas as pl
from jax.experimental.pallas import tpu as pltpu
from jax.sharding import PartitionSpec as P

MESH = pl.DeviceIdType.MESH
F32 = jnp.float32
BF16 = jnp.bfloat16
HIGHEST = lax.Precision.HIGHEST

QK_NOPE = 128
QK_ROPE = 64
norm_floor = 1e-06
rope_base = 10000.0
masked_score = -1e30

LAT_AT, KEY_AT, ROT_AT, KEY_ROT_AT, MESSAGE = 0, 256, 512, 640, 768


def dot(a, b, precision=None):
    return lax.dot_general(
        a, b, (((1,), (0,)), ((), ())), preferred_element_type=F32, precision=precision
    )


def dot_t(a, b, precision=None):
    return lax.dot_general(
        a, b, (((1,), (1,)), ((), ())), preferred_element_type=F32, precision=precision
    )


def swap_halves(x):
    half = x.shape[-1] // 2
    return jnp.concatenate([x[:, half:], x[:, :half]], axis=1)


def gain_row(ref, first, size):
    return ref[pl.ds(first, size)].astype(F32).reshape(1, size)


def cos_sin(x):
    return jnp.cos(x), jnp.sin(x)


def iota(shape, dim):
    return lax.broadcasted_iota(jnp.int32, shape, dim)


def kernel(
    n_tp,
    n_ep,
    tokens,
    lengths,
    latent_cache,
    rope_cache,
    attn_gain,
    mix_gain,
    expert_gain,
    latent_gain,
    query_weight,
    query_rot_weight,
    latent_weight,
    key_rot_weight,
    absorb_weight,
    value_weight,
    output_weight,
    gate_weight,
    up_weight,
    down_weight,
    expert_ids,
    route_weights,
    out,
    new_latent,
    new_rope,
    len_v,
    ids_v,
    rw_v,
    attn_v,
    mixg_v,
    expg_v,
    latg_v,
    lat_v,
    rope_v,
    query_v,
    qrw_v,
    lw_v,
    krw_v,
    abs_v,
    val_pair,
    ow_pair,
    gate_v,
    up_v,
    down_v,
    tok_f,
    normed_b,
    msg_f,
    lat_f,
    route_f,
    factor_f,
    tok_in,
    qry_out,
    qry_in,
    att_out,
    att_in,
    mix_out,
    mix_in,
    sum_in,
    dis_out,
    dis_in,
    part_out,
    part_in,
    tok_dis_out,
    tok_dis_in,
    tok_part_out,
    tok_part_in,
    factor_out,
    factor_in,
    hid_in,
    ret_out,
    ret_in,
    gate_in,
    up_in,
    down_in,
    local_sems,
    send_sems,
    recv_sems,
    tok_sems,
):
    me = lax.axis_index("tp")
    group = lax.axis_index("ep")
    rows = tok_f.shape[0]
    own = rows // n_tp
    width = tok_f.shape[1]
    cols = width // n_tp
    slots = dis_out.shape[1]
    ff_dev = gate_v.shape[0]
    latent = abs_v.shape[1]
    my_first = pl.multiple_of(me * cols, cols)
    my_cols = pl.ds(my_first, cols)
    n_chip = n_tp // 2
    half_ep = n_ep // 2
    chip = me // 2
    core = lax.rem(me, 2)
    sibling = me + 1 - 2 * core
    side = lax.rem(group, 2)
    at_home = side == core

    def load(index, src, dst):
        copy = pltpu.make_async_copy(src, dst, local_sems.at[index])
        copy.start()
        return copy

    tok_copy = load(0, tokens, tok_in.at[me])

    barrier = pltpu.get_barrier_semaphore()

    def greet(device):
        pl.semaphore_signal(barrier, inc=1, device_id=device, device_id_type=MESH)

    for d in range(1, n_tp):
        greet({"tp": lax.rem(me + d, n_tp)})

    for d in range(1, n_ep):
        greet({"ep": lax.rem(group + d, n_ep), "tp": 2 * chip + side})

    @pl.when(jnp.logical_not(at_home))
    def _():
        greet({"tp": sibling})

    for d in range(half_ep):
        greet({"ep": 2 * d + core, "tp": 2 * chip + 1 - side})

    small = [
        load(13, lengths, len_v),
        load(14, expert_ids, ids_v),
        load(15, route_weights, rw_v),
        load(16, attn_gain, attn_v),
        load(17, mix_gain, mixg_v),
        load(18, expert_gain, expg_v),
        load(19, latent_gain, latg_v),
    ]
    qw_copy = load(1, query_weight, query_v.at[:, pl.ds(0, QK_NOPE)])
    qrw_copy = load(2, query_rot_weight, qrw_v)
    lw_copy = load(3, latent_weight, lw_v)
    krw_copy = load(4, key_rot_weight, krw_v)
    abs_copy = load(5, absorb_weight.at[0], abs_v)
    gate_copy = load(6, gate_weight.at[0], gate_v)
    up_copy = load(7, up_weight.at[0], up_v)
    lat_copy = load(8, latent_cache, lat_v)
    rope_copy = load(9, rope_cache, rope_v)
    val_copy = load(10, value_weight.at[0], val_pair.at[core])
    value_dim = value_weight.shape[2]
    head_rows = pl.ds(pl.multiple_of(core * value_dim, value_dim), value_dim)

    def block(index):
        return pl.ds(pl.multiple_of(index * cols, cols), cols)

    for y in range(n_chip):
        pltpu.make_async_copy(
            output_weight.at[:, block(2 * y + core)],
            ow_pair.at[y, head_rows],
            local_sems.at[11],
        ).start()
    down_copy = load(12, down_weight.at[0], down_v)

    pl.semaphore_wait(
        barrier, n_tp - 1 + n_ep + half_ep - jnp.where(at_home, 1, 0)
    )

    order = sorted(range(1, n_tp), key=lambda d: -min(d, n_tp - d))
    chip_order = sorted(range(1, n_chip), key=lambda d: -min(d, n_chip - d))

    def send(src, dst, stage, device, recv_sem=None):
        pltpu.make_async_remote_copy(
            src_ref=src,
            dst_ref=dst,
            send_sem=send_sems.at[stage],
            recv_sem=recv_sems.at[stage] if recv_sem is None else recv_sem,
            device_id=device,
            device_id_type=MESH,
        ).start()

    def send_tp(stage, src_of, dst):
        for d in order:
            peer = lax.rem(me + d, n_tp)
            send(src_of(peer), dst(peer) if callable(dst) else dst, stage, {"tp": peer})

    def send_chips(stage, src_of, dst):
        for d in chip_order:
            peer = lax.rem(chip + d, n_chip)
            send(src_of(peer), dst, stage, {"tp": 2 * peer + core})

    def wait_for(sem, buffer, count):
        some = buffer.at[pl.ds(0, count)]
        pltpu.make_async_copy(some, some, sem).wait()

    def arrived(stage, buffer, count=None):
        wait_for(recv_sems.at[stage], buffer, buffer.shape[0] - 1 if count is None else count)

    def sent(stage, buffer, count=None):
        wait_for(send_sems.at[stage], buffer, buffer.shape[0] - 1 if count is None else count)

    def arrived_all(stage, buffer):
        pltpu.make_async_copy(buffer, buffer, recv_sems.at[stage]).wait()

    def sent_all(stage, buffer):
        pltpu.make_async_copy(buffer, buffer, send_sems.at[stage]).wait()

    def at_home_or_not(stage, buffer, sems):
        count = buffer.shape[0]

        @pl.when(at_home)
        def _():
            wait_for(sems.at[stage], buffer, count - 1)

        @pl.when(jnp.logical_not(at_home))
        def _():
            wait_for(sems.at[stage], buffer, count)

    tok_copy.wait()
    send(tok_in.at[me], tok_in.at[me], 0, {"tp": sibling}, recv_sems.at[12])
    for d in chip_order:
        peer = lax.rem(chip + d, n_chip)
        send(tok_in.at[me], tok_in.at[me], 0, {"tp": 2 * peer + core}, tok_sems.at[chip])

    square = (rows, rows)
    eye = (iota(square, 0) == iota(square, 1)).astype(F32)
    ahead_row = iota(square, 0) < iota(square, 1)
    ahead_col = iota(square, 1) < iota(square, 0)
    for copy in small:
        copy.wait()
    ids = ids_v[...].astype(F32)
    weights_row = rw_v[...]
    id_rows = [ids[k : k + 1, :] for k in range(2)]
    id_cols = [jnp.sum(eye * r, axis=1, keepdims=True) for r in id_rows]
    weight_cols = [
        jnp.sum(eye * weights_row[k : k + 1, :], axis=1, keepdims=True) for k in range(2)
    ]

    def same(j, k):
        return id_cols[j] == id_rows[k]

    def count(mask, axis):
        return jnp.sum(jnp.where(mask, 1.0, 0.0), axis=axis, keepdims=True)

    rank_row0 = count(same(0, 0) & ahead_row, 0)
    rank_row1 = count(same(0, 1), 0) + count(same(1, 1) & ahead_row, 0)
    rank_col0 = count(same(0, 0) & ahead_col, 1)
    rank_col1 = count(same(1, 0), 1) + count(same(1, 1) & ahead_col, 1)
    target_rows = [id_rows[0] * slots + rank_row0, id_rows[1] * slots + rank_row1]
    target_cols = [id_cols[0] * slots + rank_col0, id_cols[1] * slots + rank_col1]
    all_slots = n_ep * slots
    down_iota = iota((all_slots, rows), 0).astype(F32)
    across_iota = iota((rows, all_slots), 1).astype(F32)
    dispatch = (
        jnp.where(down_iota == target_rows[0], 1.0, 0.0)
        + jnp.where(down_iota == target_rows[1], 1.0, 0.0)
    ).astype(BF16)
    combine = jnp.where(across_iota == target_cols[0], weight_cols[0], 0.0) + jnp.where(
        across_iota == target_cols[1], weight_cols[1], 0.0
    )

    half = QK_ROPE // 2
    freqs = jnp.zeros((1, QK_ROPE), F32)
    lane = lax.rem(iota((1, QK_ROPE), 1), half)
    for i in range(half):
        freqs = jnp.where(lane == i, float(np.float32(rope_base ** (-i / half))), freqs)
    lengths_row = len_v[...].astype(F32)
    lengths_col = jnp.sum(eye * lengths_row, axis=1, keepdims=True)
    cosine, sine = cos_sin(lengths_col * freqs)
    sine = jnp.where(iota((1, QK_ROPE), 1) < half, -sine, sine)
    own_rows = (iota((8, rows), 1) == own * me + iota((8, rows), 0)).astype(F32)
    own_cosine = dot(own_rows, cosine, HIGHEST)[:own]
    own_sine = dot(own_rows, sine, HIGHEST)[:own]
    own_lengths = jnp.sum(own_rows * lengths_row, axis=1, keepdims=True).astype(jnp.int32)

    qrw_copy.wait()
    for c in range(0, width, 512):
        query_v[c : c + 512, QK_NOPE : QK_NOPE + QK_ROPE] = qrw_v[:, c : c + 512].T
    qw_copy.wait()
    for d in reversed(chip_order):
        peer = lax.rem(chip + d, n_chip)
        slot = tok_in.at[2 * peer + core]
        pltpu.make_async_copy(slot, slot, tok_sems.at[peer]).wait()
        send(slot, slot, 0, {"tp": sibling}, recv_sems.at[12])
    arrived(12, tok_in, n_chip)
    for t in range(n_tp):
        tok_f[own * t : own * (t + 1), :] = tok_in[t].astype(F32)
    chunk = 512
    square_sum = jnp.zeros((rows, 1), F32)
    for c in range(0, width, chunk):
        x = tok_f[:, c : c + chunk]
        square_sum = square_sum + jnp.sum(x * x, axis=1, keepdims=True)
    factor = lax.rsqrt(square_sum / width + norm_floor)
    for c in range(0, width, chunk):
        x = tok_f[:, c : c + chunk]
        normed_b[:, c : c + chunk] = (x * factor * gain_row(attn_v, c, chunk)).astype(BF16)

    mid = width // 2
    query = dot(normed_b[:, :mid], query_v[:mid]) + dot(normed_b[:, mid:], query_v[mid:])
    q_nope = query[:, :QK_NOPE].astype(BF16)
    q_rot = query[:, QK_NOPE : QK_NOPE + QK_ROPE]
    abs_copy.wait()
    msg_f[:, LAT_AT : LAT_AT + latent] = dot(q_nope, abs_v[...])
    msg_f[:, ROT_AT : ROT_AT + QK_ROPE] = q_rot * cosine + swap_halves(q_rot) * sine
    slice_rows = normed_b[:, my_cols]
    lw_copy.wait()
    msg_f[:, KEY_AT : KEY_AT + latent] = dot(slice_rows, lw_v[...])
    krw_copy.wait()
    msg_f[:, KEY_ROT_AT : KEY_ROT_AT + QK_ROPE] = dot_t(slice_rows, krw_v[...])
    for t in range(n_tp):
        qry_out[t] = msg_f[own * t : own * (t + 1), :].astype(BF16)

    send_tp(1, lambda peer: qry_out.at[peer], qry_in.at[me])
    qry_in[me] = qry_out[me]
    send(value_weight.at[0], val_pair.at[core], 16, {"tp": sibling})
    for y in range(n_chip):
        send(
            output_weight.at[:, block(2 * y + 1 - core)],
            ow_pair.at[y, head_rows],
            17,
            {"tp": sibling},
        )
    gate_copy.wait()

    def piece(ref, peer):
        return ref.at[:, pl.ds(pl.multiple_of(peer * cols, cols), cols)]

    def half_of(ref):
        return lambda peer: ref.at[lax.rem(peer, 2), me]

    send_tp(2, lambda peer: piece(gate_v, peer), half_of(gate_in))
    gate_in[core, me] = gate_v[:, my_cols]

    tok_cols = tok_f[:, my_cols]
    my_mix_gain = gain_row(mixg_v, my_first, cols)
    my_expert_gain = gain_row(expg_v, my_first, cols)
    place = 2 * (group // 2) + core

    def to_experts(stage, value, out_ref, in_ref):
        route_f[...] = dot(dispatch, value.astype(BF16))
        for e in range(n_ep):
            out_ref[e] = route_f[slots * e : slots * (e + 1), :].astype(BF16)
        for d in range(1, n_ep):
            peer = lax.rem(group + d, n_ep)
            send(out_ref.at[peer], in_ref.at[place], stage, {"ep": peer, "tp": 2 * chip + side})

        @pl.when(at_home)
        def _():
            in_ref[place] = out_ref[group]

        @pl.when(jnp.logical_not(at_home))
        def _():
            send(out_ref.at[group], in_ref.at[place], stage, {"tp": sibling})

    to_experts(18, tok_cols * my_expert_gain, tok_dis_out, tok_dis_in)

    lat_copy.wait()
    rope_copy.wait()

    arrived(1, qry_in)
    key_sum = jnp.zeros((own, MESSAGE), F32)
    for h in range(n_tp):
        part = qry_in[h].astype(F32)
        key_sum = key_sum + part
        msg_f[own * h : own * (h + 1), :] = part
    key_raw = key_sum[:, KEY_AT : KEY_AT + latent]
    key_factor = lax.rsqrt(jnp.mean(key_raw * key_raw, axis=1, keepdims=True) + norm_floor)
    own_lat = (key_raw * key_factor * gain_row(latg_v, 0, latent)).astype(BF16)
    rope_raw = key_sum[:, KEY_ROT_AT : KEY_ROT_AT + QK_ROPE]
    own_rot = (rope_raw * own_cosine + swap_halves(rope_raw) * own_sine).astype(BF16)
    new_latent[...] = own_lat
    new_rope[...] = own_rot
    own_lat = own_lat.astype(F32)
    own_rot = own_rot.astype(F32)

    scale = (QK_NOPE + QK_ROPE) ** (-0.5)
    queries = msg_f[:, LAT_AT : LAT_AT + latent]
    rotated = msg_f[:, ROT_AT : ROT_AT + QK_ROPE]
    queries_b = queries.astype(BF16)
    rotated_b = rotated.astype(BF16)
    context = lat_v.shape[1]
    row_col = iota((rows, 1), 0)
    first = lax.rem(row_col, own) == 0

    def of_row(a, b):
        return jnp.where(first, a, b)

    scores = of_row(
        dot_t(queries_b, lat_v[0]) + dot(rotated_b, rope_v[0]),
        dot_t(queries_b, lat_v[1]) + dot(rotated_b, rope_v[1]),
    )
    row_len = of_row(own_lengths[0:1], own_lengths[1:2])
    valid = iota((rows, context), 1) < row_len
    scores = jnp.where(valid, scores * scale, masked_score)
    lat_rows = of_row(own_lat[0:1], own_lat[1:2])
    rot_rows = of_row(own_rot[0:1], own_rot[1:2])
    own_score = (
        jnp.sum(queries * lat_rows, axis=1, keepdims=True)
        + jnp.sum(rotated * rot_rows, axis=1, keepdims=True)
    ) * scale
    top = jnp.maximum(jnp.max(scores, axis=1, keepdims=True), own_score)
    weights = jnp.where(valid, jnp.exp(scores - top), 0.0)
    own_weight = jnp.exp(own_score - top)
    total = jnp.sum(weights, axis=1, keepdims=True) + own_weight
    summed = (
        dot(jnp.where(first, weights, 0.0).astype(BF16), lat_v[0])
        + dot(jnp.where(first, 0.0, weights).astype(BF16), lat_v[1])
        + own_weight.astype(BF16).astype(F32) * lat_rows
    )
    lat_f[...] = summed / total
    for y in range(n_chip):
        for c in range(2):
            at = own * (2 * y + c)
            att_out[y, :, c * latent : (c + 1) * latent] = lat_f[at : at + own, :].astype(BF16)

    send_tp(3, lambda peer: att_out.at[peer // 2], att_in.at[me])
    att_in[me] = att_out[chip]
    up_copy.wait()
    send_tp(4, lambda peer: piece(up_v, peer), half_of(up_in))
    up_in[core, me] = up_v[:, my_cols]
    val_copy.wait()
    pltpu.make_async_copy(
        ow_pair.at[:, head_rows], ow_pair.at[:, head_rows], local_sems.at[11]
    ).wait()
    arrived(16, val_pair)
    pltpu.make_async_copy(
        ow_pair.at[:, head_rows], ow_pair.at[:, head_rows], recv_sems.at[17]
    ).wait()

    arrived(3, att_in)
    for t in range(n_tp):
        msg_f[own * t : own * (t + 1), : 2 * latent] = att_in[t].astype(F32)
    results = msg_f[:, : 2 * latent].astype(BF16)
    head_values = jnp.concatenate(
        [dot(results[:, c * latent : (c + 1) * latent], val_pair[c]) for c in range(2)], axis=1
    ).astype(BF16)

    for batch in (chip_order[:3], chip_order[3:]):
        peers = [lax.rem(chip + d, n_chip) for d in batch]
        for peer in peers:
            mix_out[peer] = dot(head_values, ow_pair[peer]).astype(BF16)
        for peer in peers:
            send(mix_out.at[peer], mix_in.at[chip], 5, {"tp": 2 * peer + core})
    mix_in[chip] = dot(head_values, ow_pair[chip]).astype(BF16)

    arrived(2, gate_in.at[core])
    send(gate_in.at[core], gate_in.at[core], 13, {"tp": sibling})
    arrived(4, up_in.at[core])
    send(up_in.at[core], up_in.at[core], 14, {"tp": sibling})
    side_rows = half_ep * slots
    ff = n_tp * ff_dev
    out_rows = side_rows // n_chip

    def partial_sums(in_ref, out_ref):
        for g in range(half_ep):
            for c in range(2):
                at = c * side_rows + slots * g
                route_f[at : at + slots, :] = in_ref[2 * g + c].astype(F32)
        received = [
            route_f[c * side_rows : (c + 1) * side_rows, :].astype(BF16) for c in range(2)
        ]
        for n, source in enumerate((gate_in, up_in)):
            part = dot_t(received[0], source[0].reshape(ff, cols)) + dot_t(
                received[1], source[1].reshape(ff, cols)
            )
            out_ref[:, :, n * ff : (n + 1) * ff] = part.reshape(n_chip, out_rows, ff).astype(BF16)

    def summed_parts(in_ref):
        both = in_ref[0].astype(F32)
        for t in range(1, n_chip):
            both = both + in_ref[t].astype(F32)
        return both

    at_home_or_not(18, tok_dis_in, recv_sems)
    arrived_all(13, gate_in.at[core])
    arrived_all(14, up_in.at[core])
    partial_sums(tok_dis_in, tok_part_out)
    send_chips(19, lambda peer: tok_part_out.at[peer], tok_part_in.at[chip])
    tok_part_in[chip] = tok_part_out[chip]

    arrived(5, mix_in)
    mixed = mix_in[0].astype(F32)
    for t in range(1, n_chip):
        mixed = mixed + mix_in[t].astype(F32)
    mixed = mixed.astype(BF16).astype(F32)
    scaled = mixed * my_mix_gain

    to_experts(7, scaled * my_expert_gain, dis_out, dis_in)

    def as_row(col):
        return jnp.sum(eye * col, axis=0, keepdims=True)

    def as_col(row):
        return jnp.sum(eye * row, axis=1, keepdims=True)

    def row_sum(value):
        return as_row(jnp.sum(value, axis=1, keepdims=True))

    sums = jnp.concatenate(
        [
            row_sum(mixed * mixed),
            row_sum(tok_cols * scaled),
            row_sum(scaled * scaled),
            jnp.zeros((1, rows), F32),
        ],
        axis=1,
    )
    sum_in[me] = sums
    send_tp(6, lambda peer: sum_in.at[me], sum_in.at[me])
    down_copy.wait()
    send_tp(8, lambda peer: piece(down_v, peer), half_of(down_in))
    down_in[core, me] = down_v[:, my_cols]

    arrived(6, sum_in)
    sums = sum_in[0]
    for t in range(1, n_tp):
        sums = sums + sum_in[t]
    mix_square = as_col(sums[:, 0:rows])
    cross = as_col(sums[:, rows : 2 * rows])
    scaled_square = as_col(sums[:, 2 * rows : 3 * rows])
    mix_factor = lax.rsqrt(mix_square / width + norm_floor)
    resid = (tok_cols + scaled * mix_factor).astype(BF16).astype(F32)
    resid_square = square_sum + mix_factor * (2.0 * cross + mix_factor * scaled_square)
    resid_factor = lax.rsqrt(jnp.maximum(resid_square, 0.0) / width + norm_floor)

    lanes = iota((rows, 128), 1)
    factors = jnp.where(lanes < 64, mix_factor, resid_factor)
    factor_f[...] = dot(dispatch.astype(F32), factors, HIGHEST)
    for e in range(n_ep):
        factor_out[e] = factor_f[slots * e : slots * (e + 1), :]
    per_device_groups = out_rows // slots
    speaks = me == 2 * (group // (2 * per_device_groups)) + side
    factor_place = lax.rem(group // 2, per_device_groups)

    @pl.when(speaks)
    def _():
        for d in range(1, n_ep):
            peer = lax.rem(group + d, n_ep)
            send(factor_out.at[peer], factor_in.at[factor_place], 20, {"ep": peer})
        factor_in[factor_place] = factor_out[group]

    at_home_or_not(7, dis_in, recv_sems)
    partial_sums(dis_in, part_out)

    send_chips(9, lambda peer: part_out.at[peer], part_in.at[chip])
    part_in[chip] = part_out[chip]
    arrived(9, part_in)
    arrived(19, tok_part_in)

    @pl.when(speaks)
    def _():
        wait_for(recv_sems.at[20], factor_in, per_device_groups - 1)

    @pl.when(jnp.logical_not(speaks))
    def _():
        wait_for(recv_sems.at[20], factor_in, per_device_groups)

    for g in range(per_device_groups):
        factor_f[slots * g : slots * (g + 1), :] = factor_in[g]
    mix_factors = factor_f[:out_rows, 0:1]
    resid_factors = factor_f[:out_rows, 64:65]
    both = (summed_parts(tok_part_in) + mix_factors * summed_parts(part_in)) * resid_factors
    gate, upward = both[:, :ff], both[:, ff:]
    hid_in[chip] = (gate / (1.0 + jnp.exp(-gate)) * upward).astype(BF16)

    send_chips(10, lambda peer: hid_in.at[chip], hid_in.at[chip])
    arrived(8, down_in.at[core])
    send(down_in.at[core], down_in.at[core], 15, {"tp": sibling})
    arrived_all(15, down_in.at[core])
    arrived(10, hid_in)
    hidden = hid_in[...].astype(F32).reshape(side_rows, ff).astype(BF16)
    for c in range(2):
        at = c * side_rows
        route_f[at : at + side_rows, :] = dot(hidden, down_in[c].reshape(ff, cols))
        for g in range(half_ep):
            at = c * side_rows + slots * g
            ret_out[2 * g + c] = route_f[at : at + slots, :].astype(BF16)

    for d in range(1, half_ep):
        pair = lax.rem(group // 2 + d, half_ep)
        for c in range(2):
            send(
                ret_out.at[2 * pair + c],
                ret_in.at[group],
                11,
                {"ep": 2 * pair + core, "tp": 2 * chip + c},
            )

    @pl.when(at_home)
    def _():
        ret_in[group] = ret_out[place]
        send(ret_out.at[place + 1 - 2 * core], ret_in.at[group], 11, {"tp": sibling})

    @pl.when(jnp.logical_not(at_home))
    def _():
        for c in range(2):
            send(
                ret_out.at[2 * (group // 2) + c],
                ret_in.at[group],
                11,
                {"ep": 2 * (group // 2) + core, "tp": 2 * chip + c},
            )

    at_home_or_not(11, ret_in, recv_sems)
    for e in range(n_ep):
        route_f[slots * e : slots * (e + 1), :] = ret_in[e].astype(F32)
    out[...] = (resid + dot(combine, route_f[...], HIGHEST)).astype(BF16)

    sent(0, tok_in)
    for stage, buffer in (
        (1, qry_in),
        (2, gate_in.at[core]),
        (3, att_in),
        (4, up_in.at[core]),
        (5, mix_in),
        (6, sum_in),
        (8, down_in.at[core]),
        (9, part_in),
        (10, hid_in),
        (16, val_pair),
        (19, tok_part_in),
    ):
        sent(stage, buffer)
    sent_all(13, gate_in.at[core])
    sent_all(14, up_in.at[core])
    sent_all(15, down_in.at[core])
    sent_all(17, ow_pair.at[:, head_rows])
    at_home_or_not(7, dis_in, send_sems)
    at_home_or_not(18, tok_dis_in, send_sems)

    @pl.when(speaks)
    def _():
        sent(20, factor_out)

    at_home_or_not(11, ret_in, send_sems)


def hand_over(*refs):
    sources, targets, sems = refs[:3], refs[3:6], refs[6]
    copies = [
        pltpu.make_async_copy(a, b, sems.at[i]) for i, (a, b) in enumerate(zip(sources, targets))
    ]
    for copy in copies:
        copy.start()
    for copy in copies:
        copy.wait()


def per_device(
    tokens,
    lengths,
    latent_cache,
    rope_cache,
    attn_gain,
    query_weight,
    query_rot_weight,
    latent_weight,
    key_rot_weight,
    latent_gain,
    absorb_weight,
    value_weight,
    output_weight,
    mix_gain,
    expert_gain,
    gate_weight,
    up_weight,
    down_weight,
    expert_ids,
    route_weights,
):
    n_tp, n_ep = lax.axis_size("tp"), lax.axis_size("ep")
    own, width = tokens.shape
    rows = own * n_tp
    cols = width // n_tp
    latent = latent_weight.shape[1]
    context = latent_cache.shape[1]
    ff_dev = gate_weight.shape[2]
    ff = ff_dev * n_tp
    slots = 2 * rows * expert_ids.shape[1] // n_ep
    all_slots = n_ep * slots
    n_chip = n_tp // 2
    out_rows = all_slots // n_tp

    operands = (
        tokens,
        lengths.reshape(1, rows),
        latent_cache,
        jnp.swapaxes(rope_cache, 1, 2),
        attn_gain,
        mix_gain,
        expert_gain,
        latent_gain,
        query_weight,
        query_rot_weight.T,
        latent_weight,
        key_rot_weight.T,
        absorb_weight,
        value_weight,
        output_weight,
        jnp.swapaxes(gate_weight, 1, 2),
        jnp.swapaxes(up_weight, 1, 2),
        down_weight,
        expert_ids.T,
        route_weights.T,
    )
    vmem = pltpu.VMEM
    shapes = (
        jax.ShapeDtypeStruct((rows, cols), BF16),
        jax.ShapeDtypeStruct((own, latent), BF16),
        jax.ShapeDtypeStruct((own, QK_ROPE), BF16),
    )
    results = pl.pallas_call(
        functools.partial(kernel, n_tp, n_ep),
        out_shape=shapes,
        in_specs=[
            pl.BlockSpec(memory_space=pltpu.HBM) for _ in operands
        ],
        out_specs=[pl.BlockSpec(memory_space=vmem)] * 3,
        scratch_shapes=[
            vmem((1, rows), jnp.int32),
            vmem(expert_ids.shape[::-1], jnp.int32),
            vmem(route_weights.shape[::-1], F32),
            vmem((width,), BF16),
            vmem((width,), BF16),
            vmem((width,), BF16),
            vmem((latent,), BF16),
            vmem(latent_cache.shape, BF16),
            vmem((own, QK_ROPE, context), BF16),
            vmem((width, QK_NOPE + QK_ROPE), BF16),
            vmem((QK_ROPE, width), BF16),
            vmem(latent_weight.shape, BF16),
            vmem((QK_ROPE, cols), BF16),
            vmem(absorb_weight.shape[1:], BF16),
            vmem((2, *value_weight.shape[1:]), BF16),
            vmem((n_chip, 2 * output_weight.shape[0], cols), BF16),
            vmem((ff_dev, width), BF16),
            vmem((ff_dev, width), BF16),
            vmem((ff_dev, width), BF16),
            vmem((rows, width), F32),
            vmem((rows, width), BF16),
            vmem((rows, MESSAGE), F32),
            vmem((rows, latent), F32),
            vmem((all_slots, cols), F32),
            vmem((all_slots, 128), F32),
            vmem((n_tp, own, width), BF16),
            vmem((n_tp, own, MESSAGE), BF16),
            vmem((n_tp, own, MESSAGE), BF16),
            vmem((n_chip, own, 2 * latent), BF16),
            vmem((n_tp, own, 2 * latent), BF16),
            vmem((n_chip, rows, cols), BF16),
            vmem((n_chip, rows, cols), BF16),
            vmem((n_tp, 1, 4 * rows), F32),
            vmem((n_ep, slots, cols), BF16),
            vmem((n_ep, slots, cols), BF16),
            vmem((n_chip, out_rows, 2 * ff), BF16),
            vmem((n_chip, out_rows, 2 * ff), BF16),
            vmem((n_ep, slots, cols), BF16),
            vmem((n_ep, slots, cols), BF16),
            vmem((n_chip, out_rows, 2 * ff), BF16),
            vmem((n_chip, out_rows, 2 * ff), BF16),
            vmem((n_ep, slots, 128), F32),
            vmem((out_rows // slots, slots, 128), F32),
            vmem((n_chip, out_rows, ff), BF16),
            vmem((n_ep, slots, cols), BF16),
            vmem((n_ep, slots, cols), BF16),
            vmem((2, n_tp, ff_dev, cols), BF16),
            vmem((2, n_tp, ff_dev, cols), BF16),
            vmem((2, n_tp, ff_dev, cols), BF16),
            pltpu.SemaphoreType.DMA((20,)),
            pltpu.SemaphoreType.DMA((21,)),
            pltpu.SemaphoreType.DMA((21,)),
            pltpu.SemaphoreType.DMA((n_chip,)),
        ],
        compiler_params=pltpu.CompilerParams(
            collective_id=0, has_side_effects=True, vmem_limit_bytes=40 * 1024 * 1024
        ),
    )(*[pltpu.with_memory_space_constraint(x, pltpu.HBM) for x in operands])
    return pl.pallas_call(
        hand_over,
        out_shape=shapes,
        in_specs=[pl.BlockSpec(memory_space=vmem)] * 3,
        out_specs=[pl.BlockSpec(memory_space=pltpu.HBM)] * 3,
        scratch_shapes=[pltpu.SemaphoreType.DMA((3,))],
        compiler_params=pltpu.CompilerParams(vmem_limit_bytes=16 * 1024 * 1024),
    )(*results)


def solution(mesh):
    placed = (
        P(("ep", "tp"), None),
        P("ep"),
        P(("ep", "tp"), None, None),
        P(("ep", "tp"), None, None),
        P(),
        P(None, "tp"),
        P(None, "tp"),
        P("tp", None),
        P("tp", None),
        P(),
        P("tp", None, None),
        P("tp", None, None),
        P("tp", None),
        P(),
        P(),
        P("ep", None, "tp"),
        P("ep", None, "tp"),
        P("ep", "tp", None),
        P("ep", None),
        P("ep", None),
    )
    return jax.shard_map(
        per_device,
        mesh=mesh,
        in_specs=placed,
        out_specs=(P("ep", "tp"), P(("ep", "tp"), None), P(("ep", "tp"), None)),
        check_vma=False,
    )
```

```python
import functools

import jax
import jax.numpy as jnp
import numpy as np
from jax import lax
from jax.experimental import pallas as pl
from jax.experimental.pallas import tpu as pltpu
from jax.sharding import PartitionSpec as P

MESH = pl.DeviceIdType.MESH
F32 = jnp.float32
BF16 = jnp.bfloat16
HIGHEST = lax.Precision.HIGHEST

QK_NOPE = 128
QK_ROPE = 64
norm_floor = 1e-06
rope_base = 10000.0
masked_score = -1e30

EP_X = 4
GATE_NEAR, UP_NEAR, DOWN_NEAR = 5, 4, 4

LAT_AT, KEY_AT, ROT_AT, KEY_ROT_AT, MESSAGE = 0, 256, 512, 640, 768


def dot(a, b, precision=None):
    return lax.dot_general(
        a, b, (((1,), (0,)), ((), ())), preferred_element_type=F32, precision=precision
    )


def dot_t(a, b, precision=None):
    return lax.dot_general(
        a, b, (((1,), (1,)), ((), ())), preferred_element_type=F32, precision=precision
    )


def swap_halves(x):
    half = x.shape[-1] // 2
    return jnp.concatenate([x[:, half:], x[:, :half]], axis=1)


def gain_row(ref, first, size):
    return ref[pl.ds(first, size)].astype(F32).reshape(1, size)


def cos_sin(x):
    return jnp.cos(x), jnp.sin(x)


def iota(shape, dim):
    return lax.broadcasted_iota(jnp.int32, shape, dim)


def kernel(
    n_tp,
    n_ep,
    tokens,
    lengths,
    latent_cache,
    rope_cache,
    attn_gain,
    mix_gain,
    expert_gain,
    latent_gain,
    query_weight,
    query_rot_weight,
    latent_weight,
    key_rot_weight,
    absorb_weight,
    value_weight,
    output_weight,
    gate_weight,
    up_weight,
    down_weight,
    expert_ids,
    route_weights,
    out,
    new_latent,
    new_rope,
    len_v,
    ids_v,
    rw_v,
    attn_v,
    mixg_v,
    expg_v,
    latg_v,
    lat_v,
    rope_v,
    query_v,
    qrw_v,
    lw_v,
    krw_v,
    abs_v,
    val_pair,
    ow_pair,
    gate_v,
    up_v,
    down_v,
    tok_f,
    normed_b,
    msg_f,
    lat_f,
    route_f,
    factor_f,
    tok_in,
    qry_out,
    qry_in,
    att_out,
    att_in,
    mix_out,
    mix_in,
    sum_in,
    dis_out,
    dis_in,
    part_out,
    part_in,
    tok_dis_out,
    tok_dis_in,
    tok_part_out,
    tok_part_in,
    factor_out,
    factor_in,
    hid_in,
    ret_out,
    ret_in,
    gate_in,
    up_in,
    down_in,
    local_sems,
    send_sems,
    recv_sems,
    tok_sems,
):
    me = lax.axis_index("tp")
    group = lax.axis_index("ep")
    rows = tok_f.shape[0]
    own = rows // n_tp
    width = tok_f.shape[1]
    cols = width // n_tp
    slots = dis_out.shape[1]
    ff_dev = gate_v.shape[0]
    latent = abs_v.shape[1]
    my_first = pl.multiple_of(me * cols, cols)
    my_cols = pl.ds(my_first, cols)
    n_chip = n_tp // 2
    half_ep = n_ep // 2
    chip = me // 2
    core = lax.rem(me, 2)
    sibling = me + 1 - 2 * core
    side = lax.rem(group, 2)
    at_home = side == core

    def load(index, src, dst):
        copy = pltpu.make_async_copy(src, dst, local_sems.at[index])
        copy.start()
        return copy

    tok_copy = load(0, tokens, tok_in.at[me])

    barrier = pltpu.get_barrier_semaphore()

    def greet(device):
        pl.semaphore_signal(barrier, inc=1, device_id=device, device_id_type=MESH)

    n_z = n_ep // EP_X
    group_z, group_x = group // EP_X, lax.rem(group, EP_X)
    ep_order = sorted(
        [(z, x) for z in range(n_z) for x in range(EP_X) if z or x],
        key=lambda o: -min(o[0], n_z - o[0]) - min(o[1], EP_X - o[1]),
    )

    def ep_peer(offset):
        return EP_X * lax.rem(group_z + offset[0], n_z) + lax.rem(group_x + offset[1], EP_X)

    for offset in ep_order:
        greet({"ep": ep_peer(offset), "tp": 2 * chip + side})

    for d in range(1, n_tp):
        greet({"tp": lax.rem(me + d, n_tp)})

    @pl.when(jnp.logical_not(at_home))
    def _():
        greet({"tp": sibling})

    for d in range(half_ep):
        greet({"ep": 2 * d + core, "tp": 2 * chip + 1 - side})

    small = [
        load(13, lengths, len_v),
        load(14, expert_ids, ids_v),
        load(15, route_weights, rw_v),
        load(16, attn_gain, attn_v),
        load(17, mix_gain, mixg_v),
        load(18, expert_gain, expg_v),
        load(19, latent_gain, latg_v),
    ]
    qw_copy = load(1, query_weight, query_v.at[:, pl.ds(0, QK_NOPE)])
    qrw_copy = load(2, query_rot_weight, qrw_v)
    lw_copy = load(3, latent_weight, lw_v)
    krw_copy = load(4, key_rot_weight, krw_v)
    abs_copy = load(5, absorb_weight.at[0], abs_v)
    gate_copy = load(6, gate_weight.at[0], gate_v)
    up_copy = load(7, up_weight.at[0], up_v)
    lat_copy = load(8, latent_cache, lat_v)
    rope_copy = load(9, rope_cache, rope_v)
    val_copy = load(10, value_weight.at[0], val_pair.at[core])
    value_dim = value_weight.shape[2]
    head_rows = pl.ds(pl.multiple_of(core * value_dim, value_dim), value_dim)

    def block(index):
        return pl.ds(pl.multiple_of(index * cols, cols), cols)

    for y in range(n_chip):
        pltpu.make_async_copy(
            output_weight.at[:, block(2 * y + core)],
            ow_pair.at[y, head_rows],
            local_sems.at[11],
        ).start()
    down_copy = load(12, down_weight.at[0], down_v)

    pl.semaphore_wait(
        barrier, n_tp - 1 + n_ep + half_ep - jnp.where(at_home, 1, 0)
    )

    order = sorted(range(1, n_tp), key=lambda d: -min(d, n_tp - d))
    chip_order = sorted(range(1, n_chip), key=lambda d: -min(d, n_chip - d))

    def send(src, dst, stage, device, recv_sem=None):
        pltpu.make_async_remote_copy(
            src_ref=src,
            dst_ref=dst,
            send_sem=send_sems.at[stage],
            recv_sem=recv_sems.at[stage] if recv_sem is None else recv_sem,
            device_id=device,
            device_id_type=MESH,
        ).start()

    def send_tp(stage, src_of, dst):
        for d in order:
            peer = lax.rem(me + d, n_tp)
            send(src_of(peer), dst, stage, {"tp": peer})

    def send_chips(stage, src_of, dst):
        for d in chip_order:
            peer = lax.rem(chip + d, n_chip)
            send(src_of(peer), dst, stage, {"tp": 2 * peer + core})

    def wait_for(sem, buffer, count):
        some = buffer.at[pl.ds(0, count)]
        pltpu.make_async_copy(some, some, sem).wait()

    def arrived(stage, buffer, count=None):
        wait_for(recv_sems.at[stage], buffer, buffer.shape[0] - 1 if count is None else count)

    def sent(stage, buffer, count=None):
        wait_for(send_sems.at[stage], buffer, buffer.shape[0] - 1 if count is None else count)

    def arrived_all(stage, buffer):
        pltpu.make_async_copy(buffer, buffer, recv_sems.at[stage]).wait()

    def sent_all(stage, buffer):
        pltpu.make_async_copy(buffer, buffer, send_sems.at[stage]).wait()

    def at_home_or_not(stage, buffer, sems):
        count = buffer.shape[0]

        @pl.when(at_home)
        def _():
            wait_for(sems.at[stage], buffer, count - 1)

        @pl.when(jnp.logical_not(at_home))
        def _():
            wait_for(sems.at[stage], buffer, count)

    tok_copy.wait()
    send(tok_in.at[me], tok_in.at[me], 0, {"tp": sibling}, recv_sems.at[12])
    for d in chip_order:
        peer = lax.rem(chip + d, n_chip)
        send(tok_in.at[me], tok_in.at[me], 0, {"tp": 2 * peer + core}, tok_sems.at[chip])

    def near_of(limit):
        return [d for d in order if min(d, n_tp - d) <= limit]

    def far_of(limit):
        return [d for d in order if min(d, n_tp - d) > limit]

    def send_weights(stage, source, target, offsets):
        for d in offsets:
            peer = lax.rem(me + d, n_tp)
            send(
                source.at[:, block(peer)],
                target.at[lax.rem(peer, 2), me],
                stage,
                {"tp": peer},
            )

    gate_copy.wait()
    send_weights(2, gate_v, gate_in, near_of(GATE_NEAR))

    square = (rows, rows)
    eye = (iota(square, 0) == iota(square, 1)).astype(F32)
    ahead_row = iota(square, 0) < iota(square, 1)
    ahead_col = iota(square, 1) < iota(square, 0)
    for copy in small:
        copy.wait()
    ids = ids_v[...].astype(F32)
    weights_row = rw_v[...]
    id_rows = [ids[k : k + 1, :] for k in range(2)]
    id_cols = [jnp.sum(eye * r, axis=1, keepdims=True) for r in id_rows]
    weight_cols = [
        jnp.sum(eye * weights_row[k : k + 1, :], axis=1, keepdims=True) for k in range(2)
    ]

    def same(j, k):
        return id_cols[j] == id_rows[k]

    def count(mask, axis):
        return jnp.sum(jnp.where(mask, 1.0, 0.0), axis=axis, keepdims=True)

    rank_row0 = count(same(0, 0) & ahead_row, 0)
    rank_row1 = count(same(0, 1), 0) + count(same(1, 1) & ahead_row, 0)
    rank_col0 = count(same(0, 0) & ahead_col, 1)
    rank_col1 = count(same(1, 0), 1) + count(same(1, 1) & ahead_col, 1)
    target_rows = [id_rows[0] * slots + rank_row0, id_rows[1] * slots + rank_row1]
    target_cols = [id_cols[0] * slots + rank_col0, id_cols[1] * slots + rank_col1]
    all_slots = n_ep * slots
    down_iota = iota((all_slots, rows), 0).astype(F32)
    across_iota = iota((rows, all_slots), 1).astype(F32)
    dispatch = (
        jnp.where(down_iota == target_rows[0], 1.0, 0.0)
        + jnp.where(down_iota == target_rows[1], 1.0, 0.0)
    ).astype(BF16)
    combine = jnp.where(across_iota == target_cols[0], weight_cols[0], 0.0) + jnp.where(
        across_iota == target_cols[1], weight_cols[1], 0.0
    )

    half = QK_ROPE // 2
    freqs = jnp.zeros((1, QK_ROPE), F32)
    lane = lax.rem(iota((1, QK_ROPE), 1), half)
    for i in range(half):
        freqs = jnp.where(lane == i, float(np.float32(rope_base ** (-i / half))), freqs)
    lengths_row = len_v[...].astype(F32)
    lengths_col = jnp.sum(eye * lengths_row, axis=1, keepdims=True)
    cosine, sine = cos_sin(lengths_col * freqs)
    sine = jnp.where(iota((1, QK_ROPE), 1) < half, -sine, sine)
    own_rows = (iota((8, rows), 1) == own * me + iota((8, rows), 0)).astype(F32)
    own_cosine = dot(own_rows, cosine, HIGHEST)[:own]
    own_sine = dot(own_rows, sine, HIGHEST)[:own]
    own_lengths = jnp.sum(own_rows * lengths_row, axis=1, keepdims=True).astype(jnp.int32)

    qrw_copy.wait()
    for c in range(0, width, 512):
        turned = qrw_v[:, c : c + 512].T
        query_v[c : c + 512, QK_NOPE:] = jnp.concatenate([turned, turned], axis=1)
    qw_copy.wait()
    for d in reversed(chip_order):
        peer = lax.rem(chip + d, n_chip)
        slot = tok_in.at[2 * peer + core]
        pltpu.make_async_copy(slot, slot, tok_sems.at[peer]).wait()
        send(slot, slot, 0, {"tp": sibling}, recv_sems.at[12])
    arrived(12, tok_in, n_chip)
    for t in range(n_tp):
        tok_f[own * t : own * (t + 1), :] = tok_in[t].astype(F32)
    chunk = 512
    square_sum = jnp.zeros((rows, 1), F32)
    for c in range(0, width, chunk):
        x = tok_f[:, c : c + chunk]
        square_sum = square_sum + jnp.sum(x * x, axis=1, keepdims=True)
    factor = lax.rsqrt(square_sum / width + norm_floor)
    for c in range(0, width, chunk):
        x = tok_f[:, c : c + chunk]
        normed_b[:, c : c + chunk] = (x * factor * gain_row(attn_v, c, chunk)).astype(BF16)

    mid = width // 2
    query = dot(normed_b[:, :mid], query_v[:mid]) + dot(normed_b[:, mid:], query_v[mid:])
    q_nope = query[:, :QK_NOPE].astype(BF16)
    q_rot = query[:, QK_NOPE : QK_NOPE + QK_ROPE]
    abs_copy.wait()
    msg_f[:, LAT_AT : LAT_AT + latent] = dot(q_nope, abs_v[...])
    msg_f[:, ROT_AT : ROT_AT + QK_ROPE] = q_rot * cosine + swap_halves(q_rot) * sine
    slice_rows = normed_b[:, my_cols]
    lw_copy.wait()
    msg_f[:, KEY_AT : KEY_AT + latent] = dot(slice_rows, lw_v[...])
    krw_copy.wait()
    msg_f[:, KEY_ROT_AT : KEY_ROT_AT + QK_ROPE] = dot_t(slice_rows, krw_v[...])
    for t in range(n_tp):
        qry_out[t] = msg_f[own * t : own * (t + 1), :].astype(BF16)

    send_tp(1, lambda peer: qry_out.at[peer], qry_in.at[me])
    qry_in[me] = qry_out[me]
    send(value_weight.at[0], val_pair.at[core], 16, {"tp": sibling})
    for y in range(n_chip):
        send(
            output_weight.at[:, block(2 * y + 1 - core)],
            ow_pair.at[y, head_rows],
            17,
            {"tp": sibling},
        )
    send_weights(2, gate_v, gate_in, far_of(GATE_NEAR))
    up_copy.wait()
    send_weights(4, up_v, up_in, near_of(UP_NEAR))
    gate_in[core, me] = gate_v[:, my_cols]

    tok_cols = tok_f[:, my_cols]
    my_mix_gain = gain_row(mixg_v, my_first, cols)
    my_expert_gain = gain_row(expg_v, my_first, cols)
    place = 2 * (group // 2) + core

    def to_experts(stage, value, out_ref, in_ref):
        route_f[...] = dot(dispatch, value.astype(BF16))
        for e in range(n_ep):
            out_ref[e] = route_f[slots * e : slots * (e + 1), :].astype(BF16)
        for offset in ep_order:
            peer = ep_peer(offset)
            send(out_ref.at[peer], in_ref.at[place], stage, {"ep": peer, "tp": 2 * chip + side})

        @pl.when(at_home)
        def _():
            in_ref[place] = out_ref[group]

        @pl.when(jnp.logical_not(at_home))
        def _():
            send(out_ref.at[group], in_ref.at[place], stage, {"tp": sibling})

    to_experts(18, tok_cols * my_expert_gain, tok_dis_out, tok_dis_in)

    lat_copy.wait()
    rope_copy.wait()

    arrived(1, qry_in)
    key_sum = jnp.zeros((own, MESSAGE), F32)
    for h in range(n_tp):
        part = qry_in[h].astype(F32)
        key_sum = key_sum + part
        msg_f[own * h : own * (h + 1), :] = part
    key_raw = key_sum[:, KEY_AT : KEY_AT + latent]
    key_factor = lax.rsqrt(jnp.mean(key_raw * key_raw, axis=1, keepdims=True) + norm_floor)
    own_lat = (key_raw * key_factor * gain_row(latg_v, 0, latent)).astype(BF16)
    rope_raw = key_sum[:, KEY_ROT_AT : KEY_ROT_AT + QK_ROPE]
    own_rot = (rope_raw * own_cosine + swap_halves(rope_raw) * own_sine).astype(BF16)
    new_latent[...] = own_lat
    new_rope[...] = own_rot
    own_lat = own_lat.astype(F32)
    own_rot = own_rot.astype(F32)

    scale = (QK_NOPE + QK_ROPE) ** (-0.5)
    queries = msg_f[:, LAT_AT : LAT_AT + latent]
    rotated = msg_f[:, ROT_AT : ROT_AT + QK_ROPE]
    queries_b = queries.astype(BF16)
    rotated_b = rotated.astype(BF16)
    context = lat_v.shape[1]
    row_col = iota((rows, 1), 0)
    first = lax.rem(row_col, own) == 0

    def of_row(a, b):
        return jnp.where(first, a, b)

    scores = of_row(
        dot_t(queries_b, lat_v[0]) + dot(rotated_b, rope_v[0]),
        dot_t(queries_b, lat_v[1]) + dot(rotated_b, rope_v[1]),
    )
    row_len = of_row(own_lengths[0:1], own_lengths[1:2])
    valid = iota((rows, context), 1) < row_len
    scores = jnp.where(valid, scores * scale, masked_score)
    lat_rows = of_row(own_lat[0:1], own_lat[1:2])
    rot_rows = of_row(own_rot[0:1], own_rot[1:2])
    own_score = (
        jnp.sum(queries * lat_rows, axis=1, keepdims=True)
        + jnp.sum(rotated * rot_rows, axis=1, keepdims=True)
    ) * scale
    top = jnp.maximum(jnp.max(scores, axis=1, keepdims=True), own_score)
    weights = jnp.where(valid, jnp.exp(scores - top), 0.0)
    own_weight = jnp.exp(own_score - top)
    total = jnp.sum(weights, axis=1, keepdims=True) + own_weight
    summed = (
        dot(jnp.where(first, weights, 0.0).astype(BF16), lat_v[0])
        + dot(jnp.where(first, 0.0, weights).astype(BF16), lat_v[1])
        + own_weight.astype(BF16).astype(F32) * lat_rows
    )
    lat_f[...] = summed / total
    for y in range(n_chip):
        for c in range(2):
            at = own * (2 * y + c)
            att_out[y, :, c * latent : (c + 1) * latent] = lat_f[at : at + own, :].astype(BF16)

    send_tp(3, lambda peer: att_out.at[peer // 2], att_in.at[me])
    att_in[me] = att_out[chip]
    send_weights(4, up_v, up_in, far_of(UP_NEAR))
    down_copy.wait()
    send_weights(8, down_v, down_in, near_of(DOWN_NEAR))
    up_in[core, me] = up_v[:, my_cols]
    val_copy.wait()
    pltpu.make_async_copy(
        ow_pair.at[:, head_rows], ow_pair.at[:, head_rows], local_sems.at[11]
    ).wait()
    arrived(16, val_pair)
    pltpu.make_async_copy(
        ow_pair.at[:, head_rows], ow_pair.at[:, head_rows], recv_sems.at[17]
    ).wait()

    arrived(3, att_in)
    for t in range(n_tp):
        msg_f[own * t : own * (t + 1), : 2 * latent] = att_in[t].astype(F32)
    results = msg_f[:, : 2 * latent].astype(BF16)
    head_values = jnp.concatenate(
        [dot(results[:, c * latent : (c + 1) * latent], val_pair[c]) for c in range(2)], axis=1
    ).astype(BF16)

    for batch in (chip_order[:3], chip_order[3:]):
        peers = [lax.rem(chip + d, n_chip) for d in batch]
        for peer in peers:
            mix_out[peer] = dot(head_values, ow_pair[peer]).astype(BF16)
        for peer in peers:
            send(mix_out.at[peer], mix_in.at[chip], 5, {"tp": 2 * peer + core})
    mix_in[chip] = dot(head_values, ow_pair[chip]).astype(BF16)

    arrived(2, gate_in.at[core])
    send(gate_in.at[core], gate_in.at[core], 13, {"tp": sibling})
    arrived(4, up_in.at[core])
    send(up_in.at[core], up_in.at[core], 14, {"tp": sibling})
    side_rows = half_ep * slots
    ff = n_tp * ff_dev
    out_rows = side_rows // n_chip

    def partial_sums(in_ref, out_ref):
        for g in range(half_ep):
            for c in range(2):
                at = c * side_rows + slots * g
                route_f[at : at + slots, :] = in_ref[2 * g + c].astype(F32)
        received = [
            route_f[c * side_rows : (c + 1) * side_rows, :].astype(BF16) for c in range(2)
        ]
        for n, source in enumerate((gate_in, up_in)):
            part = dot_t(received[0], source[0].reshape(ff, cols)) + dot_t(
                received[1], source[1].reshape(ff, cols)
            )
            out_ref[:, :, n * ff : (n + 1) * ff] = part.reshape(n_chip, out_rows, ff).astype(BF16)

    def summed_parts(in_ref):
        both = in_ref[0].astype(F32)
        for t in range(1, n_chip):
            both = both + in_ref[t].astype(F32)
        return both

    at_home_or_not(18, tok_dis_in, recv_sems)
    arrived_all(13, gate_in.at[core])
    arrived_all(14, up_in.at[core])
    partial_sums(tok_dis_in, tok_part_out)
    send_chips(19, lambda peer: tok_part_out.at[peer], tok_part_in.at[chip])
    tok_part_in[chip] = tok_part_out[chip]

    arrived(5, mix_in)
    mixed = mix_in[0].astype(F32)
    for t in range(1, n_chip):
        mixed = mixed + mix_in[t].astype(F32)
    mixed = mixed.astype(BF16).astype(F32)
    scaled = mixed * my_mix_gain

    to_experts(7, scaled * my_expert_gain, dis_out, dis_in)

    def as_row(col):
        return jnp.sum(eye * col, axis=0, keepdims=True)

    def as_col(row):
        return jnp.sum(eye * row, axis=1, keepdims=True)

    def row_sum(value):
        return as_row(jnp.sum(value, axis=1, keepdims=True))

    sums = jnp.concatenate(
        [
            row_sum(mixed * mixed),
            row_sum(tok_cols * scaled),
            row_sum(scaled * scaled),
            jnp.zeros((1, rows), F32),
        ],
        axis=1,
    )
    sum_in[me] = sums
    send_tp(6, lambda peer: sum_in.at[me], sum_in.at[me])
    send_weights(8, down_v, down_in, far_of(DOWN_NEAR))
    down_in[core, me] = down_v[:, my_cols]

    arrived(6, sum_in)
    sums = sum_in[0]
    for t in range(1, n_tp):
        sums = sums + sum_in[t]
    mix_square = as_col(sums[:, 0:rows])
    cross = as_col(sums[:, rows : 2 * rows])
    scaled_square = as_col(sums[:, 2 * rows : 3 * rows])
    mix_factor = lax.rsqrt(mix_square / width + norm_floor)
    resid = (tok_cols + scaled * mix_factor).astype(BF16).astype(F32)
    resid_square = square_sum + mix_factor * (2.0 * cross + mix_factor * scaled_square)
    resid_factor = lax.rsqrt(jnp.maximum(resid_square, 0.0) / width + norm_floor)

    lanes = iota((rows, 128), 1)
    factors = jnp.where(lanes < 64, mix_factor, resid_factor)
    factor_f[...] = dot(dispatch.astype(F32), factors, HIGHEST)
    for e in range(n_ep):
        factor_out[e] = factor_f[slots * e : slots * (e + 1), :]
    per_device_groups = out_rows // slots
    speaks = me == 2 * (group // (2 * per_device_groups)) + side
    factor_place = lax.rem(group // 2, per_device_groups)

    @pl.when(speaks)
    def _():
        for offset in ep_order:
            peer = ep_peer(offset)
            send(factor_out.at[peer], factor_in.at[factor_place], 20, {"ep": peer})
        factor_in[factor_place] = factor_out[group]

    at_home_or_not(7, dis_in, recv_sems)
    partial_sums(dis_in, part_out)

    send_chips(9, lambda peer: part_out.at[peer], part_in.at[chip])
    part_in[chip] = part_out[chip]
    arrived(8, down_in.at[core])
    send(down_in.at[core], down_in.at[core], 15, {"tp": sibling})
    arrived(9, part_in)
    arrived(19, tok_part_in)

    @pl.when(speaks)
    def _():
        wait_for(recv_sems.at[20], factor_in, per_device_groups - 1)

    @pl.when(jnp.logical_not(speaks))
    def _():
        wait_for(recv_sems.at[20], factor_in, per_device_groups)

    for g in range(per_device_groups):
        factor_f[slots * g : slots * (g + 1), :] = factor_in[g]
    mix_factors = factor_f[:out_rows, 0:1]
    resid_factors = factor_f[:out_rows, 64:65]
    both = (summed_parts(tok_part_in) + mix_factors * summed_parts(part_in)) * resid_factors
    gate, upward = both[:, :ff], both[:, ff:]
    hid_in[chip] = (gate / (1.0 + jnp.exp(-gate)) * upward).astype(BF16)

    send_chips(10, lambda peer: hid_in.at[chip], hid_in.at[chip])
    arrived_all(15, down_in.at[core])
    arrived(10, hid_in)
    hidden = hid_in[...].astype(F32).reshape(side_rows, ff).astype(BF16)
    for c in range(2):
        at = c * side_rows
        route_f[at : at + side_rows, :] = dot(hidden, down_in[c].reshape(ff, cols))
        for g in range(half_ep):
            at = c * side_rows + slots * g
            ret_out[2 * g + c] = route_f[at : at + slots, :].astype(BF16)

    for z in sorted(range(1, n_z), key=lambda z: -min(z, n_z - z)):
        for x in range(EP_X // 2):
            pair = EP_X // 2 * lax.rem(group_z + z, n_z) + x
            for c in range(2):
                send(
                    ret_out.at[2 * pair + c],
                    ret_in.at[group],
                    11,
                    {"ep": 2 * pair + core, "tp": 2 * chip + c},
                )
    for x in range(1, EP_X // 2):
        pair = EP_X // 2 * group_z + lax.rem(group_x // 2 + x, EP_X // 2)
        for c in range(2):
            send(
                ret_out.at[2 * pair + c],
                ret_in.at[group],
                11,
                {"ep": 2 * pair + core, "tp": 2 * chip + c},
            )

    @pl.when(at_home)
    def _():
        ret_in[group] = ret_out[place]
        send(ret_out.at[place + 1 - 2 * core], ret_in.at[group], 11, {"tp": sibling})

    @pl.when(jnp.logical_not(at_home))
    def _():
        for c in range(2):
            send(
                ret_out.at[2 * (group // 2) + c],
                ret_in.at[group],
                11,
                {"ep": 2 * (group // 2) + core, "tp": 2 * chip + c},
            )

    at_home_or_not(11, ret_in, recv_sems)
    for e in range(n_ep):
        route_f[slots * e : slots * (e + 1), :] = ret_in[e].astype(F32)
    out[...] = (resid + dot(combine, route_f[...], HIGHEST)).astype(BF16)

    sent(0, tok_in)
    for stage, buffer in (
        (1, qry_in),
        (2, gate_in.at[core]),
        (3, att_in),
        (4, up_in.at[core]),
        (5, mix_in),
        (6, sum_in),
        (8, down_in.at[core]),
        (9, part_in),
        (10, hid_in),
        (16, val_pair),
        (19, tok_part_in),
    ):
        sent(stage, buffer)
    sent_all(13, gate_in.at[core])
    sent_all(14, up_in.at[core])
    sent_all(15, down_in.at[core])
    sent_all(17, ow_pair.at[:, head_rows])
    at_home_or_not(7, dis_in, send_sems)
    at_home_or_not(18, tok_dis_in, send_sems)

    @pl.when(speaks)
    def _():
        sent(20, factor_out)

    at_home_or_not(11, ret_in, send_sems)


def hand_over(*refs):
    sources, targets, sems = refs[:3], refs[3:6], refs[6]
    copies = [
        pltpu.make_async_copy(a, b, sems.at[i]) for i, (a, b) in enumerate(zip(sources, targets))
    ]
    for copy in copies:
        copy.start()
    for copy in copies:
        copy.wait()


def per_device(
    tokens,
    lengths,
    latent_cache,
    rope_cache,
    attn_gain,
    query_weight,
    query_rot_weight,
    latent_weight,
    key_rot_weight,
    latent_gain,
    absorb_weight,
    value_weight,
    output_weight,
    mix_gain,
    expert_gain,
    gate_weight,
    up_weight,
    down_weight,
    expert_ids,
    route_weights,
):
    n_tp, n_ep = lax.axis_size("tp"), lax.axis_size("ep")
    own, width = tokens.shape
    rows = own * n_tp
    cols = width // n_tp
    latent = latent_weight.shape[1]
    context = latent_cache.shape[1]
    ff_dev = gate_weight.shape[2]
    ff = ff_dev * n_tp
    slots = 2 * rows * expert_ids.shape[1] // n_ep
    all_slots = n_ep * slots
    n_chip = n_tp // 2
    out_rows = all_slots // n_tp

    operands = (
        tokens,
        lengths.reshape(1, rows),
        latent_cache,
        jnp.swapaxes(rope_cache, 1, 2),
        attn_gain,
        mix_gain,
        expert_gain,
        latent_gain,
        query_weight,
        query_rot_weight.T,
        latent_weight,
        key_rot_weight.T,
        absorb_weight,
        value_weight,
        output_weight,
        jnp.swapaxes(gate_weight, 1, 2),
        jnp.swapaxes(up_weight, 1, 2),
        down_weight,
        expert_ids.T,
        route_weights.T,
    )
    vmem = pltpu.VMEM
    shapes = (
        jax.ShapeDtypeStruct((rows, cols), BF16),
        jax.ShapeDtypeStruct((own, latent), BF16),
        jax.ShapeDtypeStruct((own, QK_ROPE), BF16),
    )
    results = pl.pallas_call(
        functools.partial(kernel, n_tp, n_ep),
        out_shape=shapes,
        in_specs=[
            pl.BlockSpec(memory_space=pltpu.HBM) for _ in operands
        ],
        out_specs=[pl.BlockSpec(memory_space=vmem)] * 3,
        scratch_shapes=[
            vmem((1, rows), jnp.int32),
            vmem(expert_ids.shape[::-1], jnp.int32),
            vmem(route_weights.shape[::-1], F32),
            vmem((width,), BF16),
            vmem((width,), BF16),
            vmem((width,), BF16),
            vmem((latent,), BF16),
            vmem(latent_cache.shape, BF16),
            vmem((own, QK_ROPE, context), BF16),
            vmem((width, 2 * QK_NOPE), BF16),
            vmem((QK_ROPE, width), BF16),
            vmem(latent_weight.shape, BF16),
            vmem((QK_ROPE, cols), BF16),
            vmem(absorb_weight.shape[1:], BF16),
            vmem((2, *value_weight.shape[1:]), BF16),
            vmem((n_chip, 2 * output_weight.shape[0], cols), BF16),
            vmem((ff_dev, width), BF16),
            vmem((ff_dev, width), BF16),
            vmem((ff_dev, width), BF16),
            vmem((rows, width), F32),
            vmem((rows, width), BF16),
            vmem((rows, MESSAGE), F32),
            vmem((rows, latent), F32),
            vmem((all_slots, cols), F32),
            vmem((all_slots, 128), F32),
            vmem((n_tp, own, width), BF16),
            vmem((n_tp, own, MESSAGE), BF16),
            vmem((n_tp, own, MESSAGE), BF16),
            vmem((n_chip, own, 2 * latent), BF16),
            vmem((n_tp, own, 2 * latent), BF16),
            vmem((n_chip, rows, cols), BF16),
            vmem((n_chip, rows, cols), BF16),
            vmem((n_tp, 1, 4 * rows), F32),
            vmem((n_ep, slots, cols), BF16),
            vmem((n_ep, slots, cols), BF16),
            vmem((n_chip, out_rows, 2 * ff), BF16),
            vmem((n_chip, out_rows, 2 * ff), BF16),
            vmem((n_ep, slots, cols), BF16),
            vmem((n_ep, slots, cols), BF16),
            vmem((n_chip, out_rows, 2 * ff), BF16),
            vmem((n_chip, out_rows, 2 * ff), BF16),
            vmem((n_ep, slots, 128), F32),
            vmem((out_rows // slots, slots, 128), F32),
            vmem((n_chip, out_rows, ff), BF16),
            vmem((n_ep, slots, cols), BF16),
            vmem((n_ep, slots, cols), BF16),
            vmem((2, n_tp, ff_dev, cols), BF16),
            vmem((2, n_tp, ff_dev, cols), BF16),
            vmem((2, n_tp, ff_dev, cols), BF16),
            pltpu.SemaphoreType.DMA((20,)),
            pltpu.SemaphoreType.DMA((21,)),
            pltpu.SemaphoreType.DMA((21,)),
            pltpu.SemaphoreType.DMA((n_chip,)),
        ],
        compiler_params=pltpu.CompilerParams(
            collective_id=0, has_side_effects=True, vmem_limit_bytes=40 * 1024 * 1024
        ),
    )(*[pltpu.with_memory_space_constraint(x, pltpu.HBM) for x in operands])
    return pl.pallas_call(
        hand_over,
        out_shape=shapes,
        in_specs=[pl.BlockSpec(memory_space=vmem)] * 3,
        out_specs=[pl.BlockSpec(memory_space=pltpu.HBM)] * 3,
        scratch_shapes=[pltpu.SemaphoreType.DMA((3,))],
        compiler_params=pltpu.CompilerParams(vmem_limit_bytes=16 * 1024 * 1024),
    )(*results)


def solution(mesh):
    placed = (
        P(("ep", "tp"), None),
        P("ep"),
        P(("ep", "tp"), None, None),
        P(("ep", "tp"), None, None),
        P(),
        P(None, "tp"),
        P(None, "tp"),
        P("tp", None),
        P("tp", None),
        P(),
        P("tp", None, None),
        P("tp", None, None),
        P("tp", None),
        P(),
        P(),
        P("ep", None, "tp"),
        P("ep", None, "tp"),
        P("ep", "tp", None),
        P("ep", None),
        P("ep", None),
    )
    return jax.shard_map(
        per_device,
        mesh=mesh,
        in_specs=placed,
        out_specs=(P("ep", "tp"), P(("ep", "tp"), None), P(("ep", "tp"), None)),
        check_vma=False,
    )
```

```python
import functools

import jax
import jax.numpy as jnp
import numpy as np
from jax import lax
from jax.experimental import pallas as pl
from jax.experimental.pallas import tpu as pltpu
from jax.sharding import PartitionSpec as P

MESH = pl.DeviceIdType.MESH
F32 = jnp.float32
BF16 = jnp.bfloat16
HIGHEST = lax.Precision.HIGHEST

QK_NOPE = 128
QK_ROPE = 64
norm_floor = 1e-06
rope_base = 10000.0
masked_score = -1e30

EP_X = 4
GATE_NEAR, UP_NEAR, DOWN_NEAR = 5, 4, 4

LAT_AT, KEY_AT, ROT_AT, KEY_ROT_AT, MESSAGE = 0, 256, 512, 576, 640


def dot(a, b, precision=None):
    return lax.dot_general(
        a, b, (((1,), (0,)), ((), ())), preferred_element_type=F32, precision=precision
    )


def dot_t(a, b, precision=None):
    return lax.dot_general(
        a, b, (((1,), (1,)), ((), ())), preferred_element_type=F32, precision=precision
    )


def swap_halves(x):
    half = x.shape[-1] // 2
    return jnp.concatenate([x[:, half:], x[:, :half]], axis=1)


def gain_row(ref, first, size):
    return ref[pl.ds(first, size)].astype(F32).reshape(1, size)


def cos_sin(x):
    return jnp.cos(x), jnp.sin(x)


def iota(shape, dim):
    return lax.broadcasted_iota(jnp.int32, shape, dim)


def kernel(
    n_tp,
    n_ep,
    tokens,
    lengths,
    latent_cache,
    rope_cache,
    attn_gain,
    mix_gain,
    expert_gain,
    latent_gain,
    query_weight,
    query_rot_weight,
    latent_weight,
    key_rot_weight,
    absorb_weight,
    value_weight,
    output_weight,
    gate_weight,
    up_weight,
    down_weight,
    expert_ids,
    route_weights,
    out,
    new_latent,
    new_rope,
    len_v,
    ids_v,
    rw_v,
    attn_v,
    mixg_v,
    expg_v,
    latg_v,
    lat_v,
    rope_v,
    query_v,
    qrw_v,
    lw_v,
    krw_v,
    abs_v,
    val_pair,
    ow_pair,
    gate_v,
    up_v,
    down_v,
    tok_f,
    normed_b,
    msg_f,
    lat_f,
    route_f,
    factor_f,
    tok_in,
    qry_out,
    qry_in,
    att_out,
    att_in,
    mix_out,
    mix_in,
    sum_in,
    dis_out,
    dis_in,
    part_out,
    part_in,
    tok_dis_out,
    tok_dis_in,
    tok_part_out,
    tok_part_in,
    factor_out,
    factor_in,
    hid_in,
    ret_out,
    ret_in,
    gate_in,
    up_in,
    down_in,
    local_sems,
    send_sems,
    recv_sems,
    tok_sems,
):
    me = lax.axis_index("tp")
    group = lax.axis_index("ep")
    rows = tok_f.shape[0]
    own = rows // n_tp
    width = tok_f.shape[1]
    cols = width // n_tp
    slots = dis_out.shape[1]
    ff_dev = gate_v.shape[0]
    latent = abs_v.shape[1]
    my_first = pl.multiple_of(me * cols, cols)
    my_cols = pl.ds(my_first, cols)
    n_chip = n_tp // 2
    half_ep = n_ep // 2
    chip = me // 2
    core = lax.rem(me, 2)
    sibling = me + 1 - 2 * core
    side = lax.rem(group, 2)
    at_home = side == core

    def load(index, src, dst):
        copy = pltpu.make_async_copy(src, dst, local_sems.at[index])
        copy.start()
        return copy

    tok_copy = load(0, tokens, tok_in.at[me])

    barrier = pltpu.get_barrier_semaphore()

    def greet(device):
        pl.semaphore_signal(barrier, inc=1, device_id=device, device_id_type=MESH)

    n_z = n_ep // EP_X
    group_z, group_x = group // EP_X, lax.rem(group, EP_X)
    ep_order = sorted(
        [(z, x) for z in range(n_z) for x in range(EP_X) if z or x],
        key=lambda o: -min(o[0], n_z - o[0]) - min(o[1], EP_X - o[1]),
    )

    def ep_peer(offset):
        return EP_X * lax.rem(group_z + offset[0], n_z) + lax.rem(group_x + offset[1], EP_X)

    for offset in ep_order:
        greet({"ep": ep_peer(offset), "tp": 2 * chip + side})

    for d in range(1, n_tp):
        greet({"tp": lax.rem(me + d, n_tp)})

    @pl.when(jnp.logical_not(at_home))
    def _():
        greet({"tp": sibling})

    for d in range(half_ep):
        greet({"ep": 2 * d + core, "tp": 2 * chip + 1 - side})

    small = [
        load(13, lengths, len_v),
        load(14, expert_ids, ids_v),
        load(15, route_weights, rw_v),
        load(16, attn_gain, attn_v),
        load(17, mix_gain, mixg_v),
        load(18, expert_gain, expg_v),
        load(19, latent_gain, latg_v),
    ]
    qw_copy = load(1, query_weight, query_v.at[:, pl.ds(0, QK_NOPE)])
    qrw_copy = load(2, query_rot_weight, qrw_v)
    lw_copy = load(3, latent_weight, lw_v)
    krw_copy = load(4, key_rot_weight, krw_v)
    abs_copy = load(5, absorb_weight.at[0], abs_v)
    gate_copy = load(6, gate_weight.at[0], gate_v)
    up_copy = load(7, up_weight.at[0], up_v)
    lat_copy = load(8, latent_cache, lat_v)
    rope_copy = load(9, rope_cache, rope_v)
    val_copy = load(10, value_weight.at[0], val_pair.at[core])
    value_dim = value_weight.shape[2]
    head_rows = pl.ds(pl.multiple_of(core * value_dim, value_dim), value_dim)

    def block(index):
        return pl.ds(pl.multiple_of(index * cols, cols), cols)

    for y in range(n_chip):
        pltpu.make_async_copy(
            output_weight.at[:, block(2 * y + core)],
            ow_pair.at[y, head_rows],
            local_sems.at[11],
        ).start()
    down_copy = load(12, down_weight.at[0], down_v)

    pl.semaphore_wait(
        barrier, n_tp - 1 + n_ep + half_ep - jnp.where(at_home, 1, 0)
    )

    order = sorted(range(1, n_tp), key=lambda d: -min(d, n_tp - d))
    chip_order = sorted(range(1, n_chip), key=lambda d: -min(d, n_chip - d))

    def send(src, dst, stage, device, recv_sem=None):
        pltpu.make_async_remote_copy(
            src_ref=src,
            dst_ref=dst,
            send_sem=send_sems.at[stage],
            recv_sem=recv_sems.at[stage] if recv_sem is None else recv_sem,
            device_id=device,
            device_id_type=MESH,
        ).start()

    def send_tp(stage, src_of, dst):
        for d in order:
            peer = lax.rem(me + d, n_tp)
            send(src_of(peer), dst, stage, {"tp": peer})

    def send_chips(stage, src_of, dst):
        for d in chip_order:
            peer = lax.rem(chip + d, n_chip)
            send(src_of(peer), dst, stage, {"tp": 2 * peer + core})

    def wait_for(sem, buffer, count):
        some = buffer.at[pl.ds(0, count)]
        pltpu.make_async_copy(some, some, sem).wait()

    def arrived(stage, buffer, count=None):
        wait_for(recv_sems.at[stage], buffer, buffer.shape[0] - 1 if count is None else count)

    def sent(stage, buffer, count=None):
        wait_for(send_sems.at[stage], buffer, buffer.shape[0] - 1 if count is None else count)

    def arrived_all(stage, buffer):
        pltpu.make_async_copy(buffer, buffer, recv_sems.at[stage]).wait()

    def sent_all(stage, buffer):
        pltpu.make_async_copy(buffer, buffer, send_sems.at[stage]).wait()

    def at_home_or_not(stage, buffer, sems):
        count = buffer.shape[0]

        @pl.when(at_home)
        def _():
            wait_for(sems.at[stage], buffer, count - 1)

        @pl.when(jnp.logical_not(at_home))
        def _():
            wait_for(sems.at[stage], buffer, count)

    tok_copy.wait()
    send(tok_in.at[me], tok_in.at[me], 0, {"tp": sibling}, recv_sems.at[12])
    for d in chip_order:
        peer = lax.rem(chip + d, n_chip)
        send(tok_in.at[me], tok_in.at[me], 0, {"tp": 2 * peer + core}, tok_sems.at[chip])

    def near_of(limit):
        return [d for d in order if min(d, n_tp - d) <= limit]

    def far_of(limit):
        return [d for d in order if min(d, n_tp - d) > limit]

    def send_weights(stage, source, target, offsets):
        for d in offsets:
            peer = lax.rem(me + d, n_tp)
            send(
                source.at[:, block(peer)],
                target.at[lax.rem(peer, 2), me],
                stage,
                {"tp": peer},
            )

    gate_copy.wait()
    send_weights(2, gate_v, gate_in, near_of(GATE_NEAR))

    square = (rows, rows)
    eye = (iota(square, 0) == iota(square, 1)).astype(F32)
    ahead_row = iota(square, 0) < iota(square, 1)
    ahead_col = iota(square, 1) < iota(square, 0)
    for copy in small:
        copy.wait()
    ids = ids_v[...].astype(F32)
    weights_row = rw_v[...]
    id_rows = [ids[k : k + 1, :] for k in range(2)]
    id_cols = [jnp.sum(eye * r, axis=1, keepdims=True) for r in id_rows]
    weight_cols = [
        jnp.sum(eye * weights_row[k : k + 1, :], axis=1, keepdims=True) for k in range(2)
    ]

    def same(j, k):
        return id_cols[j] == id_rows[k]

    def count(mask, axis):
        return jnp.sum(jnp.where(mask, 1.0, 0.0), axis=axis, keepdims=True)

    rank_row0 = count(same(0, 0) & ahead_row, 0)
    rank_row1 = count(same(0, 1), 0) + count(same(1, 1) & ahead_row, 0)
    rank_col0 = count(same(0, 0) & ahead_col, 1)
    rank_col1 = count(same(1, 0), 1) + count(same(1, 1) & ahead_col, 1)
    target_rows = [id_rows[0] * slots + rank_row0, id_rows[1] * slots + rank_row1]
    target_cols = [id_cols[0] * slots + rank_col0, id_cols[1] * slots + rank_col1]
    all_slots = n_ep * slots
    down_iota = iota((all_slots, rows), 0).astype(F32)
    across_iota = iota((rows, all_slots), 1).astype(F32)
    dispatch = (
        jnp.where(down_iota == target_rows[0], 1.0, 0.0)
        + jnp.where(down_iota == target_rows[1], 1.0, 0.0)
    ).astype(BF16)
    combine = jnp.where(across_iota == target_cols[0], weight_cols[0], 0.0) + jnp.where(
        across_iota == target_cols[1], weight_cols[1], 0.0
    )

    half = QK_ROPE // 2
    freqs = jnp.zeros((1, QK_ROPE), F32)
    lane = lax.rem(iota((1, QK_ROPE), 1), half)
    for i in range(half):
        freqs = jnp.where(lane == i, float(np.float32(rope_base ** (-i / half))), freqs)
    lengths_row = len_v[...].astype(F32)
    lengths_col = jnp.sum(eye * lengths_row, axis=1, keepdims=True)
    cosine, sine = cos_sin(lengths_col * freqs)
    sine = jnp.where(iota((1, QK_ROPE), 1) < half, -sine, sine)
    own_rows = (iota((8, rows), 1) == own * me + iota((8, rows), 0)).astype(F32)
    own_cosine = dot(own_rows, cosine, HIGHEST)[:own]
    own_sine = dot(own_rows, sine, HIGHEST)[:own]
    own_lengths = jnp.sum(own_rows * lengths_row, axis=1, keepdims=True).astype(jnp.int32)

    qrw_copy.wait()
    for c in range(0, width, 512):
        turned = qrw_v[:, c : c + 512].T
        query_v[c : c + 512, QK_NOPE:] = jnp.concatenate([turned, turned], axis=1)
    qw_copy.wait()
    for d in reversed(chip_order):
        peer = lax.rem(chip + d, n_chip)
        slot = tok_in.at[2 * peer + core]
        pltpu.make_async_copy(slot, slot, tok_sems.at[peer]).wait()
        send(slot, slot, 0, {"tp": sibling}, recv_sems.at[12])
    arrived(12, tok_in, n_chip)
    for t in range(n_tp):
        tok_f[own * t : own * (t + 1), :] = tok_in[t].astype(F32)
    chunk = 512
    square_sum = jnp.zeros((rows, 1), F32)
    for c in range(0, width, chunk):
        x = tok_f[:, c : c + chunk]
        square_sum = square_sum + jnp.sum(x * x, axis=1, keepdims=True)
    factor = lax.rsqrt(square_sum / width + norm_floor)
    for c in range(0, width, chunk):
        x = tok_f[:, c : c + chunk]
        normed_b[:, c : c + chunk] = (x * factor * gain_row(attn_v, c, chunk)).astype(BF16)

    mid = width // 2
    query = dot(normed_b[:, :mid], query_v[:mid]) + dot(normed_b[:, mid:], query_v[mid:])
    q_nope = query[:, :QK_NOPE].astype(BF16)
    q_rot = query[:, QK_NOPE : QK_NOPE + QK_ROPE]
    abs_copy.wait()
    msg_f[:, LAT_AT : LAT_AT + latent] = dot(q_nope, abs_v[...])
    msg_f[:, ROT_AT : ROT_AT + QK_ROPE] = q_rot * cosine + swap_halves(q_rot) * sine
    slice_rows = normed_b[:, my_cols]
    lw_copy.wait()
    msg_f[:, KEY_AT : KEY_AT + latent] = dot(slice_rows, lw_v[...])
    krw_copy.wait()
    msg_f[:, KEY_ROT_AT : KEY_ROT_AT + QK_ROPE] = dot_t(slice_rows, krw_v[...])
    for t in range(n_tp):
        qry_out[t] = msg_f[own * t : own * (t + 1), :].astype(BF16)

    send_tp(1, lambda peer: qry_out.at[peer], qry_in.at[me])
    qry_in[me] = qry_out[me]
    send(value_weight.at[0], val_pair.at[core], 16, {"tp": sibling})
    for y in range(n_chip):
        send(
            output_weight.at[:, block(2 * y + 1 - core)],
            ow_pair.at[y, head_rows],
            17,
            {"tp": sibling},
        )
    send_weights(2, gate_v, gate_in, far_of(GATE_NEAR))
    up_copy.wait()
    send_weights(4, up_v, up_in, near_of(UP_NEAR))
    gate_in[core, me] = gate_v[:, my_cols]

    tok_cols = tok_f[:, my_cols]
    my_mix_gain = gain_row(mixg_v, my_first, cols)
    my_expert_gain = gain_row(expg_v, my_first, cols)
    place = 2 * (group // 2) + core

    def to_experts(stage, value, out_ref, in_ref):
        route_f[...] = dot(dispatch, value.astype(BF16))
        for e in range(n_ep):
            out_ref[e] = route_f[slots * e : slots * (e + 1), :].astype(BF16)
        for offset in ep_order:
            peer = ep_peer(offset)
            send(out_ref.at[peer], in_ref.at[place], stage, {"ep": peer, "tp": 2 * chip + side})

        @pl.when(at_home)
        def _():
            in_ref[place] = out_ref[group]

        @pl.when(jnp.logical_not(at_home))
        def _():
            send(out_ref.at[group], in_ref.at[place], stage, {"tp": sibling})

    to_experts(18, tok_cols * my_expert_gain, tok_dis_out, tok_dis_in)

    lat_copy.wait()
    rope_copy.wait()

    arrived(1, qry_in)
    key_sum = jnp.zeros((own, MESSAGE), F32)
    for h in range(n_tp):
        part = qry_in[h].astype(F32)
        key_sum = key_sum + part
        msg_f[own * h : own * (h + 1), :] = part
    key_raw = key_sum[:, KEY_AT : KEY_AT + latent]
    key_factor = lax.rsqrt(jnp.mean(key_raw * key_raw, axis=1, keepdims=True) + norm_floor)
    own_lat = (key_raw * key_factor * gain_row(latg_v, 0, latent)).astype(BF16)
    rope_raw = key_sum[:, KEY_ROT_AT : KEY_ROT_AT + QK_ROPE]
    own_rot = (rope_raw * own_cosine + swap_halves(rope_raw) * own_sine).astype(BF16)
    new_latent[...] = own_lat
    new_rope[...] = own_rot
    own_lat = own_lat.astype(F32)
    own_rot = own_rot.astype(F32)

    scale = (QK_NOPE + QK_ROPE) ** (-0.5)
    queries = msg_f[:, LAT_AT : LAT_AT + latent]
    rotated = msg_f[:, ROT_AT : ROT_AT + QK_ROPE]
    queries_b = queries.astype(BF16)
    rotated_b = rotated.astype(BF16)
    context = lat_v.shape[1]
    row_col = iota((rows, 1), 0)
    first = lax.rem(row_col, own) == 0

    def of_row(a, b):
        return jnp.where(first, a, b)

    scores = of_row(
        dot_t(queries_b, lat_v[0]) + dot(rotated_b, rope_v[0]),
        dot_t(queries_b, lat_v[1]) + dot(rotated_b, rope_v[1]),
    )
    row_len = of_row(own_lengths[0:1], own_lengths[1:2])
    valid = iota((rows, context), 1) < row_len
    scores = jnp.where(valid, scores * scale, masked_score)
    lat_rows = of_row(own_lat[0:1], own_lat[1:2])
    rot_rows = of_row(own_rot[0:1], own_rot[1:2])
    own_score = (
        jnp.sum(queries * lat_rows, axis=1, keepdims=True)
        + jnp.sum(rotated * rot_rows, axis=1, keepdims=True)
    ) * scale
    top = jnp.maximum(jnp.max(scores, axis=1, keepdims=True), own_score)
    weights = jnp.where(valid, jnp.exp(scores - top), 0.0)
    own_weight = jnp.exp(own_score - top)
    total = jnp.sum(weights, axis=1, keepdims=True) + own_weight
    summed = (
        dot(jnp.where(first, weights, 0.0).astype(BF16), lat_v[0])
        + dot(jnp.where(first, 0.0, weights).astype(BF16), lat_v[1])
        + own_weight.astype(BF16).astype(F32) * lat_rows
    )
    lat_f[...] = summed / total
    for y in range(n_chip):
        for c in range(2):
            at = own * (2 * y + c)
            att_out[y, :, c * latent : (c + 1) * latent] = lat_f[at : at + own, :].astype(BF16)

    send_tp(3, lambda peer: att_out.at[peer // 2], att_in.at[me])
    att_in[me] = att_out[chip]
    send_weights(4, up_v, up_in, far_of(UP_NEAR))
    down_copy.wait()
    send_weights(8, down_v, down_in, near_of(DOWN_NEAR))
    up_in[core, me] = up_v[:, my_cols]
    val_copy.wait()
    pltpu.make_async_copy(
        ow_pair.at[:, head_rows], ow_pair.at[:, head_rows], local_sems.at[11]
    ).wait()
    arrived(16, val_pair)
    pltpu.make_async_copy(
        ow_pair.at[:, head_rows], ow_pair.at[:, head_rows], recv_sems.at[17]
    ).wait()

    arrived(3, att_in)
    for t in range(n_tp):
        msg_f[own * t : own * (t + 1), : 2 * latent] = att_in[t].astype(F32)
    results = msg_f[:, : 2 * latent].astype(BF16)
    head_values = jnp.concatenate(
        [dot(results[:, c * latent : (c + 1) * latent], val_pair[c]) for c in range(2)], axis=1
    ).astype(BF16)

    for batch in (chip_order[:3], chip_order[3:]):
        peers = [lax.rem(chip + d, n_chip) for d in batch]
        for peer in peers:
            mix_out[peer] = dot(head_values, ow_pair[peer]).astype(BF16)
        for peer in peers:
            send(mix_out.at[peer], mix_in.at[chip], 5, {"tp": 2 * peer + core})
    mix_in[chip] = dot(head_values, ow_pair[chip]).astype(BF16)

    arrived(2, gate_in.at[core])
    send(gate_in.at[core], gate_in.at[core], 13, {"tp": sibling})
    arrived(4, up_in.at[core])
    send(up_in.at[core], up_in.at[core], 14, {"tp": sibling})
    side_rows = half_ep * slots
    ff = n_tp * ff_dev
    out_rows = side_rows // n_chip

    def partial_sums(in_ref, out_ref):
        for g in range(half_ep):
            for c in range(2):
                at = c * side_rows + slots * g
                route_f[at : at + slots, :] = in_ref[2 * g + c].astype(F32)
        received = [
            route_f[c * side_rows : (c + 1) * side_rows, :].astype(BF16) for c in range(2)
        ]
        for n, source in enumerate((gate_in, up_in)):
            part = dot_t(received[0], source[0].reshape(ff, cols)) + dot_t(
                received[1], source[1].reshape(ff, cols)
            )
            out_ref[:, :, n * ff : (n + 1) * ff] = part.reshape(n_chip, out_rows, ff).astype(BF16)

    def summed_parts(in_ref):
        both = in_ref[0].astype(F32)
        for t in range(1, n_chip):
            both = both + in_ref[t].astype(F32)
        return both

    at_home_or_not(18, tok_dis_in, recv_sems)
    arrived_all(13, gate_in.at[core])
    arrived_all(14, up_in.at[core])
    partial_sums(tok_dis_in, tok_part_out)
    send_chips(19, lambda peer: tok_part_out.at[peer], tok_part_in.at[chip])
    tok_part_in[chip] = tok_part_out[chip]

    arrived(5, mix_in)
    mixed = mix_in[0].astype(F32)
    for t in range(1, n_chip):
        mixed = mixed + mix_in[t].astype(F32)
    mixed = mixed.astype(BF16).astype(F32)
    scaled = mixed * my_mix_gain

    to_experts(7, scaled * my_expert_gain, dis_out, dis_in)

    def as_row(col):
        return jnp.sum(eye * col, axis=0, keepdims=True)

    def as_col(row):
        return jnp.sum(eye * row, axis=1, keepdims=True)

    def row_sum(value):
        return as_row(jnp.sum(value, axis=1, keepdims=True))

    sums = jnp.concatenate(
        [
            row_sum(mixed * mixed),
            row_sum(tok_cols * scaled),
            row_sum(scaled * scaled),
            jnp.zeros((1, rows), F32),
        ],
        axis=1,
    )
    sum_in[me] = sums
    send_tp(6, lambda peer: sum_in.at[me], sum_in.at[me])
    send_weights(8, down_v, down_in, far_of(DOWN_NEAR))
    down_in[core, me] = down_v[:, my_cols]

    arrived(6, sum_in)
    sums = sum_in[0]
    for t in range(1, n_tp):
        sums = sums + sum_in[t]
    mix_square = as_col(sums[:, 0:rows])
    cross = as_col(sums[:, rows : 2 * rows])
    scaled_square = as_col(sums[:, 2 * rows : 3 * rows])
    mix_factor = lax.rsqrt(mix_square / width + norm_floor)
    resid = (tok_cols + scaled * mix_factor).astype(BF16).astype(F32)
    resid_square = square_sum + mix_factor * (2.0 * cross + mix_factor * scaled_square)
    resid_factor = lax.rsqrt(jnp.maximum(resid_square, 0.0) / width + norm_floor)

    lanes = iota((rows, 128), 1)
    factors = jnp.where(lanes < 64, mix_factor, resid_factor)
    factor_f[...] = dot(dispatch.astype(F32), factors, HIGHEST)
    for e in range(n_ep):
        factor_out[e] = factor_f[slots * e : slots * (e + 1), :]
    per_device_groups = out_rows // slots
    speaks = me == 2 * (group // (2 * per_device_groups)) + side
    factor_place = lax.rem(group // 2, per_device_groups)

    @pl.when(speaks)
    def _():
        for offset in ep_order:
            peer = ep_peer(offset)
            send(factor_out.at[peer], factor_in.at[factor_place], 20, {"ep": peer})
        factor_in[factor_place] = factor_out[group]

    at_home_or_not(7, dis_in, recv_sems)
    partial_sums(dis_in, part_out)

    send_chips(9, lambda peer: part_out.at[peer], part_in.at[chip])
    part_in[chip] = part_out[chip]
    arrived(8, down_in.at[core])
    send(down_in.at[core], down_in.at[core], 15, {"tp": sibling})
    arrived(9, part_in)
    arrived(19, tok_part_in)

    @pl.when(speaks)
    def _():
        wait_for(recv_sems.at[20], factor_in, per_device_groups - 1)

    @pl.when(jnp.logical_not(speaks))
    def _():
        wait_for(recv_sems.at[20], factor_in, per_device_groups)

    for g in range(per_device_groups):
        factor_f[slots * g : slots * (g + 1), :] = factor_in[g]
    mix_factors = factor_f[:out_rows, 0:1]
    resid_factors = factor_f[:out_rows, 64:65]
    both = (summed_parts(tok_part_in) + mix_factors * summed_parts(part_in)) * resid_factors
    gate, upward = both[:, :ff], both[:, ff:]
    hid_in[chip] = (gate / (1.0 + jnp.exp(-gate)) * upward).astype(BF16)

    send_chips(10, lambda peer: hid_in.at[chip], hid_in.at[chip])
    arrived_all(15, down_in.at[core])
    arrived(10, hid_in)
    hidden = hid_in[...].astype(F32).reshape(side_rows, ff).astype(BF16)
    for c in range(2):
        at = c * side_rows
        route_f[at : at + side_rows, :] = dot(hidden, down_in[c].reshape(ff, cols))
        for g in range(half_ep):
            at = c * side_rows + slots * g
            ret_out[2 * g + c] = route_f[at : at + slots, :].astype(BF16)

    for z in sorted(range(1, n_z), key=lambda z: -min(z, n_z - z)):
        for x in range(EP_X // 2):
            pair = EP_X // 2 * lax.rem(group_z + z, n_z) + x
            for c in range(2):
                send(
                    ret_out.at[2 * pair + c],
                    ret_in.at[group],
                    11,
                    {"ep": 2 * pair + core, "tp": 2 * chip + c},
                )
    for x in range(1, EP_X // 2):
        pair = EP_X // 2 * group_z + lax.rem(group_x // 2 + x, EP_X // 2)
        for c in range(2):
            send(
                ret_out.at[2 * pair + c],
                ret_in.at[group],
                11,
                {"ep": 2 * pair + core, "tp": 2 * chip + c},
            )

    @pl.when(at_home)
    def _():
        ret_in[group] = ret_out[place]
        send(ret_out.at[place + 1 - 2 * core], ret_in.at[group], 11, {"tp": sibling})

    @pl.when(jnp.logical_not(at_home))
    def _():
        for c in range(2):
            send(
                ret_out.at[2 * (group // 2) + c],
                ret_in.at[group],
                11,
                {"ep": 2 * (group // 2) + core, "tp": 2 * chip + c},
            )

    at_home_or_not(11, ret_in, recv_sems)
    for e in range(n_ep):
        route_f[slots * e : slots * (e + 1), :] = ret_in[e].astype(F32)
    out[...] = (resid + dot(combine, route_f[...], HIGHEST)).astype(BF16)

    sent(0, tok_in)
    for stage, buffer in (
        (1, qry_in),
        (2, gate_in.at[core]),
        (3, att_in),
        (4, up_in.at[core]),
        (5, mix_in),
        (6, sum_in),
        (8, down_in.at[core]),
        (9, part_in),
        (10, hid_in),
        (16, val_pair),
        (19, tok_part_in),
    ):
        sent(stage, buffer)
    sent_all(13, gate_in.at[core])
    sent_all(14, up_in.at[core])
    sent_all(15, down_in.at[core])
    sent_all(17, ow_pair.at[:, head_rows])
    at_home_or_not(7, dis_in, send_sems)
    at_home_or_not(18, tok_dis_in, send_sems)

    @pl.when(speaks)
    def _():
        sent(20, factor_out)

    at_home_or_not(11, ret_in, send_sems)


def hand_over(*refs):
    sources, targets, sems = refs[:3], refs[3:6], refs[6]
    copies = [
        pltpu.make_async_copy(a, b, sems.at[i]) for i, (a, b) in enumerate(zip(sources, targets))
    ]
    for copy in copies:
        copy.start()
    for copy in copies:
        copy.wait()


def per_device(
    tokens,
    lengths,
    latent_cache,
    rope_cache,
    attn_gain,
    query_weight,
    query_rot_weight,
    latent_weight,
    key_rot_weight,
    latent_gain,
    absorb_weight,
    value_weight,
    output_weight,
    mix_gain,
    expert_gain,
    gate_weight,
    up_weight,
    down_weight,
    expert_ids,
    route_weights,
):
    n_tp, n_ep = lax.axis_size("tp"), lax.axis_size("ep")
    own, width = tokens.shape
    rows = own * n_tp
    cols = width // n_tp
    latent = latent_weight.shape[1]
    context = latent_cache.shape[1]
    ff_dev = gate_weight.shape[2]
    ff = ff_dev * n_tp
    slots = 2 * rows * expert_ids.shape[1] // n_ep
    all_slots = n_ep * slots
    n_chip = n_tp // 2
    out_rows = all_slots // n_tp

    operands = (
        tokens,
        lengths.reshape(1, rows),
        latent_cache,
        jnp.swapaxes(rope_cache, 1, 2),
        attn_gain,
        mix_gain,
        expert_gain,
        latent_gain,
        query_weight,
        query_rot_weight.T,
        latent_weight,
        key_rot_weight.T,
        absorb_weight,
        value_weight,
        output_weight,
        jnp.swapaxes(gate_weight, 1, 2),
        jnp.swapaxes(up_weight, 1, 2),
        down_weight,
        expert_ids.T,
        route_weights.T,
    )
    vmem = pltpu.VMEM
    shapes = (
        jax.ShapeDtypeStruct((rows, cols), BF16),
        jax.ShapeDtypeStruct((own, latent), BF16),
        jax.ShapeDtypeStruct((own, QK_ROPE), BF16),
    )
    results = pl.pallas_call(
        functools.partial(kernel, n_tp, n_ep),
        out_shape=shapes,
        in_specs=[
            pl.BlockSpec(memory_space=pltpu.HBM) for _ in operands
        ],
        out_specs=[pl.BlockSpec(memory_space=vmem)] * 3,
        scratch_shapes=[
            vmem((1, rows), jnp.int32),
            vmem(expert_ids.shape[::-1], jnp.int32),
            vmem(route_weights.shape[::-1], F32),
            vmem((width,), BF16),
            vmem((width,), BF16),
            vmem((width,), BF16),
            vmem((latent,), BF16),
            vmem(latent_cache.shape, BF16),
            vmem((own, QK_ROPE, context), BF16),
            vmem((width, 2 * QK_NOPE), BF16),
            vmem((QK_ROPE, width), BF16),
            vmem(latent_weight.shape, BF16),
            vmem((QK_ROPE, cols), BF16),
            vmem(absorb_weight.shape[1:], BF16),
            vmem((2, *value_weight.shape[1:]), BF16),
            vmem((n_chip, 2 * output_weight.shape[0], cols), BF16),
            vmem((ff_dev, width), BF16),
            vmem((ff_dev, width), BF16),
            vmem((ff_dev, width), BF16),
            vmem((rows, width), F32),
            vmem((rows, width), BF16),
            vmem((rows, MESSAGE), F32),
            vmem((rows, latent), F32),
            vmem((all_slots, cols), F32),
            vmem((all_slots, 128), F32),
            vmem((n_tp, own, width), BF16),
            vmem((n_tp, own, MESSAGE), BF16),
            vmem((n_tp, own, MESSAGE), BF16),
            vmem((n_chip, own, 2 * latent), BF16),
            vmem((n_tp, own, 2 * latent), BF16),
            vmem((n_chip, rows, cols), BF16),
            vmem((n_chip, rows, cols), BF16),
            vmem((n_tp, 1, 4 * rows), F32),
            vmem((n_ep, slots, cols), BF16),
            vmem((n_ep, slots, cols), BF16),
            vmem((n_chip, out_rows, 2 * ff), BF16),
            vmem((n_chip, out_rows, 2 * ff), BF16),
            vmem((n_ep, slots, cols), BF16),
            vmem((n_ep, slots, cols), BF16),
            vmem((n_chip, out_rows, 2 * ff), BF16),
            vmem((n_chip, out_rows, 2 * ff), BF16),
            vmem((n_ep, slots, 128), F32),
            vmem((out_rows // slots, slots, 128), F32),
            vmem((n_chip, out_rows, ff), BF16),
            vmem((n_ep, slots, cols), BF16),
            vmem((n_ep, slots, cols), BF16),
            vmem((2, n_tp, ff_dev, cols), BF16),
            vmem((2, n_tp, ff_dev, cols), BF16),
            vmem((2, n_tp, ff_dev, cols), BF16),
            pltpu.SemaphoreType.DMA((20,)),
            pltpu.SemaphoreType.DMA((21,)),
            pltpu.SemaphoreType.DMA((21,)),
            pltpu.SemaphoreType.DMA((n_chip,)),
        ],
        compiler_params=pltpu.CompilerParams(
            collective_id=0, has_side_effects=True, vmem_limit_bytes=40 * 1024 * 1024
        ),
    )(*[pltpu.with_memory_space_constraint(x, pltpu.HBM) for x in operands])
    return pl.pallas_call(
        hand_over,
        out_shape=shapes,
        in_specs=[pl.BlockSpec(memory_space=vmem)] * 3,
        out_specs=[pl.BlockSpec(memory_space=pltpu.HBM)] * 3,
        scratch_shapes=[pltpu.SemaphoreType.DMA((3,))],
        compiler_params=pltpu.CompilerParams(vmem_limit_bytes=16 * 1024 * 1024),
    )(*results)


def solution(mesh):
    placed = (
        P(("ep", "tp"), None),
        P("ep"),
        P(("ep", "tp"), None, None),
        P(("ep", "tp"), None, None),
        P(),
        P(None, "tp"),
        P(None, "tp"),
        P("tp", None),
        P("tp", None),
        P(),
        P("tp", None, None),
        P("tp", None, None),
        P("tp", None),
        P(),
        P(),
        P("ep", None, "tp"),
        P("ep", None, "tp"),
        P("ep", "tp", None),
        P("ep", None),
        P("ep", None),
    )
    return jax.shard_map(
        per_device,
        mesh=mesh,
        in_specs=placed,
        out_specs=(P("ep", "tp"), P(("ep", "tp"), None), P(("ep", "tp"), None)),
        check_vma=False,
    )
```
